256 devices in a mesh: sp: 32 (over z, y), tp: 8 (over x, core).
Axes of the slice: x: 4, y: 4, z: 8, core: 2. Of those that a mesh axis runs over, the one named last changes fastest.
Arguments:
- tokens: bfloat16 [16384, 2048], P(('sp', 'tp')), may hold values from -8 to 8, as said below
- w_query: bfloat16 [2048, 1024], P(None, 'tp'), may hold values from -0.125 to 0.125
- w_key: bfloat16 [2048, 1024], P(None, 'tp'), may hold values from -0.125 to 0.125
- w_value: bfloat16 [2048, 1024], P(None, 'tp'), may hold values from -0.125 to 0.125
- head_bias: float32 [16], P('tp'), may hold values from -40 to -3
- w_out: bfloat16 [1024, 2048], P('tp'), may hold values from -0.1875 to 0.1875
Outputs:
- mixed: bfloat16 [16384, 2048], P(('sp', 'tp'))
The draws below stay inside these ranges and needn't reach their ends.
Inputs may be any that keep to these rules, and one draw needn't show every extreme that they name: `tokens`: activations of order one whose mean shifts between blocks of 512 positions.
All inputs are finite; a program needn't handle non-finite values.
Results may differ from the reference program's by a relative error of at most 0.014.
Values may be sent and summed in bfloat16 or wider, within the bound.
A program may use at most 128 MiB of HBM per device.

```python
import jax
import jax.numpy as jnp
from jax import lax

D = 2048
HEADS = 16
HEAD_DIM = 64
TOK_DEV = 512
TOKENS = 16384
N_SP = 32
N_TP = 8


def draw_tokens(key, part):
    noise = jax.random.normal(jax.random.fold_in(key, 11), (TOKENS, D), jnp.float32)
    spread_level = 1.0
    direction = jax.random.normal(jax.random.fold_in(key, 12), (D,), jnp.float32)
    region_scale = jax.random.uniform(jax.random.fold_in(key, 13), (TOKENS // TOK_DEV,), jnp.float32, -1.2, 1.2)
    level = jnp.repeat(region_scale, TOK_DEV) * spread_level
    values = 0.8 * noise + level[:, None] * direction[None, :]
    return jnp.clip(values, -8.0, 8.0).astype(jnp.bfloat16)


def draw_head_bias(key, part):
    fast_count = HEADS // 2
    ranking = jax.random.permutation(jax.random.fold_in(key, 21), HEADS)
    is_fast = ranking < fast_count
    slow_value = -jnp.log(jnp.float32(TOKENS)) - 1.0 + jax.random.uniform(jax.random.fold_in(key, 22), (HEADS,), jnp.float32, -0.5, 0.5)
    fast_value = -jnp.log(jax.random.uniform(jax.random.fold_in(key, 23), (HEADS,), jnp.float32, 30.0, 100.0)) - 1.0
    return jnp.where(is_fast, fast_value, slow_value).astype(jnp.float32)


def levels(stream_key, extent, split, smallest, largest):
    gain, own = 1.0, jax.random.fold_in(stream_key, 6)
    for dim, shards_of in split:
        draws = jnp.exp(jax.random.uniform(jax.random.fold_in(own, dim), (shards_of,), jnp.float32, smallest / len(split), largest / len(split)))
        gain = gain * jnp.repeat(draws, extent[dim] // shards_of).reshape([-1 if axis == dim else 1 for axis in range(len(extent))])
    return gain


def centred(key, dims, deviation, bound, shards=(), kind=jnp.bfloat16):
    values = deviation * jax.random.normal(key, dims, jnp.float32)
    if shards:
        values = values * levels(key, dims, shards, -0.22, 0.18)
    return jnp.clip(values, -bound, bound).astype(kind)


def setup_inputs(seed: int = 0) -> dict:
    key_of = jax.random.split(jax.random.key(seed), 7)
    tokens = draw_tokens(jax.random.fold_in(key_of[6], 71), 0)
    w_query = centred(key_of[1], (D, HEADS * HEAD_DIM), D ** -0.5, 0.125, ((1, 8),))
    w_key = centred(key_of[2], (D, HEADS * HEAD_DIM), D ** -0.5, 0.125, ((1, 8),))
    w_value = centred(key_of[3], (D, HEADS * HEAD_DIM), D ** -0.5, 0.125, ((1, 8),))
    head_bias = draw_head_bias(jax.random.fold_in(key_of[6], 71), 0)
    w_out = centred(key_of[5], (HEADS * HEAD_DIM, D), (HEADS * HEAD_DIM) ** -0.5, 0.1875, ((0, 8),))
    return dict(tokens=tokens, w_query=w_query, w_key=w_key, w_value=w_value, head_bias=head_bias, w_out=w_out)


def reference(tokens, w_query, w_key, w_value, head_bias, w_out):
    query_all = jnp.dot(tokens, w_query, preferred_element_type=jnp.float32).astype(jnp.bfloat16)
    key_all = jnp.dot(tokens, w_key, preferred_element_type=jnp.float32).astype(jnp.bfloat16)
    value_all = jnp.dot(tokens, w_value, preferred_element_type=jnp.float32).astype(jnp.bfloat16)
    key_pos = jnp.arange(TOKENS, dtype=jnp.int32).reshape(N_SP, TOK_DEV)

    def by_head(head_index):
        first_col = (head_index * HEAD_DIM).astype(jnp.int32)
        query_head = lax.dynamic_slice_in_dim(query_all, first_col, HEAD_DIM, 1)
        key_head = lax.dynamic_slice_in_dim(key_all, first_col, HEAD_DIM, 1)
        value_head = lax.dynamic_slice_in_dim(value_all, first_col, HEAD_DIM, 1)
        value_segments = value_head.reshape(N_SP, TOK_DEV, HEAD_DIM).astype(jnp.float32)
        bias_value = head_bias[head_index]

        def by_block(block_index):
            first_row = (block_index * TOK_DEV).astype(jnp.int32)
            query_block = lax.dynamic_slice_in_dim(query_head, first_row, TOK_DEV, 0)
            query_pos = first_row + jnp.arange(TOK_DEV, dtype=jnp.int32)
            scores = jnp.dot(query_block, key_head.T, preferred_element_type=jnp.float32)
            scores = scores.reshape(TOK_DEV, N_SP, TOK_DEV) * (HEAD_DIM ** -0.5) + bias_value
            causal = key_pos[None] < query_pos[:, None, None]
            log_keep = jnp.where(causal, jax.nn.log_sigmoid(-scores), 0.0)
            tail = lax.cumsum(log_keep, axis=2, reverse=True) - log_keep
            weights = jnp.where(causal, jnp.exp(jax.nn.log_sigmoid(scores) + tail), 0.0).astype(jnp.bfloat16)
            segment_out = jnp.einsum('qst,std->qsd', weights.astype(jnp.float32), value_segments)
            segment_total = jnp.sum(log_keep, axis=2)
            later = lax.cumsum(segment_total, axis=1, reverse=True) - segment_total
            return jnp.sum(jnp.exp(later)[..., None] * segment_out, axis=1)

        return lax.map(by_block, jnp.arange(N_SP, dtype=jnp.int32)).reshape(TOKENS, HEAD_DIM)

    heads_out = lax.map(by_head, jnp.arange(HEADS, dtype=jnp.int32))
    attended = jnp.transpose(heads_out, (1, 0, 2)).reshape(TOKENS, HEADS * HEAD_DIM).astype(jnp.bfloat16)
    group_width = HEADS * HEAD_DIM // N_TP
    total = jnp.zeros((TOKENS, D), jnp.float32)
    for group_index in range(N_TP):
        lower = group_index * group_width
        partial_value = jnp.dot(attended[:, lower:lower + group_width], w_out[lower:lower + group_width, :],
                          preferred_element_type=jnp.float32).astype(jnp.bfloat16)
        partial_value = lax.optimization_barrier(partial_value)
        total = total + partial_value.astype(jnp.float32)
    return total.astype(jnp.bfloat16)
```

```python
import functools
import math

import jax
import jax.numpy as jnp
from jax import lax
from jax.experimental import pallas as pl
from jax.experimental.pallas import tpu as pltpu
from jax.sharding import PartitionSpec as P

MESH = pl.DeviceIdType.MESH
F32, BF16 = jnp.float32, jnp.bfloat16
LOG2E = math.log2(math.e)
PARTS = 4
COLS = 512
EXP_MAX = 126.0
DEAD = -1e30
NZ, NY = 8, 4
SEG = 512
HALF = 256
LANES = 128
DIM = 64
RUN = 64
SHARE = 32
SHARES = SEG // SHARE
TILES = 8
FAR = 1 << 20


def layer_kernel(
    bias_ref, tokens_ref, wq_ref, wk_ref, wv_ref, wo_ref, out_ref,
    tok, wqkv, wfull, proj, bias_all, kv_own, q_own, q_all, kv_all, q_top, q_low, xs, seg_acc,
    seg_keep, packed, att, att_rows,
    load_sem, tok_send, tok_recv, wo_send, wo_recv, bias_send, bias_recv, kv_send, kv_recv,
    ring_send, share_send, q_send, q_recv, back_send, back_recv,
):
    me = lax.axis_index("sp")
    col = lax.axis_index("tp")
    n_sp, n_tp = NZ * NY, 8
    z, y = me // NY, lax.rem(me, NY)
    place, core = col // 2, lax.rem(col, 2)
    places = n_tp // 2
    sibling = place * 2 + 1 - core
    head_core, head_local = y // 2, lax.rem(y, 2)
    mine = core == head_core

    loads = [
        pltpu.make_async_copy(src, dst, load_sem.at[index])
        for index, (src, dst) in enumerate(
            [
                (tokens_ref, tok.at[col]),
                (wq_ref, wqkv.at[:, 0:LANES]),
                (wk_ref, wqkv.at[:, LANES : 2 * LANES]),
                (wv_ref, wqkv.at[:, 2 * LANES : 3 * LANES]),
                (wo_ref, wfull.at[col]),
            ]
        )
    ]
    for copy in loads:
        copy.start()

    barrier = pltpu.get_barrier_semaphore()
    total = n_sp * n_tp
    flat = me * n_tp + col

    def greet(step, carry):
        other = lax.rem(flat + step, total)
        pl.semaphore_signal(
            barrier, inc=1, device_id=(other // n_tp, lax.rem(other, n_tp)), device_id_type=MESH
        )
        return carry

    lax.fori_loop(1, total, greet, 0)
    for head in range(2):
        bias_all[core, head] = jnp.full((8, LANES), bias_ref[head] * LOG2E, F32)
    pl.semaphore_wait(barrier, total - 1)

    def same_core(k):
        return lax.rem(place + k, places) * 2 + core

    def arrived(ref, sem):
        pltpu.make_async_copy(ref, ref, sem).wait()

    def token_copy(kind, part):
        if kind < places:
            src, block = tokens_ref.at[part], col
            target = sibling if kind == 0 else same_core(kind)
        else:
            block = same_core(kind - places + 1)
            src, target = tok.at[block, part], sibling
        return pltpu.make_async_remote_copy(
            src_ref=src, dst_ref=tok.at[block, part],
            send_sem=tok_send.at[kind, part], recv_sem=tok_recv.at[block, part],
            device_id=(me, target), device_id_type=MESH,
        )

    def wo_copy(kind):
        if kind < places:
            src, block = wo_ref, col
            target = sibling if kind == 0 else same_core(kind)
        else:
            block = same_core(kind - places + 1)
            src, target = wfull.at[block], sibling
        return pltpu.make_async_remote_copy(
            src_ref=src, dst_ref=wfull.at[block],
            send_sem=wo_send.at[kind], recv_sem=wo_recv.at[block],
            device_id=(me, target), device_id_type=MESH,
        )

    bias_copy = pltpu.make_async_remote_copy(
        src_ref=bias_all.at[core], dst_ref=bias_all.at[core],
        send_sem=bias_send, recv_sem=bias_recv, device_id=(me, sibling), device_id_type=MESH,
    )

    for part in range(PARTS):
        for kind in range(places):
            token_copy(kind, part).start()
    bias_copy.start()

    def kv_copy(head, half):
        aim = core * 2 + head
        own = aim == y
        sp = jnp.where(own, me, z * NY + aim)
        tp = jnp.where(own, sibling, place * 2 + half)
        return pltpu.make_async_remote_copy(
            src_ref=kv_own.at[head, half], dst_ref=kv_all.at[me, half],
            send_sem=kv_send.at[head, half], recv_sem=kv_recv.at[me, half],
            device_id=(sp, tp), device_id_type=MESH,
        )

    def ring_copy(block, way):
        peer = lax.rem(z + (1 if way == 0 else NZ - 1), NZ) * NY + y
        return pltpu.make_async_remote_copy(
            src_ref=kv_all.at[block, core], dst_ref=kv_all.at[block, core],
            send_sem=ring_send.at[block, way], recv_sem=kv_recv.at[block, core],
            device_id=(peer, col), device_id_type=MESH,
        )

    def share_copy(block):
        return pltpu.make_async_remote_copy(
            src_ref=kv_all.at[block, core], dst_ref=kv_all.at[block, core],
            send_sem=share_send.at[block], recv_sem=kv_recv.at[block, core],
            device_id=(me, sibling), device_id_type=MESH,
        )

    def rows_of(to_z, to_core, block):
        return lax.rem(2 * to_z + to_core + 2 * block, SHARES)

    def q_copy(head, step):
        to_z, to_core = step // 2, lax.rem(step, 2)
        return pltpu.make_async_remote_copy(
            src_ref=q_own.at[head, rows_of(to_z, to_core, me)], dst_ref=q_all.at[me],
            send_sem=q_send.at[head, step], recv_sem=q_recv.at[me],
            device_id=(to_z * NY + core * 2 + head, place * 2 + to_core), device_id_type=MESH,
        )

    def q_here(head, step):
        to_z, to_core = step // 2, lax.rem(step, 2)
        return jnp.logical_and(to_z * NY + core * 2 + head == me, to_core == core)

    def back_owner(block):
        return lax.rem(z + block, n_tp)

    my_slot = (place * NY + y) * 2 + core

    def back_here(block):
        return jnp.logical_and(block == me, back_owner(block) == col)

    def back_copy(block):
        return pltpu.make_async_remote_copy(
            src_ref=packed.at[block], dst_ref=att.at[my_slot],
            send_sem=back_send.at[block], recv_sem=back_recv.at[my_slot],
            device_id=(block, back_owner(block)), device_id_type=MESH,
        )

    for copy in loads:
        copy.wait()
    for part in range(PARTS):
        for k in range(1, places):
            block = same_core(k)
            arrived(tok.at[block, part], tok_recv.at[block, part])
            token_copy(places + k - 1, part).start()
        arrived(tok.at[sibling, part], tok_recv.at[sibling, part])
        for k in range(1, places):
            block = lax.rem(place + k, places) * 2 + 1 - core
            arrived(tok.at[block, part], tok_recv.at[block, part])
        x = tok[:, part]
        depth = x.shape[1]
        both = jnp.dot(
            x.reshape(n_tp * depth, x.shape[2]), wqkv[...], preferred_element_type=F32
        )
        proj[:, part * depth : (part + 1) * depth, :] = both.reshape(n_tp, depth, 3 * LANES)
    for kind in range(places):
        wo_copy(kind).start()

    def turn(value):
        return pltpu.roll(value, DIM, 1)

    lane16 = lax.broadcasted_iota(jnp.int32, (16, LANES), 1)

    def weave(upper, lower):
        first = jnp.where(lane16 < DIM, upper, turn(lower)).astype(BF16)
        second = jnp.where(lane16 < DIM, turn(upper), lower).astype(BF16)
        return first, second

    def strided(i, kind):
        return proj[:, RUN - 1 - i, kind * LANES : (kind + 1) * LANES]

    for i in range(0, RUN // 2, 2):
        upper = jnp.concatenate([strided(i, 1), strided(i + 1, 1)], axis=0)
        lower = jnp.concatenate([strided(i + 32, 1), strided(i + 33, 1)], axis=0)
        kv_own[0, 0, 8 * i : 8 * i + 16], kv_own[1, 0, 8 * i : 8 * i + 16] = weave(upper, lower)
    for half in range(1):
        for head in range(2):
            kv_copy(head, half).start()
    for piece in range(4):
        block = jnp.concatenate([strided(16 * piece + i, 2) for i in range(16)], axis=0)
        flipped = block.T.astype(BF16)
        for head in range(2):
            kv_own[head, 1, DIM * piece : DIM * (piece + 1)] = flipped[DIM * head : DIM * (head + 1)]
    for head in range(2):
        kv_copy(head, 1).start()

    for share in range(SHARES):
        block, first = share // 2, 32 * (share % 2)
        q = proj[block, first : first + 32, 0:LANES] * (LOG2E * DIM ** (-0.5))
        q_own[0, share], q_own[1, share] = weave(q[:16], q[16:])

    def send_q(step, carry):
        for head in range(2):

            @pl.when(jnp.logical_not(q_here(head, step)))
            def _():
                q_copy(head, step).start()

        return carry

    lax.fori_loop(0, 2 * NZ, send_q, 0)

    for head in range(2):

        @pl.when(core * 2 + head == y)
        def _():
            kv_all[me] = kv_own[head]
            q_all[me] = q_own[head, rows_of(z, core, me)]

    def pass_on(block, step, sign):
        if step == 0:

            @pl.when(block != me)
            def _():
                arrived(kv_all.at[block, core], kv_recv.at[block, core])
                share_copy(block).start()

            @pl.when(jnp.logical_and(block == me, jnp.logical_not(mine)))
            def _():
                arrived(kv_all.at[block, core], kv_recv.at[block, core])

            for way in range(2):
                ring_copy(block, way).start()
        else:
            arrived(kv_all.at[block, core], kv_recv.at[block, core])
            share_copy(block).start()

    def group_at(offset):
        return lax.rem(z + offset + NZ, NZ)

    for part in range(NY):
        block = z * NY + part
        pass_on(block, 0, 0)

    def take_q(block, carry):
        @pl.when(jnp.logical_not(jnp.logical_and(block == me, mine)))
        def _():
            arrived(q_all.at[block], q_recv.at[block])

        return carry

    lax.fori_loop(0, n_sp, take_q, 0)

    def build(tile, carry):
        pieces = []
        for part in range(NY):
            pair = q_all[tile * NY + part].astype(F32)
            pieces.append(jnp.where(lane16 < DIM, pair, 0.0))
            pieces.append(jnp.where(lane16 < DIM, turn(pair), 0.0))
        flipped = jnp.concatenate(pieces, axis=0).T
        q_top[tile] = flipped.astype(BF16)
        q_low[tile] = jnp.concatenate([flipped[DIM:], flipped[:DIM]], axis=0).astype(BF16)
        return carry

    lax.fori_loop(0, TILES, build, 0)
    arrived(bias_all.at[1 - core], bias_recv)

    def suffix(keep):
        row = lax.broadcasted_iota(jnp.int32, keep.shape, 0)
        product = keep
        for step in (1, 2, 4):
            moved = pltpu.roll(product, 8 - step, 0)
            product = product * jnp.where(row + step < 8, moved, 1.0)
        after = jnp.where(row + 1 < 8, pltpu.roll(product, 7, 0), 1.0)
        return after, product[0:1]

    def segment(block, slot, q, width, bias, reach):
        scores = jnp.dot(kv_all[block, 0], q, preferred_element_type=F32)
        keep = jnp.ones((8, 2 * width), F32)
        for i in range(RUN // 2):
            score = scores[8 * i : 8 * i + 8] + bias
            if reach is not None:
                score = jnp.where(reach > -i, score, DEAD)
            odds = jnp.exp2(jnp.minimum(score, EXP_MAX))
            lose = 1.0 / (1.0 + odds)
            xs[slot, 8 * i : 8 * i + 8, 0 : 2 * width] = odds * lose * keep
            keep = keep * lose
        near, far = keep[:, :width], keep[:, width:]
        after, whole = suffix(near * far)
        values = kv_all[block, 1]
        out = None
        for half, factor in enumerate((after, after * near)):
            part = xs[slot, :, half * width : (half + 1) * width].reshape(RUN // 2, 8, width)
            weight = (part * factor[None]).reshape(HALF, width).astype(BF16)
            first = 2 * half * DIM
            value = jnp.concatenate(
                [values[first : first + DIM], values[first + DIM : first + 2 * DIM]], axis=1
            )
            term = jnp.dot(value, weight, preferred_element_type=F32)
            out = term if out is None else out + term
        return out, whole

    def cover(group, tile, count, diagonal):
        width = count * LANES
        q = jnp.concatenate(
            [q_top[tile + n] for n in range(count)] + [q_low[tile + n] for n in range(count)],
            axis=1,
        )
        bias = bias_all[head_core, head_local]
        bias = jnp.concatenate([bias] * (2 * count), axis=1)
        if diagonal:
            lane = lax.broadcasted_iota(jnp.int32, (8, 2 * width), 1)
            row = lax.broadcasted_iota(jnp.int32, (8, 2 * width), 0)
            half = lane // width
            inside = lax.rem(lane, width)
            part = lax.rem(inside // SHARE, NY)
            share = rows_of(z, core, tile * NY + part)
            query = SEG * part + SHARE * share + lax.rem(inside, SHARE)
            query = jnp.where(inside < LANES, query, FAR)
            reach = query - row * RUN - (RUN - 1) + half * (RUN // 2)
        acc = keep = None
        for part in range(NY):
            limit = reach - SEG * part if diagonal else None
            out, whole = segment(group * NY + part, part, q, width, bias, limit)
            acc = out if acc is None else acc * whole + out
            keep = whole if keep is None else keep * whole
        for n in range(count):
            seg_acc[group, tile + n] = acc[:, n * LANES : (n + 1) * LANES]
            seg_keep[group, tile + n] = jnp.broadcast_to(
                keep[:, n * LANES : (n + 1) * LANES], (8, LANES)
            )

    def attend(group):
        count = TILES - group
        odd = lax.rem(count, 2)

        @pl.when(odd == 1)
        def _():
            cover(group, group, 1, True)

        @pl.when(odd == 0)
        def _():
            cover(group, group, 2, True)

        def pair(step, carry):
            cover(group, group + 2 - odd + 2 * step, 2, False)
            return carry

        lax.fori_loop(0, (count - 1) // 2, pair, 0)

    def visit(step, carry):
        distance = (step + 1) // 2
        back = lax.rem(step, 2)
        group = lax.rem(z + NZ + jnp.where(back == 1, -distance, distance), NZ)

        @pl.when(jnp.logical_and(step > 0, step < NZ - 1))
        def _():
            for part in range(NY):
                block = group * NY + part
                arrived(kv_all.at[block, core], kv_recv.at[block, core])
                for way in range(2):
                    last = (part < NY // 2) == (way == 0)

                    @pl.when(
                        jnp.logical_and(back == 1 - way, distance < (4 if last else 3))
                    )
                    def _():
                        ring_copy(block, way).start()

                share_copy(block).start()

        @pl.when(step == NZ - 1)
        def _():
            for part in range(NY):
                block = group * NY + part
                arrived(kv_all.at[block, core], kv_recv.at[block, core])
                share_copy(block).start()
            for k in range(1, places):
                arrived(wfull.at[same_core(k)], wo_recv.at[same_core(k)])
                wo_copy(places + k - 1).start()

        for part in range(NY):
            block = group * NY + part

            @pl.when(jnp.logical_not(jnp.logical_and(block == me, mine)))
            def _():
                arrived(kv_all.at[block, 1 - core], kv_recv.at[block, 1 - core])

        attend(group)
        return carry

    lax.fori_loop(0, NZ, visit, 0)

    def combine(tile):
        def add(group, acc):
            return acc * seg_keep[group, tile][0:1] + seg_acc[group, tile]

        return lax.fori_loop(0, tile + 1, add, jnp.zeros((DIM, LANES), F32))

    def deliver(pair, carry):
        flipped = jnp.concatenate([combine(2 * pair), combine(2 * pair + 1)], axis=0).T
        for part in range(NY):
            upper = flipped[SHARE * part : SHARE * part + 16]
            lower = flipped[SHARE * part + 16 : SHARE * (part + 1)]
            for n, folded in enumerate(weave(upper, lower)):
                block = (2 * pair + n) * NY + part
                packed[block] = folded
                here = back_here(block)

                @pl.when(here)
                def _():
                    att[my_slot] = folded

                @pl.when(jnp.logical_not(here))
                def _():
                    back_copy(block).start()

        return carry

    lax.fori_loop(0, TILES // 2, deliver, 0)

    source_z = lax.rem(col + n_sp - me, NZ)
    for pair in range(n_tp):
        for sub in range(2):
            values = []
            for head in (2 * pair, 2 * pair + 1):
                slot = head * 2 + sub
                here = jnp.logical_and(source_z * NY + head % NY == me, 2 * (head // NY) + sub == col)

                @pl.when(jnp.logical_not(here))
                def _():
                    arrived(att.at[slot], back_recv.at[slot])

                values.append(att[slot].astype(F32))
            top = jnp.where(lane16 < DIM, values[0], turn(values[1]))
            low = jnp.where(lane16 < DIM, turn(values[0]), values[1])
            cols = slice(pair * LANES, (pair + 1) * LANES)
            att_rows[SHARE * sub : SHARE * sub + 16, cols] = top.astype(BF16)
            att_rows[SHARE * sub + 16 : SHARE * (sub + 1), cols] = low.astype(BF16)

    arrived(wfull.at[sibling], wo_recv.at[sibling])
    for k in range(1, places):
        block = lax.rem(place + k, places) * 2 + 1 - core
        arrived(wfull.at[block], wo_recv.at[block])
    for first in range(0, out_ref.shape[1], COLS):
        w = wfull[:, :, first : first + COLS].reshape(att_rows.shape[1], COLS)
        out_ref[:, first : first + COLS] = jnp.dot(
            att_rows[...], w, preferred_element_type=F32
        ).astype(BF16)

    bias_copy.wait_send()
    for kind in range(2 * places - 1):
        wo_copy(kind).wait_send()
        for part in range(PARTS):
            token_copy(kind, part).wait_send()
    for head in range(2):
        for half in range(2):
            kv_copy(head, half).wait_send()

    def drain_q(step, carry):
        for head in range(2):

            @pl.when(jnp.logical_not(q_here(head, step)))
            def _():
                q_copy(head, step).wait_send()

        return carry

    lax.fori_loop(0, 2 * NZ, drain_q, 0)

    def drain(block, carry):
        ahead = lax.rem(z - block // NY + NZ, NZ)
        behind = lax.rem(NZ - ahead, NZ)
        first = lax.rem(block, NY) < NY // 2

        @pl.when(jnp.logical_or(ahead < 3, jnp.logical_and(ahead == 3, first)))
        def _():
            ring_copy(block, 0).wait_send()

        @pl.when(
            jnp.logical_or(behind < 3, jnp.logical_and(behind == 3, jnp.logical_not(first)))
        )
        def _():
            ring_copy(block, 1).wait_send()

        @pl.when(block != me)
        def _():
            share_copy(block).wait_send()

        @pl.when(jnp.logical_not(back_here(block)))
        def _():
            back_copy(block).wait_send()

        return carry

    lax.fori_loop(0, n_sp, drain, 0)


def shards(tokens, w_query, w_key, w_value, head_bias, w_out):
    model, local_width = w_query.shape
    n_tp = lax.axis_size("tp")
    n_sp = lax.axis_size("sp")
    device_rows = tokens.shape[0]
    out_width = w_out.shape[1]
    kinds = n_tp - 1

    smem = pl.BlockSpec(memory_space=pltpu.SMEM)
    anywhere = pl.BlockSpec(memory_space=pl.ANY)
    dma = pltpu.SemaphoreType.DMA

    def vmem(*shape):
        return pltpu.VMEM(shape, BF16)

    return pl.pallas_call(
        layer_kernel,
        out_shape=jax.ShapeDtypeStruct((device_rows, out_width), BF16),
        in_specs=[smem] + [anywhere] * 5,
        out_specs=pl.BlockSpec(memory_space=pltpu.VMEM),
        scratch_shapes=[
            vmem(n_tp, PARTS, device_rows // PARTS, model),
            vmem(model, 3 * local_width),
            vmem(n_tp, local_width, out_width),
            pltpu.VMEM((n_tp, device_rows, 3 * local_width), F32),
            pltpu.VMEM((2, 2, 8, LANES), F32),
            vmem(2, 2, HALF, LANES),
            vmem(2, SHARES, SHARE // 2, LANES),
            vmem(n_sp, SHARE // 2, LANES),
            vmem(n_sp, 2, HALF, LANES),
            vmem(TILES, LANES, LANES),
            vmem(TILES, LANES, LANES),
            pltpu.VMEM((NY, HALF, 4 * LANES), F32),
            pltpu.VMEM((NZ, TILES, DIM, LANES), F32),
            pltpu.VMEM((NZ, TILES, 8, LANES), F32),
            vmem(n_sp, SHARE // 2, LANES),
            vmem(32, SHARE // 2, LANES),
            vmem(device_rows, n_tp * local_width),
            dma((5,)),
            dma((kinds, PARTS)),
            dma((n_tp, PARTS)),
            dma((kinds,)),
            dma((n_tp,)),
            dma,
            dma,
            dma((2, 2)),
            dma((n_sp, 2)),
            dma((n_sp, 2)),
            dma((n_sp,)),
            dma((2, 2 * NZ)),
            dma((n_sp,)),
            dma((n_sp,)),
            dma((32,)),
        ],
        compiler_params=pltpu.CompilerParams(
            collective_id=0, has_side_effects=True, vmem_limit_bytes=60 * 2**20
        ),
        name="layer",
    )(
        head_bias,
        tokens.reshape(PARTS, device_rows // PARTS, model),
        w_query, w_key, w_value, w_out,
    )


def solution(mesh):
    placed = (
        P(("sp", "tp"), None),
        P(None, "tp"),
        P(None, "tp"),
        P(None, "tp"),
        P("tp"),
        P("tp", None),
    )
    return jax.shard_map(
        shards, mesh=mesh, in_specs=placed, out_specs=P(("sp", "tp"), None), check_vma=False
    )
```

```python
import functools
import math

import jax
import jax.numpy as jnp
from jax import lax
from jax.experimental import pallas as pl
from jax.experimental.pallas import tpu as pltpu
from jax.sharding import PartitionSpec as P

MESH = pl.DeviceIdType.MESH
F32, BF16 = jnp.float32, jnp.bfloat16
LOG2E = math.log2(math.e)
PARTS = 4
COLS = 512
EXP_MAX = 126.0
DEAD = -1e30
NZ, NY = 8, 4
SEG = 512
HALF = 256
LANES = 128
DIM = 64
RUN = 64
SHARE = 32
SHARES = SEG // SHARE
TILES = 8
FAR = 1 << 20
BATCH = 2
STEPS = NZ * NY // BATCH


def layer_kernel(
    bias_ref, tokens_ref, wq_ref, wk_ref, wv_ref, wo_ref, out_ref,
    tok, wqkv, wfull, proj, bias_all, kv_own, q_own, q_all, kv_all, q_top, q_low, raw, xs,
    seg_acc, seg_keep, packed, att, att_rows,
    plane_sem, load_sem, tok_send, tok_recv, wo_send, wo_recv, bias_send, bias_recv, kv_send, kv_recv,
    ring_send, share_send, q_send, q_recv, back_send, back_recv,
):
    me = lax.axis_index("sp")
    col = lax.axis_index("tp")
    n_sp, n_tp = NZ * NY, 8
    z, y = me // NY, lax.rem(me, NY)
    place, core = col // 2, lax.rem(col, 2)
    places = n_tp // 2
    sibling = place * 2 + 1 - core
    head_core, head_local = y // 2, lax.rem(y, 2)
    mine = core == head_core

    loads = [
        pltpu.make_async_copy(src, dst, load_sem.at[index])
        for index, (src, dst) in enumerate(
            [
                (tokens_ref, tok.at[col]),
                (wq_ref, wqkv.at[:, 0:LANES]),
                (wk_ref, wqkv.at[:, LANES : 2 * LANES]),
                (wv_ref, wqkv.at[:, 2 * LANES : 3 * LANES]),
                (wo_ref, wfull.at[col]),
            ]
        )
    ]
    for copy in loads:
        copy.start()

    barrier = pltpu.get_barrier_semaphore()
    for step in range(1, n_tp):
        pl.semaphore_signal(
            barrier, inc=1, device_id=(me, lax.rem(col + step, n_tp)), device_id_type=MESH
        )
    for step in range(1, NY):
        peer = z * NY + lax.rem(y + step, NY)
        for other in range(2):
            pl.semaphore_signal(
                barrier, inc=1, device_id=(peer, place * 2 + other), device_id_type=MESH
            )
    for step in range(1, NZ):
        peer = lax.rem(z + step, NZ) * NY + y
        pl.semaphore_signal(barrier, inc=1, device_id=(peer, col), device_id_type=MESH)
    for head in range(2):
        bias_all[core, head] = jnp.full((8, LANES), bias_ref[head] * LOG2E, F32)
    seg_acc[...] = jnp.zeros_like(seg_acc)
    seg_keep[...] = jnp.ones_like(seg_keep)
    pl.semaphore_wait(barrier, n_tp - 1 + 2 * (NY - 1) + NZ - 1)
    for step in range(1, NZ):
        peer = lax.rem(z + step, NZ) * NY + y
        pl.semaphore_signal(plane_sem, inc=1, device_id=(peer, col), device_id_type=MESH)

    def same_core(k):
        return lax.rem(place + k, places) * 2 + core

    def arrived(ref, sem):
        pltpu.make_async_copy(ref, ref, sem).wait()

    def link(kind, own, kept, sent, received, part):
        if kind == 2:
            ahead = part < PARTS // 2
            block = same_core(3 if ahead else 1)
            src, target = kept.at[block, part], same_core(1 if ahead else 3)
        elif kind < places:
            src, block = own.at[part], col
            target = sibling if kind == 0 else same_core(kind)
        else:
            block = same_core(kind - places + 1)
            src, target = kept.at[block, part], sibling
        return pltpu.make_async_remote_copy(
            src_ref=src, dst_ref=kept.at[block, part],
            send_sem=sent.at[kind, part], recv_sem=received.at[block, part],
            device_id=(me, target), device_id_type=MESH,
        )

    def token_copy(kind, part):
        return link(kind, tokens_ref, tok, tok_send, tok_recv, part)

    def wo_copy(kind, part):
        return link(kind, wo_ref, wfull, wo_send, wo_recv, part)

    def relay(copy, kept, received, part, k):
        block = same_core(k)
        arrived(kept.at[block, part], received.at[block, part])
        copy(places + k - 1, part).start()
        if k != 2 and (part < PARTS // 2) == (k == 3):
            copy(2, part).start()

    bias_copy = pltpu.make_async_remote_copy(
        src_ref=bias_all.at[core], dst_ref=bias_all.at[core],
        send_sem=bias_send, recv_sem=bias_recv, device_id=(me, sibling), device_id_type=MESH,
    )

    turned = (2, 3, 0, 1)
    for part in range(PARTS):
        token_copy(1, part).start()
        token_copy(3, turned[part]).start()
        token_copy(0, part).start()
    bias_copy.start()

    def kv_copy(head, half, stage):
        aim = core * 2 + head
        own = aim == y
        sp = jnp.where(own, me, z * NY + aim)
        tp = jnp.where(own, sibling, place * 2 + half)
        return pltpu.make_async_remote_copy(
            src_ref=kv_own.at[head, half, pl.ds(LANES * (1 - stage), LANES)],
            dst_ref=kv_all.at[me, half, pl.ds(LANES * (1 - stage), LANES)],
            send_sem=kv_send.at[head, half, stage], recv_sem=kv_recv.at[me, half],
            device_id=(sp, tp), device_id_type=MESH,
        )

    def ring_copy(block, way):
        peer = lax.rem(z + (1 if way == 0 else NZ - 1), NZ) * NY + y
        return pltpu.make_async_remote_copy(
            src_ref=kv_all.at[block, core], dst_ref=kv_all.at[block, core],
            send_sem=ring_send.at[block, way], recv_sem=kv_recv.at[block, core],
            device_id=(peer, col), device_id_type=MESH,
        )

    def share_copy(block):
        return pltpu.make_async_remote_copy(
            src_ref=kv_all.at[block, core], dst_ref=kv_all.at[block, core],
            send_sem=share_send.at[block], recv_sem=kv_recv.at[block, core],
            device_id=(me, sibling), device_id_type=MESH,
        )

    def rows_of(to_z, to_core, block):
        return lax.rem(2 * to_z + to_core + 2 * block, SHARES)

    def q_copy(head, step):
        to_z, to_core = step // 2, lax.rem(step, 2)
        return pltpu.make_async_remote_copy(
            src_ref=q_own.at[head, rows_of(to_z, to_core, me)], dst_ref=q_all.at[me],
            send_sem=q_send.at[head, step], recv_sem=q_recv.at[me],
            device_id=(to_z * NY + core * 2 + head, place * 2 + to_core), device_id_type=MESH,
        )

    def q_here(head, step):
        to_z, to_core = step // 2, lax.rem(step, 2)
        return jnp.logical_and(to_z * NY + core * 2 + head == me, to_core == core)

    def back_owner(block):
        return lax.rem(z + block, n_tp)

    my_slot = (place * NY + y) * 2 + core

    def back_here(block):
        return jnp.logical_and(block == me, back_owner(block) == col)

    def back_copy(block):
        return pltpu.make_async_remote_copy(
            src_ref=packed.at[block], dst_ref=att.at[my_slot],
            send_sem=back_send.at[block], recv_sem=back_recv.at[my_slot],
            device_id=(block, back_owner(block)), device_id_type=MESH,
        )

    for copy in loads:
        copy.wait()
    def turn(value):
        return pltpu.roll(value, DIM, 1)

    lane16 = lax.broadcasted_iota(jnp.int32, (16, LANES), 1)

    def weave(upper, lower):
        first = jnp.where(lane16 < DIM, upper, turn(lower)).astype(BF16)
        second = jnp.where(lane16 < DIM, turn(upper), lower).astype(BF16)
        return first, second

    def strided(i, kind):
        return proj[:, RUN - 1 - i, kind * LANES : (kind + 1) * LANES]

    for part in range(PARTS):
        relay(token_copy, tok, tok_recv, part, 3)
        relay(token_copy, tok, tok_recv, turned[part], 1)
    for stage in range(2):
        parts = (stage, stage + 2)
        for part in parts:
            relay(token_copy, tok, tok_recv, part, 2)
        for part in parts:
            arrived(tok.at[sibling, part], tok_recv.at[sibling, part])
            for k in range(1, places):
                block = lax.rem(place + k, places) * 2 + 1 - core
                arrived(tok.at[block, part], tok_recv.at[block, part])
        depth, model = tok.shape[2:]
        x = jnp.concatenate([tok[:, part].reshape(n_tp * depth, model) for part in parts], axis=0)
        both = jnp.dot(x, wqkv[...], preferred_element_type=F32)
        for index, part in enumerate(parts):
            proj[:, part * depth : (part + 1) * depth, :] = both[
                index * n_tp * depth : (index + 1) * n_tp * depth
            ].reshape(n_tp, depth, 3 * LANES)
        base = 16 * (1 - stage)
        for i in range(base, base + 16, 2):
            upper = jnp.concatenate([strided(i, 1), strided(i + 1, 1)], axis=0)
            lower = jnp.concatenate([strided(i + 32, 1), strided(i + 33, 1)], axis=0)
            kv_own[0, 0, 8 * i : 8 * i + 16], kv_own[1, 0, 8 * i : 8 * i + 16] = weave(
                upper, lower
            )
        for head in range(2):
            kv_copy(head, 0, stage).start()
        for index in range(2):
            first = base + 32 * index
            block = jnp.concatenate([strided(first + i, 2) for i in range(16)], axis=0)
            flipped = block.T.astype(BF16)
            at = LANES * (1 - stage) + DIM * index
            for head in range(2):
                kv_own[head, 1, at : at + DIM] = flipped[DIM * head : DIM * (head + 1)]
        for head in range(2):
            kv_copy(head, 1, stage).start()

    for part in range(PARTS):
        for kind in (1, 3, 0):
            wo_copy(kind, turned[part] if kind == 3 else part).start()

    for share in range(SHARES):
        block, first = share // 2, 32 * (share % 2)
        q = proj[block, first : first + 32, 0:LANES] * (LOG2E * DIM ** (-0.5))
        q_own[0, share], q_own[1, share] = weave(q[:16], q[16:])

    pl.semaphore_wait(plane_sem, NZ - 1)

    def send_q(step, carry):
        for head in range(2):

            @pl.when(jnp.logical_not(q_here(head, step)))
            def _():
                q_copy(head, step).start()

        return carry

    lax.fori_loop(0, 2 * NZ, send_q, 0)

    for head in range(2):

        @pl.when(core * 2 + head == y)
        def _():
            kv_all[me] = kv_own[head]
            q_all[me] = q_own[head, rows_of(z, core, me)]

    for part in range(NY):
        block = z * NY + part

        @pl.when(jnp.logical_not(jnp.logical_and(block == me, mine)))
        def _():
            arrived(kv_all.at[block, core], kv_recv.at[block, core])

        for way in range(2):
            ring_copy(block, way).start()

        @pl.when(block != me)
        def _():
            share_copy(block).start()

    def take_q(block, carry):
        @pl.when(jnp.logical_not(jnp.logical_and(block == me, mine)))
        def _():
            arrived(q_all.at[block], q_recv.at[block])

        return carry

    lax.fori_loop(0, n_sp, take_q, 0)

    def build(tile, carry):
        pieces = []
        for part in range(NY):
            pair = q_all[tile * NY + part].astype(F32)
            pieces.append(jnp.where(lane16 < DIM, pair, 0.0))
            pieces.append(jnp.where(lane16 < DIM, turn(pair), 0.0))
        flipped = jnp.concatenate(pieces, axis=0).T
        q_top[tile] = flipped.astype(BF16)
        q_low[tile] = jnp.concatenate([flipped[DIM:], flipped[:DIM]], axis=0).astype(BF16)
        return carry

    lax.fori_loop(0, TILES, build, 0)
    arrived(bias_all.at[1 - core], bias_recv)

    def suffix(keep):
        row = lax.broadcasted_iota(jnp.int32, keep.shape, 0)
        product = keep
        for step in (1, 2, 4):
            moved = pltpu.roll(product, 8 - step, 0)
            product = product * jnp.where(row + step < 8, moved, 1.0)
        after = jnp.where(row + 1 < 8, pltpu.roll(product, 7, 0), 1.0)
        return after, product[0:1]

    def segment(block, slot, width, bias, reach):
        keep = jnp.ones((8, 2 * width), F32)
        for i in range(RUN // 2):
            score = raw[slot, 8 * i : 8 * i + 8, 0 : 2 * width] + bias
            if reach is not None:
                score = jnp.where(reach > -i, score, DEAD)
            odds = jnp.exp2(jnp.minimum(score, EXP_MAX))
            lose = 1.0 / (1.0 + odds)
            xs[slot, 8 * i : 8 * i + 8, 0 : 2 * width] = odds * lose * keep
            keep = keep * lose
        near, far = keep[:, :width], keep[:, width:]
        after, whole = suffix(near * far)
        values = kv_all[block, 1]
        out = None
        for half, factor in enumerate((after, after * near)):
            part = xs[slot, :, half * width : (half + 1) * width].reshape(RUN // 2, 8, width)
            weight = (part * factor[None]).reshape(HALF, width).astype(BF16)
            first = half * DIM
            value = jnp.concatenate(
                [values[first : first + DIM], values[LANES + first : LANES + first + DIM]], axis=1
            )
            term = jnp.dot(value, weight, preferred_element_type=F32)
            out = term if out is None else out + term
        return out, whole

    def cover(group, part, tile, count, diagonal):
        width = count * LANES
        q = jnp.concatenate(
            [q_top[tile + n] for n in range(count)] + [q_low[tile + n] for n in range(count)],
            axis=1,
        )
        bias = bias_all[head_core, head_local]
        bias = jnp.concatenate([bias] * (2 * count), axis=1)
        if diagonal:
            lane = lax.broadcasted_iota(jnp.int32, (8, 2 * width), 1)
            row = lax.broadcasted_iota(jnp.int32, (8, 2 * width), 0)
            half = lane // width
            inside = lax.rem(lane, width)
            owner = lax.rem(inside // SHARE, NY)
            share = rows_of(z, core, tile * NY + owner)
            query = SEG * owner + SHARE * share + lax.rem(inside, SHARE)
            query = jnp.where(inside < LANES, query, FAR)
            reach = query - row * RUN - (RUN - 1) + half * (RUN // 2) - SEG * part
        first = group * NY + part
        raw[:, :, 0 : 2 * width] = jnp.dot(
            kv_all[pl.ds(first, BATCH), 0].reshape(BATCH * HALF, LANES), q,
            preferred_element_type=F32,
        ).reshape(BATCH, HALF, 2 * width)
        acc = [seg_acc[group, tile + n] for n in range(count)]
        keep = [seg_keep[group, tile + n][0:1] for n in range(count)]
        for index in range(BATCH):
            limit = reach - SEG * index if diagonal else None
            out, whole = segment(first + index, index, width, bias, limit)
            for n in range(count):
                lanes = slice(n * LANES, (n + 1) * LANES)
                acc[n] = acc[n] * whole[:, lanes] + out[:, lanes]
                keep[n] = keep[n] * whole[:, lanes]
        for n in range(count):
            seg_acc[group, tile + n] = acc[n]
            seg_keep[group, tile + n] = jnp.broadcast_to(keep[n], (8, LANES))

    def attend(group, part):
        count = TILES - group
        odd = lax.rem(count, 2)

        @pl.when(odd == 1)
        def _():
            cover(group, part, group, 1, True)

        @pl.when(odd == 0)
        def _():
            cover(group, part, group, 2, True)

        def pair(step, carry):
            cover(group, part, group + 2 - odd + 2 * step, 2, False)
            return carry

        lax.fori_loop(0, (count - 1) // 2, pair, 0)

    def stop_at(step):
        turn_of = lax.rem(step + 2, 4)
        far = step >= STEPS - 2
        distance = (step + 2) // 4
        own = step < 2
        behind = jnp.logical_or(jnp.logical_and(far, turn_of == 0), lax.rem(step, 2) == 0)
        part = jnp.where(jnp.logical_or(own, far), lax.rem(step, 2), turn_of // 2) * BATCH
        group = lax.rem(z + NZ + jnp.where(behind, -distance, distance), NZ)
        return distance, behind, group, part

    def visit(step, carry):
        ahead = step + 1

        @pl.when(jnp.logical_and(ahead >= 2, ahead < STEPS))
        def _():
            distance, behind, group, part = stop_at(ahead)
            for index in range(BATCH):
                block = group * NY + part + index
                arrived(kv_all.at[block, core], kv_recv.at[block, core])

                @pl.when(
                    jnp.logical_and(
                        behind, jnp.logical_or(distance < 3, jnp.logical_and(distance == 3, part == 0))
                    )
                )
                def _():
                    ring_copy(block, 0).start()

                @pl.when(
                    jnp.logical_and(
                        jnp.logical_not(behind),
                        jnp.logical_or(distance < 3, jnp.logical_and(distance == 3, part > 0)),
                    )
                )
                def _():
                    ring_copy(block, 1).start()

                share_copy(block).start()

        @pl.when(step == STEPS // 2)
        def _():
            for part in range(PARTS):
                relay(wo_copy, wfull, wo_recv, part, 3)
                relay(wo_copy, wfull, wo_recv, turned[part], 1)

        @pl.when(step == STEPS - 2)
        def _():
            for part in range(PARTS):
                relay(wo_copy, wfull, wo_recv, part, 2)

        distance, behind, group, part = stop_at(step)
        for index in range(BATCH):
            block = group * NY + part + index

            @pl.when(jnp.logical_not(jnp.logical_and(block == me, mine)))
            def _():
                arrived(kv_all.at[block, 1 - core], kv_recv.at[block, 1 - core])

        attend(group, part)
        return carry

    lax.fori_loop(0, STEPS, visit, 0)

    def combine(tile):
        acc = seg_acc[0, tile]
        for group in range(1, NZ):
            acc = acc * seg_keep[group, tile][0:1] + seg_acc[group, tile]
        return acc

    def deliver(pair, carry):
        flipped = jnp.concatenate([combine(2 * pair), combine(2 * pair + 1)], axis=0).T
        for part in range(NY):
            upper = flipped[SHARE * part : SHARE * part + 16]
            lower = flipped[SHARE * part + 16 : SHARE * (part + 1)]
            for n, folded in enumerate(weave(upper, lower)):
                block = (2 * pair + n) * NY + part
                packed[block] = folded
                here = back_here(block)

                @pl.when(here)
                def _():
                    att[my_slot] = folded

                @pl.when(jnp.logical_not(here))
                def _():
                    back_copy(block).start()

        return carry

    lax.fori_loop(0, TILES // 2, deliver, 0)

    bias_copy.wait_send()
    for part in range(PARTS):
        for kind in range(2 * places - 1):
            wo_copy(kind, part).wait_send()
            token_copy(kind, part).wait_send()
    for head in range(2):
        for half in range(2):
            for stage in range(2):
                kv_copy(head, half, stage).wait_send()

    def drain_q(step, carry):
        for head in range(2):

            @pl.when(jnp.logical_not(q_here(head, step)))
            def _():
                q_copy(head, step).wait_send()

        return carry

    lax.fori_loop(0, 2 * NZ, drain_q, 0)

    def drain(block, carry):
        ahead = lax.rem(z - block // NY + NZ, NZ)
        behind = lax.rem(NZ - ahead, NZ)
        first = lax.rem(block, NY) < NY // 2

        @pl.when(jnp.logical_or(ahead < 3, jnp.logical_and(ahead == 3, first)))
        def _():
            ring_copy(block, 0).wait_send()

        @pl.when(
            jnp.logical_or(behind < 3, jnp.logical_and(behind == 3, jnp.logical_not(first)))
        )
        def _():
            ring_copy(block, 1).wait_send()

        @pl.when(block != me)
        def _():
            share_copy(block).wait_send()

        return carry

    lax.fori_loop(0, n_sp, drain, 0)

    source_z = lax.rem(col + n_sp - me, NZ)
    for pair in range(n_tp):
        for sub in range(2):
            values = []
            for head in (2 * pair, 2 * pair + 1):
                slot = head * 2 + sub
                here = jnp.logical_and(source_z * NY + head % NY == me, 2 * (head // NY) + sub == col)

                @pl.when(jnp.logical_not(here))
                def _():
                    arrived(att.at[slot], back_recv.at[slot])

                values.append(att[slot].astype(F32))
            top = jnp.where(lane16 < DIM, values[0], turn(values[1]))
            low = jnp.where(lane16 < DIM, turn(values[0]), values[1])
            cols = slice(pair * LANES, (pair + 1) * LANES)
            att_rows[SHARE * sub : SHARE * sub + 16, cols] = top.astype(BF16)
            att_rows[SHARE * sub + 16 : SHARE * (sub + 1), cols] = low.astype(BF16)

    for part in range(PARTS):
        arrived(wfull.at[sibling, part], wo_recv.at[sibling, part])
        for k in range(1, places):
            block = lax.rem(place + k, places) * 2 + 1 - core
            arrived(wfull.at[block, part], wo_recv.at[block, part])
    for first in range(0, out_ref.shape[1], COLS):
        w = wfull[:, :, :, first : first + COLS].reshape(att_rows.shape[1], COLS)
        out_ref[:, first : first + COLS] = jnp.dot(
            att_rows[...], w, preferred_element_type=F32
        ).astype(BF16)

    def drain_back(block, carry):
        @pl.when(jnp.logical_not(back_here(block)))
        def _():
            back_copy(block).wait_send()

        return carry

    lax.fori_loop(0, n_sp, drain_back, 0)


def shards(tokens, w_query, w_key, w_value, head_bias, w_out):
    model, local_width = w_query.shape
    n_tp = lax.axis_size("tp")
    n_sp = lax.axis_size("sp")
    device_rows = tokens.shape[0]
    out_width = w_out.shape[1]
    kinds = n_tp - 1

    smem = pl.BlockSpec(memory_space=pltpu.SMEM)
    anywhere = pl.BlockSpec(memory_space=pl.ANY)
    dma = pltpu.SemaphoreType.DMA

    def vmem(*shape):
        return pltpu.VMEM(shape, BF16)

    return pl.pallas_call(
        layer_kernel,
        out_shape=jax.ShapeDtypeStruct((device_rows, out_width), BF16),
        in_specs=[smem] + [anywhere] * 5,
        out_specs=pl.BlockSpec(memory_space=pltpu.VMEM),
        scratch_shapes=[
            vmem(n_tp, PARTS, device_rows // PARTS, model),
            vmem(model, 3 * local_width),
            vmem(n_tp, PARTS, local_width // PARTS, out_width),
            pltpu.VMEM((n_tp, device_rows, 3 * local_width), F32),
            pltpu.VMEM((2, 2, 8, LANES), F32),
            vmem(2, 2, HALF, LANES),
            vmem(2, SHARES, SHARE // 2, LANES),
            vmem(n_sp, SHARE // 2, LANES),
            vmem(n_sp, 2, HALF, LANES),
            vmem(TILES, LANES, LANES),
            vmem(TILES, LANES, LANES),
            pltpu.VMEM((BATCH, HALF, 4 * LANES), F32),
            pltpu.VMEM((BATCH, HALF, 4 * LANES), F32),
            pltpu.VMEM((NZ, TILES, DIM, LANES), F32),
            pltpu.VMEM((NZ, TILES, 8, LANES), F32),
            vmem(n_sp, SHARE // 2, LANES),
            vmem(32, SHARE // 2, LANES),
            vmem(device_rows, n_tp * local_width),
            pltpu.SemaphoreType.REGULAR,
            dma((5,)),
            dma((kinds, PARTS)),
            dma((n_tp, PARTS)),
            dma((kinds, PARTS)),
            dma((n_tp, PARTS)),
            dma,
            dma,
            dma((2, 2, 2)),
            dma((n_sp, 2)),
            dma((n_sp, 2)),
            dma((n_sp,)),
            dma((2, 2 * NZ)),
            dma((n_sp,)),
            dma((n_sp,)),
            dma((32,)),
        ],
        compiler_params=pltpu.CompilerParams(
            collective_id=0, has_side_effects=True, vmem_limit_bytes=60 * 2**20
        ),
        name="layer",
    )(
        head_bias,
        tokens.reshape(PARTS, device_rows // PARTS, model),
        w_query, w_key, w_value,
        w_out.reshape(PARTS, local_width // PARTS, out_width),
    )


def solution(mesh):
    placed = (
        P(("sp", "tp"), None),
        P(None, "tp"),
        P(None, "tp"),
        P(None, "tp"),
        P("tp"),
        P("tp", None),
    )
    return jax.shard_map(
        shards, mesh=mesh, in_specs=placed, out_specs=P(("sp", "tp"), None), check_vma=False
    )
```

```python
import functools
import math

import jax
import jax.numpy as jnp
from jax import lax
from jax.experimental import pallas as pl
from jax.experimental.pallas import tpu as pltpu
from jax.sharding import PartitionSpec as P

MESH = pl.DeviceIdType.MESH
F32, BF16 = jnp.float32, jnp.bfloat16
LOG2E = math.log2(math.e)
PARTS = 4
COLS = 512
EXP_MAX = 126.0
DEAD = -1e30
NZ, NY = 8, 4
SEG = 512
HALF = 256
LANES = 128
DIM = 64
RUN = 64
SHARE = 32
SHARES = SEG // SHARE
TILES = 8
FAR = 1 << 20
BATCH = 2
STEPS = NZ * NY // BATCH


def layer_kernel(
    bias_ref, tokens_ref, wq_ref, wk_ref, wv_ref, wo_ref, out_ref,
    tok, wqkv, wfull, proj, bias_all, kv_own, q_own, q_all, kv_all, q_top, q_low, raw, xs,
    seg_acc, seg_keep, packed, att, att_rows, mixed,
    plane_sem, out_sem, load_sem, tok_send, tok_recv, wo_send, wo_recv, bias_send, bias_recv, kv_send, kv_recv,
    ring_send, share_send, q_send, q_recv, back_send, back_recv,
):
    me = lax.axis_index("sp")
    col = lax.axis_index("tp")
    n_sp, n_tp = NZ * NY, 8
    z, y = me // NY, lax.rem(me, NY)
    place, core = col // 2, lax.rem(col, 2)
    places = n_tp // 2
    sibling = place * 2 + 1 - core
    head_core, head_local = y // 2, lax.rem(y, 2)
    mine = core == head_core

    loads = [
        pltpu.make_async_copy(src, dst, load_sem.at[index])
        for index, (src, dst) in enumerate(
            [
                (tokens_ref, tok.at[col]),
                (wq_ref, wqkv.at[:, 0:LANES]),
                (wk_ref, wqkv.at[:, LANES : 2 * LANES]),
                (wv_ref, wqkv.at[:, 2 * LANES : 3 * LANES]),
                (wo_ref, wfull.at[col]),
            ]
        )
    ]
    for copy in loads:
        copy.start()

    barrier = pltpu.get_barrier_semaphore()
    for step in range(1, n_tp):
        pl.semaphore_signal(
            barrier, inc=1, device_id=(me, lax.rem(col + step, n_tp)), device_id_type=MESH
        )
    for step in range(1, NY):
        peer = z * NY + lax.rem(y + step, NY)
        for other in range(2):
            pl.semaphore_signal(
                barrier, inc=1, device_id=(peer, place * 2 + other), device_id_type=MESH
            )
    for step in range(1, NZ):
        peer = lax.rem(z + step, NZ) * NY + y
        pl.semaphore_signal(barrier, inc=1, device_id=(peer, col), device_id_type=MESH)
    for head in range(2):
        bias_all[core, head] = jnp.full((8, LANES), bias_ref[head] * LOG2E, F32)
    seg_acc[...] = jnp.zeros_like(seg_acc)
    seg_keep[...] = jnp.ones_like(seg_keep)
    pl.semaphore_wait(barrier, n_tp - 1 + 2 * (NY - 1) + NZ - 1)
    for step in range(1, NZ):
        peer = lax.rem(z + step, NZ) * NY + y
        pl.semaphore_signal(plane_sem, inc=1, device_id=(peer, col), device_id_type=MESH)

    def same_core(k):
        return lax.rem(place + k, places) * 2 + core

    def arrived(ref, sem):
        pltpu.make_async_copy(ref, ref, sem).wait()

    def link(kind, own, kept, sent, received, part):
        if kind == 2:
            ahead = part < PARTS // 2
            block = same_core(3 if ahead else 1)
            src, target = kept.at[block, part], same_core(1 if ahead else 3)
        elif kind < places:
            src, block = own.at[part], col
            target = sibling if kind == 0 else same_core(kind)
        else:
            block = same_core(kind - places + 1)
            src, target = kept.at[block, part], sibling
        return pltpu.make_async_remote_copy(
            src_ref=src, dst_ref=kept.at[block, part],
            send_sem=sent.at[kind, part], recv_sem=received.at[block, part],
            device_id=(me, target), device_id_type=MESH,
        )

    def token_copy(kind, part):
        return link(kind, tokens_ref, tok, tok_send, tok_recv, part)

    def wo_copy(kind, part):
        return link(kind, wo_ref, wfull, wo_send, wo_recv, part)

    def relay(copy, kept, received, part, k):
        block = same_core(k)
        arrived(kept.at[block, part], received.at[block, part])
        copy(places + k - 1, part).start()
        if k != 2 and (part < PARTS // 2) == (k == 3):
            copy(2, part).start()

    bias_copy = pltpu.make_async_remote_copy(
        src_ref=bias_all.at[core], dst_ref=bias_all.at[core],
        send_sem=bias_send, recv_sem=bias_recv, device_id=(me, sibling), device_id_type=MESH,
    )

    turned = (2, 3, 0, 1)
    for part in range(PARTS // 2):
        token_copy(1, part).start()
        token_copy(3, turned[part]).start()
    for part in (0, 2, 1, 3):
        token_copy(0, part).start()
    bias_copy.start()

    def kv_copy(head, half, stage):
        aim = core * 2 + head
        own = aim == y
        sp = jnp.where(own, me, z * NY + aim)
        tp = jnp.where(own, sibling, place * 2 + half)
        return pltpu.make_async_remote_copy(
            src_ref=kv_own.at[head, half, pl.ds(LANES * (1 - stage), LANES)],
            dst_ref=kv_all.at[me, half, pl.ds(LANES * (1 - stage), LANES)],
            send_sem=kv_send.at[head, half, stage], recv_sem=kv_recv.at[me, half],
            device_id=(sp, tp), device_id_type=MESH,
        )

    def ring_copy(block, way):
        peer = lax.rem(z + (1 if way == 0 else NZ - 1), NZ) * NY + y
        return pltpu.make_async_remote_copy(
            src_ref=kv_all.at[block, core], dst_ref=kv_all.at[block, core],
            send_sem=ring_send.at[block, way], recv_sem=kv_recv.at[block, core],
            device_id=(peer, col), device_id_type=MESH,
        )

    def share_copy(block):
        return pltpu.make_async_remote_copy(
            src_ref=kv_all.at[block, core], dst_ref=kv_all.at[block, core],
            send_sem=share_send.at[block], recv_sem=kv_recv.at[block, core],
            device_id=(me, sibling), device_id_type=MESH,
        )

    def rows_of(to_z, to_core, block):
        return lax.rem(2 * to_z + to_core + 2 * block, SHARES)

    def q_copy(head, step):
        to_z, to_core = step // 2, lax.rem(step, 2)
        return pltpu.make_async_remote_copy(
            src_ref=q_own.at[head, rows_of(to_z, to_core, me)], dst_ref=q_all.at[me],
            send_sem=q_send.at[head, step], recv_sem=q_recv.at[me],
            device_id=(to_z * NY + core * 2 + head, place * 2 + to_core), device_id_type=MESH,
        )

    def q_here(head, step):
        to_z, to_core = step // 2, lax.rem(step, 2)
        return jnp.logical_and(to_z * NY + core * 2 + head == me, to_core == core)

    def back_owner(block):
        return lax.rem(z + block, n_tp)

    my_slot = (place * NY + y) * 2 + core

    def back_here(block):
        return jnp.logical_and(block == me, back_owner(block) == col)

    def back_copy(block):
        return pltpu.make_async_remote_copy(
            src_ref=packed.at[block], dst_ref=att.at[my_slot],
            send_sem=back_send.at[block], recv_sem=back_recv.at[my_slot],
            device_id=(block, back_owner(block)), device_id_type=MESH,
        )

    for copy in loads:
        copy.wait()
    def turn(value):
        return pltpu.roll(value, DIM, 1)

    lane16 = lax.broadcasted_iota(jnp.int32, (16, LANES), 1)

    def weave(upper, lower):
        first = jnp.where(lane16 < DIM, upper, turn(lower)).astype(BF16)
        second = jnp.where(lane16 < DIM, turn(upper), lower).astype(BF16)
        return first, second

    def strided(i, kind):
        return proj[:, RUN - 1 - i, kind * LANES : (kind + 1) * LANES]

    def send_q(step, carry):
        for head in range(2):

            @pl.when(jnp.logical_not(q_here(head, step)))
            def _():
                q_copy(head, step).start()

        return carry

    for part in range(PARTS // 2):
        relay(token_copy, tok, tok_recv, part, 3)
        token_copy(1, part + 2).start()
        relay(token_copy, tok, tok_recv, turned[part], 1)
        token_copy(3, turned[part + 2]).start()
    for stage in range(2):
        parts = (stage, stage + 2)
        relay(token_copy, tok, tok_recv, stage + 2, 3)
        relay(token_copy, tok, tok_recv, turned[stage + 2], 1)
        for part in parts:
            relay(token_copy, tok, tok_recv, part, 2)
        for part in parts:
            arrived(tok.at[sibling, part], tok_recv.at[sibling, part])
            for k in range(1, places):
                block = lax.rem(place + k, places) * 2 + 1 - core
                arrived(tok.at[block, part], tok_recv.at[block, part])
        depth, model = tok.shape[2:]
        x = jnp.concatenate([tok[:, part].reshape(n_tp * depth, model) for part in parts], axis=0)
        both = jnp.dot(x, wqkv[...], preferred_element_type=F32)
        for index, part in enumerate(parts):
            proj[:, part * depth : (part + 1) * depth, :] = both[
                index * n_tp * depth : (index + 1) * n_tp * depth
            ].reshape(n_tp, depth, 3 * LANES)
        if stage == 1:
            for share in range(SHARES):
                block, first = share // 2, 32 * (share % 2)
                q = proj[block, first : first + 32, 0:LANES] * (LOG2E * DIM ** (-0.5))
                q_own[0, share], q_own[1, share] = weave(q[:16], q[16:])
            pl.semaphore_wait(plane_sem, NZ - 1)
            lax.fori_loop(0, 2 * NZ, send_q, 0)
        base = 16 * (1 - stage)
        for i in range(base, base + 16, 2):
            upper = jnp.concatenate([strided(i, 1), strided(i + 1, 1)], axis=0)
            lower = jnp.concatenate([strided(i + 32, 1), strided(i + 33, 1)], axis=0)
            kv_own[0, 0, 8 * i : 8 * i + 16], kv_own[1, 0, 8 * i : 8 * i + 16] = weave(
                upper, lower
            )
        for head in range(2):
            kv_copy(head, 0, stage).start()
        for index in range(2):
            first = base + 32 * index
            block = jnp.concatenate([strided(first + i, 2) for i in range(16)], axis=0)
            flipped = block.T.astype(BF16)
            at = LANES * (1 - stage) + DIM * index
            for head in range(2):
                kv_own[head, 1, at : at + DIM] = flipped[DIM * head : DIM * (head + 1)]
        for head in range(2):
            kv_copy(head, 1, stage).start()

    for part in range(PARTS):
        for kind in (1, 3, 0):
            wo_copy(kind, turned[part] if kind == 3 else part).start()

    for head in range(2):

        @pl.when(core * 2 + head == y)
        def _():
            kv_all[me] = kv_own[head]
            q_all[me] = q_own[head, rows_of(z, core, me)]

    for part in range(NY):
        block = z * NY + part

        @pl.when(jnp.logical_not(jnp.logical_and(block == me, mine)))
        def _():
            arrived(kv_all.at[block, core], kv_recv.at[block, core])

        for way in range(2):
            ring_copy(block, way).start()

        @pl.when(block != me)
        def _():
            share_copy(block).start()

    def take_q(block, carry):
        @pl.when(jnp.logical_not(jnp.logical_and(block == me, mine)))
        def _():
            arrived(q_all.at[block], q_recv.at[block])

        return carry

    lax.fori_loop(0, n_sp, take_q, 0)

    def build(tile, carry):
        pieces = []
        for part in range(NY):
            pair = q_all[tile * NY + part].astype(F32)
            pieces.append(jnp.where(lane16 < DIM, pair, 0.0))
            pieces.append(jnp.where(lane16 < DIM, turn(pair), 0.0))
        flipped = jnp.concatenate(pieces, axis=0).T
        q_top[tile] = flipped.astype(BF16)
        q_low[tile] = jnp.concatenate([flipped[DIM:], flipped[:DIM]], axis=0).astype(BF16)
        return carry

    lax.fori_loop(0, TILES, build, 0)
    arrived(bias_all.at[1 - core], bias_recv)

    def suffix(keep):
        row = lax.broadcasted_iota(jnp.int32, keep.shape, 0)
        product = keep
        for step in (1, 2, 4):
            moved = pltpu.roll(product, 8 - step, 0)
            product = product * jnp.where(row + step < 8, moved, 1.0)
        after = jnp.where(row + 1 < 8, pltpu.roll(product, 7, 0), 1.0)
        return after, product[0:1]

    def segment(block, bank, slot, width, bias, reach):
        keep = jnp.ones((8, 2 * width), F32)
        for i in range(RUN // 2):
            score = raw[bank, slot, 8 * i : 8 * i + 8, 0 : 2 * width] + bias
            if reach is not None:
                score = jnp.where(reach > -i, score, DEAD)
            odds = jnp.exp2(jnp.minimum(score, EXP_MAX))
            lose = 1.0 / (1.0 + odds)
            xs[bank, slot, 8 * i : 8 * i + 8, 0 : 2 * width] = odds * lose * keep
            keep = keep * lose
        near, far = keep[:, :width], keep[:, width:]
        after, whole = suffix(near * far)
        values = kv_all[block, 1]
        out = None
        for half, factor in enumerate((after, after * near)):
            part = xs[bank, slot, :, half * width : (half + 1) * width].reshape(RUN // 2, 8, width)
            weight = (part * factor[None]).reshape(HALF, width).astype(BF16)
            first = half * DIM
            value = jnp.concatenate(
                [values[first : first + DIM], values[LANES + first : LANES + first + DIM]], axis=1
            )
            term = jnp.dot(value, weight, preferred_element_type=F32)
            out = term if out is None else out + term
        return out, whole

    def cover(group, part, tile, count, diagonal, bank):
        width = count * LANES
        q = jnp.concatenate(
            [q_top[tile + n] for n in range(count)] + [q_low[tile + n] for n in range(count)],
            axis=1,
        )
        bias = bias_all[head_core, head_local]
        bias = jnp.concatenate([bias] * (2 * count), axis=1)
        if diagonal:
            lane = lax.broadcasted_iota(jnp.int32, (8, 2 * width), 1)
            row = lax.broadcasted_iota(jnp.int32, (8, 2 * width), 0)
            half = lane // width
            inside = lax.rem(lane, width)
            owner = lax.rem(inside // SHARE, NY)
            share = rows_of(z, core, tile * NY + owner)
            query = SEG * owner + SHARE * share + lax.rem(inside, SHARE)
            query = jnp.where(inside < LANES, query, FAR)
            reach = query - row * RUN - (RUN - 1) + half * (RUN // 2) - SEG * part
        first = group * NY + part
        raw[bank, :, :, 0 : 2 * width] = jnp.dot(
            kv_all[pl.ds(first, BATCH), 0].reshape(BATCH * HALF, LANES), q,
            preferred_element_type=F32,
        ).reshape(BATCH, HALF, 2 * width)
        acc = [seg_acc[group, tile + n] for n in range(count)]
        keep = [seg_keep[group, tile + n][0:1] for n in range(count)]
        for index in range(BATCH):
            limit = reach - SEG * index if diagonal else None
            out, whole = segment(first + index, bank, index, width, bias, limit)
            for n in range(count):
                lanes = slice(n * LANES, (n + 1) * LANES)
                acc[n] = acc[n] * whole[:, lanes] + out[:, lanes]
                keep[n] = keep[n] * whole[:, lanes]
        for n in range(count):
            seg_acc[group, tile + n] = acc[n]
            seg_keep[group, tile + n] = jnp.broadcast_to(keep[n], (8, LANES))

    def attend(group, part):
        count = TILES - group
        odd = lax.rem(count, 2)
        pairs = (count - 1) // 2
        first = group + 2 - odd

        for single in range(2):
            for more in range(2):

                @pl.when(jnp.logical_and(odd == single, (pairs > 0) == (more == 1)))
                def _():
                    cover(group, part, group, 2 - single, True, 0)
                    if more:
                        cover(group, part, first, 2, False, 1)

        @pl.when(pairs == 2)
        def _():
            cover(group, part, first + 2, 2, False, 0)

        @pl.when(pairs == 3)
        def _():
            cover(group, part, first + 2, 2, False, 0)
            cover(group, part, first + 4, 2, False, 1)

    def stop_at(step):
        turn_of = lax.rem(step + 2, 4)
        far = step >= STEPS - 2
        distance = (step + 2) // 4
        own = step < 2
        behind = jnp.logical_or(jnp.logical_and(far, turn_of == 0), lax.rem(step, 2) == 0)
        part = jnp.where(jnp.logical_or(own, far), lax.rem(step, 2), turn_of // 2) * BATCH
        group = lax.rem(z + NZ + jnp.where(behind, -distance, distance), NZ)
        return distance, behind, group, part

    def visit(step, carry):
        ahead = step + 1

        @pl.when(jnp.logical_and(ahead >= 2, ahead < STEPS))
        def _():
            distance, behind, group, part = stop_at(ahead)
            for index in range(BATCH):
                block = group * NY + part + index
                arrived(kv_all.at[block, core], kv_recv.at[block, core])

                @pl.when(
                    jnp.logical_and(
                        behind, jnp.logical_or(distance < 3, jnp.logical_and(distance == 3, part == 0))
                    )
                )
                def _():
                    ring_copy(block, 0).start()

                @pl.when(
                    jnp.logical_and(
                        jnp.logical_not(behind),
                        jnp.logical_or(distance < 3, jnp.logical_and(distance == 3, part > 0)),
                    )
                )
                def _():
                    ring_copy(block, 1).start()

                share_copy(block).start()

        @pl.when(step == STEPS // 2)
        def _():
            for part in range(PARTS):
                relay(wo_copy, wfull, wo_recv, part, 3)
                relay(wo_copy, wfull, wo_recv, turned[part], 1)

        @pl.when(step == STEPS - 2)
        def _():
            for part in range(PARTS):
                relay(wo_copy, wfull, wo_recv, part, 2)

        distance, behind, group, part = stop_at(step)
        for index in range(BATCH):
            block = group * NY + part + index

            @pl.when(jnp.logical_not(jnp.logical_and(block == me, mine)))
            def _():
                arrived(kv_all.at[block, 1 - core], kv_recv.at[block, 1 - core])

        attend(group, part)
        return carry

    lax.fori_loop(0, STEPS, visit, 0)

    def combine(tile):
        acc = seg_acc[0, tile]
        for group in range(1, NZ):
            acc = acc * seg_keep[group, tile][0:1] + seg_acc[group, tile]
        return acc

    def deliver(pair, carry):
        flipped = jnp.concatenate([combine(2 * pair), combine(2 * pair + 1)], axis=0).T
        for part in range(NY):
            upper = flipped[SHARE * part : SHARE * part + 16]
            lower = flipped[SHARE * part + 16 : SHARE * (part + 1)]
            for n, folded in enumerate(weave(upper, lower)):
                block = (2 * pair + n) * NY + part
                packed[block] = folded
                here = back_here(block)

                @pl.when(here)
                def _():
                    att[my_slot] = folded

                @pl.when(jnp.logical_not(here))
                def _():
                    back_copy(block).start()

        return carry

    lax.fori_loop(0, TILES // 2, deliver, 0)

    bias_copy.wait_send()
    for part in range(PARTS):
        for kind in range(2 * places - 1):
            wo_copy(kind, part).wait_send()
            token_copy(kind, part).wait_send()
    for head in range(2):
        for half in range(2):
            for stage in range(2):
                kv_copy(head, half, stage).wait_send()

    def drain_q(step, carry):
        for head in range(2):

            @pl.when(jnp.logical_not(q_here(head, step)))
            def _():
                q_copy(head, step).wait_send()

        return carry

    lax.fori_loop(0, 2 * NZ, drain_q, 0)

    def drain(block, carry):
        ahead = lax.rem(z - block // NY + NZ, NZ)
        behind = lax.rem(NZ - ahead, NZ)
        first = lax.rem(block, NY) < NY // 2

        @pl.when(jnp.logical_or(ahead < 3, jnp.logical_and(ahead == 3, first)))
        def _():
            ring_copy(block, 0).wait_send()

        @pl.when(
            jnp.logical_or(behind < 3, jnp.logical_and(behind == 3, jnp.logical_not(first)))
        )
        def _():
            ring_copy(block, 1).wait_send()

        @pl.when(block != me)
        def _():
            share_copy(block).wait_send()

        return carry

    lax.fori_loop(0, n_sp, drain, 0)

    def drain_back(block, carry):
        @pl.when(jnp.logical_not(back_here(block)))
        def _():
            back_copy(block).wait_send()

        return carry

    lax.fori_loop(0, n_sp, drain_back, 0)

    source_z = lax.rem(col + n_sp - me, NZ)
    for pair in range(n_tp):
        for sub in range(2):
            values = []
            for head in (2 * pair, 2 * pair + 1):
                slot = head * 2 + sub
                here = jnp.logical_and(source_z * NY + head % NY == me, 2 * (head // NY) + sub == col)

                @pl.when(jnp.logical_not(here))
                def _():
                    arrived(att.at[slot], back_recv.at[slot])

                values.append(att[slot].astype(F32))
            top = jnp.where(lane16 < DIM, values[0], turn(values[1]))
            low = jnp.where(lane16 < DIM, turn(values[0]), values[1])
            cols = slice(pair * LANES, (pair + 1) * LANES)
            att_rows[SHARE * sub : SHARE * sub + 16, cols] = top.astype(BF16)
            att_rows[SHARE * sub + 16 : SHARE * (sub + 1), cols] = low.astype(BF16)

    for part in range(PARTS):
        arrived(wfull.at[sibling, part], wo_recv.at[sibling, part])
        for k in range(1, places):
            block = lax.rem(place + k, places) * 2 + 1 - core
            arrived(wfull.at[block, part], wo_recv.at[block, part])

    def put(first):
        return pltpu.make_async_copy(
            mixed.at[:, pl.ds(first, COLS)], out_ref.at[:, pl.ds(first, COLS)],
            out_sem.at[first // COLS],
        )

    for first in range(0, out_ref.shape[1], COLS):
        w = wfull[:, :, :, first : first + COLS].reshape(att_rows.shape[1], COLS)
        mixed[:, first : first + COLS] = jnp.dot(
            att_rows[...], w, preferred_element_type=F32
        ).astype(BF16)
        put(first).start()
    for first in range(0, out_ref.shape[1], COLS):
        put(first).wait()


def shards(tokens, w_query, w_key, w_value, head_bias, w_out):
    model, local_width = w_query.shape
    n_tp = lax.axis_size("tp")
    n_sp = lax.axis_size("sp")
    device_rows = tokens.shape[0]
    out_width = w_out.shape[1]
    kinds = n_tp - 1

    smem = pl.BlockSpec(memory_space=pltpu.SMEM)
    anywhere = pl.BlockSpec(memory_space=pl.ANY)
    dma = pltpu.SemaphoreType.DMA

    def vmem(*shape):
        return pltpu.VMEM(shape, BF16)

    return pl.pallas_call(
        layer_kernel,
        out_shape=jax.ShapeDtypeStruct((device_rows, out_width), BF16),
        in_specs=[smem] + [anywhere] * 5,
        out_specs=anywhere,
        scratch_shapes=[
            vmem(n_tp, PARTS, device_rows // PARTS, model),
            vmem(model, 3 * local_width),
            vmem(n_tp, PARTS, local_width // PARTS, out_width),
            pltpu.VMEM((n_tp, device_rows, 3 * local_width), F32),
            pltpu.VMEM((2, 2, 8, LANES), F32),
            vmem(2, 2, HALF, LANES),
            vmem(2, SHARES, SHARE // 2, LANES),
            vmem(n_sp, SHARE // 2, LANES),
            vmem(n_sp, 2, HALF, LANES),
            vmem(TILES, LANES, LANES),
            vmem(TILES, LANES, LANES),
            pltpu.VMEM((2, BATCH, HALF, 4 * LANES), F32),
            pltpu.VMEM((2, BATCH, HALF, 4 * LANES), F32),
            pltpu.VMEM((NZ, TILES, DIM, LANES), F32),
            pltpu.VMEM((NZ, TILES, 8, LANES), F32),
            vmem(n_sp, SHARE // 2, LANES),
            vmem(32, SHARE // 2, LANES),
            vmem(device_rows, n_tp * local_width),
            vmem(device_rows, out_width),
            pltpu.SemaphoreType.REGULAR,
            dma((out_width // COLS,)),
            dma((5,)),
            dma((kinds, PARTS)),
            dma((n_tp, PARTS)),
            dma((kinds, PARTS)),
            dma((n_tp, PARTS)),
            dma,
            dma,
            dma((2, 2, 2)),
            dma((n_sp, 2)),
            dma((n_sp, 2)),
            dma((n_sp,)),
            dma((2, 2 * NZ)),
            dma((n_sp,)),
            dma((n_sp,)),
            dma((32,)),
        ],
        compiler_params=pltpu.CompilerParams(
            collective_id=0, has_side_effects=True, vmem_limit_bytes=60 * 2**20
        ),
        name="layer",
    )(
        head_bias,
        tokens.reshape(PARTS, device_rows // PARTS, model),
        w_query, w_key, w_value,
        w_out.reshape(PARTS, local_width // PARTS, out_width),
    )


def solution(mesh):
    placed = (
        P(("sp", "tp"), None),
        P(None, "tp"),
        P(None, "tp"),
        P(None, "tp"),
        P("tp"),
        P("tp", None),
    )
    return jax.shard_map(
        shards, mesh=mesh, in_specs=placed, out_specs=P(("sp", "tp"), None), check_vma=False
    )
```

```python
import functools
import math

import jax
import jax.numpy as jnp
from jax import lax
from jax.experimental import pallas as pl
from jax.experimental.pallas import tpu as pltpu
from jax.sharding import PartitionSpec as P

MESH = pl.DeviceIdType.MESH
F32, BF16 = jnp.float32, jnp.bfloat16
LOG2E = math.log2(math.e)
PARTS = 4
COLS = 512
EXP_MAX = 126.0
DEAD = -1e30
NZ, NY = 8, 4
SEG = 512
HALF = 256
LANES = 128
DIM = 64
RUN = 64
SHARE = 32
SHARES = SEG // SHARE
TILES = 8
FAR = 1 << 20
BATCH = 2
STEPS = NZ * NY // BATCH


def layer_kernel(
    bias_ref, tokens_ref, wq_ref, wk_ref, wv_ref, wo_ref, out_ref,
    tok, wqkv, wfull, proj, bias_all, kv_own, q_own, q_all, kv_all, q_top, q_low, raw, xs,
    seg_acc, seg_keep, packed, att, att_rows, mixed,
    plane_sem, out_sem, load_sem, tok_send, tok_recv, tok_pair, wo_send, wo_recv, wo_pair,
    bias_send, bias_recv, kv_send, kv_recv, ring_send, share_send, q_send, q_recv, back_send, back_recv,
):
    me = lax.axis_index("sp")
    col = lax.axis_index("tp")
    n_sp, n_tp = NZ * NY, 8
    z, y = me // NY, lax.rem(me, NY)
    place, core = col // 2, lax.rem(col, 2)
    places = n_tp // 2
    sibling = place * 2 + 1 - core
    head_core, head_local = y // 2, lax.rem(y, 2)
    mine = core == head_core

    loads = [
        pltpu.make_async_copy(src, dst, load_sem.at[index])
        for index, (src, dst) in enumerate(
            [
                (tokens_ref, tok.at[col]),
                (wq_ref, wqkv.at[:, 0:LANES]),
                (wk_ref, wqkv.at[:, LANES : 2 * LANES]),
                (wv_ref, wqkv.at[:, 2 * LANES : 3 * LANES]),
                (wo_ref, wfull.at[col]),
            ]
        )
    ]
    for copy in loads:
        copy.start()

    barrier = pltpu.get_barrier_semaphore()
    for step in range(1, n_tp):
        pl.semaphore_signal(
            barrier, inc=1, device_id=(me, lax.rem(col + step, n_tp)), device_id_type=MESH
        )
    for step in range(1, NY):
        peer = z * NY + lax.rem(y + step, NY)
        for other in range(2):
            pl.semaphore_signal(
                barrier, inc=1, device_id=(peer, place * 2 + other), device_id_type=MESH
            )
    for step in range(1, NZ):
        peer = lax.rem(z + step, NZ) * NY + y
        pl.semaphore_signal(barrier, inc=1, device_id=(peer, col), device_id_type=MESH)
    for head in range(2):
        bias_all[core, head] = jnp.full((8, LANES), bias_ref[head] * LOG2E, F32)
    seg_acc[...] = jnp.zeros_like(seg_acc)
    seg_keep[...] = jnp.ones_like(seg_keep)
    pl.semaphore_wait(barrier, n_tp - 1 + 2 * (NY - 1) + NZ - 1)
    for step in range(1, NZ):
        peer = lax.rem(z + step, NZ) * NY + y
        pl.semaphore_signal(plane_sem, inc=1, device_id=(peer, col), device_id_type=MESH)

    def same_core(k):
        return lax.rem(place + k, places) * 2 + core

    def arrived(ref, sem):
        pltpu.make_async_copy(ref, ref, sem).wait()

    def link(kind, own, kept, sent, received, paired, part):
        if kind == 2:
            ahead = part < kept.shape[1] // 2
            block = same_core(3 if ahead else 1)
            src, target = kept.at[block, part], same_core(1 if ahead else 3)
        elif kind < places:
            src, block = own.at[part], col
            target = sibling if kind == 0 else same_core(kind)
        else:
            block = same_core(kind - places + 1)
            src, target = kept.at[block, part], sibling
        inside = kind == 0 or kind >= places
        return pltpu.make_async_remote_copy(
            src_ref=src, dst_ref=kept.at[block, part], send_sem=sent,
            recv_sem=paired.at[part % 2] if inside else received.at[block // 2, part],
            device_id=(me, target), device_id_type=MESH,
        )

    def token_copy(kind, part):
        return link(kind, tokens_ref, tok, tok_send, tok_recv, tok_pair, part)

    def wo_copy(kind, part):
        return link(kind, wo_ref, wfull, wo_send, wo_recv, wo_pair, part)

    def relay(copy, kept, received, part, k):
        block = same_core(k)
        arrived(kept.at[block, part], received.at[block // 2, part])
        copy(places + k - 1, part).start()
        if k != 2 and (part < kept.shape[1] // 2) == (k == 3):
            copy(2, part).start()

    bias_copy = pltpu.make_async_remote_copy(
        src_ref=bias_all.at[core], dst_ref=bias_all.at[core],
        send_sem=bias_send, recv_sem=bias_recv, device_id=(me, sibling), device_id_type=MESH,
    )

    turned = (2, 3, 0, 1)
    for part in range(PARTS // 2):
        token_copy(1, part).start()
        token_copy(3, turned[part]).start()
    for part in (0, 2, 1, 3):
        token_copy(0, part).start()
    bias_copy.start()

    def pair_at(block):
        return n_sp + block // BATCH

    def kv_copy(head, half, stage):
        aim = core * 2 + head
        own = aim == y
        sp = jnp.where(own, me, z * NY + aim)
        tp = jnp.where(own, sibling, place * 2 + half)
        return pltpu.make_async_remote_copy(
            src_ref=kv_own.at[head, half, pl.ds(LANES * (1 - stage), LANES)],
            dst_ref=kv_all.at[me, half, pl.ds(LANES * (1 - stage), LANES)],
            send_sem=kv_send,
            recv_sem=kv_recv.at[
                jnp.where(jnp.logical_and(own, core == half), pair_at(me), me)
            ],
            device_id=(sp, tp), device_id_type=MESH,
        )

    def ring_copy(block, way):
        peer = lax.rem(z + (1 if way == 0 else NZ - 1), NZ) * NY + y
        return pltpu.make_async_remote_copy(
            src_ref=kv_all.at[block, core], dst_ref=kv_all.at[block, core],
            send_sem=ring_send.at[way], recv_sem=kv_recv.at[block],
            device_id=(peer, col), device_id_type=MESH,
        )

    def share_copy(block):
        return pltpu.make_async_remote_copy(
            src_ref=kv_all.at[block, core], dst_ref=kv_all.at[block, core],
            send_sem=share_send, recv_sem=kv_recv.at[pair_at(block)],
            device_id=(me, sibling), device_id_type=MESH,
        )

    def rows_of(to_z, to_core, block):
        return lax.rem(2 * to_z + to_core + 2 * block, SHARES)

    def q_copy(head, step):
        to_z, to_core = step // 2, lax.rem(step, 2)
        return pltpu.make_async_remote_copy(
            src_ref=q_own.at[head, rows_of(to_z, to_core, me)], dst_ref=q_all.at[me],
            send_sem=q_send, recv_sem=q_recv,
            device_id=(to_z * NY + core * 2 + head, place * 2 + to_core), device_id_type=MESH,
        )

    def q_here(head, step):
        to_z, to_core = step // 2, lax.rem(step, 2)
        return jnp.logical_and(to_z * NY + core * 2 + head == me, to_core == core)

    def back_owner(block):
        return lax.rem(z + block, n_tp)

    my_slot = (place * NY + y) * 2 + core

    def back_here(block):
        return jnp.logical_and(block == me, back_owner(block) == col)

    def back_copy(block):
        return pltpu.make_async_remote_copy(
            src_ref=packed.at[block], dst_ref=att.at[my_slot],
            send_sem=back_send, recv_sem=back_recv,
            device_id=(block, back_owner(block)), device_id_type=MESH,
        )

    for copy in loads:
        copy.wait()
    def turn(value):
        return pltpu.roll(value, DIM, 1)

    lane16 = lax.broadcasted_iota(jnp.int32, (16, LANES), 1)

    def weave(upper, lower):
        first = jnp.where(lane16 < DIM, upper, turn(lower)).astype(BF16)
        second = jnp.where(lane16 < DIM, turn(upper), lower).astype(BF16)
        return first, second

    def strided(i, kind):
        return proj[:, RUN - 1 - i, kind * LANES : (kind + 1) * LANES]

    def send_q(step, carry):
        for head in range(2):

            @pl.when(jnp.logical_not(q_here(head, step)))
            def _():
                q_copy(head, step).start()

        return carry

    for part in range(PARTS // 2):
        relay(token_copy, tok, tok_recv, part, 3)
        token_copy(1, part + 2).start()
        relay(token_copy, tok, tok_recv, turned[part], 1)
        token_copy(3, turned[part + 2]).start()
    for stage in range(2):
        parts = (stage, stage + 2)
        relay(token_copy, tok, tok_recv, stage + 2, 3)
        relay(token_copy, tok, tok_recv, turned[stage + 2], 1)
        for part in parts:
            relay(token_copy, tok, tok_recv, part, 2)
        arrived(tok.at[pl.ds(0, 2)], tok_pair.at[stage])
        depth, model = tok.shape[2:]
        x = jnp.concatenate([tok[:, part].reshape(n_tp * depth, model) for part in parts], axis=0)
        both = jnp.dot(x, wqkv[...], preferred_element_type=F32)
        for index, part in enumerate(parts):
            proj[:, part * depth : (part + 1) * depth, :] = both[
                index * n_tp * depth : (index + 1) * n_tp * depth
            ].reshape(n_tp, depth, 3 * LANES)
        if stage == 1:
            for share in range(SHARES):
                block, first = share // 2, 32 * (share % 2)
                q = proj[block, first : first + 32, 0:LANES] * (LOG2E * DIM ** (-0.5))
                q_own[0, share], q_own[1, share] = weave(q[:16], q[16:])
            pl.semaphore_wait(plane_sem, NZ - 1)
            lax.fori_loop(0, 2 * NZ, send_q, 0)
        base = 16 * (1 - stage)
        for i in range(base, base + 16, 2):
            upper = jnp.concatenate([strided(i, 1), strided(i + 1, 1)], axis=0)
            lower = jnp.concatenate([strided(i + 32, 1), strided(i + 33, 1)], axis=0)
            kv_own[0, 0, 8 * i : 8 * i + 16], kv_own[1, 0, 8 * i : 8 * i + 16] = weave(
                upper, lower
            )
        for head in range(2):
            kv_copy(head, 0, stage).start()
        for index in range(2):
            first = base + 32 * index
            block = jnp.concatenate([strided(first + i, 2) for i in range(16)], axis=0)
            flipped = block.T.astype(BF16)
            at = LANES * (1 - stage) + DIM * index
            for head in range(2):
                kv_own[head, 1, at : at + DIM] = flipped[DIM * head : DIM * (head + 1)]
        for head in range(2):
            kv_copy(head, 1, stage).start()

    for part in range(2):
        for kind in (1, 3, 0):
            wo_copy(kind, 1 - part if kind == 3 else part).start()

    for head in range(2):

        @pl.when(core * 2 + head == y)
        def _():
            kv_all[me] = kv_own[head]
            q_all[me] = q_own[head, rows_of(z, core, me)]

    def halves_here(block):
        return jnp.logical_and(block == me, mine)

    for step in range(NY):
        block = z * NY + lax.rem(y + step, NY)

        @pl.when(jnp.logical_not(halves_here(block)))
        def _():
            arrived(kv_all.at[block, core], kv_recv.at[block])

        for way in range(2):
            ring_copy(block, way).start()

        @pl.when(block != me)
        def _():
            share_copy(block).start()

    def whole(count, less, buffer, sem):
        for short in range(2):

            @pl.when(less == (short == 1))
            def _():
                arrived(buffer.at[pl.ds(0, count - short)], sem)

    whole(n_sp, mine, q_all, q_recv)

    for tile in range(TILES):
        pieces = []
        for part in range(NY):
            pair = q_all[tile * NY + part].astype(F32)
            pieces.append(jnp.where(lane16 < DIM, pair, 0.0))
            pieces.append(jnp.where(lane16 < DIM, turn(pair), 0.0))
        flipped = jnp.concatenate(pieces, axis=0).T
        q_top[tile] = flipped.astype(BF16)
        q_low[tile] = jnp.concatenate([flipped[DIM:], flipped[:DIM]], axis=0).astype(BF16)

    arrived(bias_all.at[1 - core], bias_recv)

    def suffix(keep):
        row = lax.broadcasted_iota(jnp.int32, keep.shape, 0)
        product = keep
        for step in (1, 2, 4):
            moved = pltpu.roll(product, 8 - step, 0)
            product = product * jnp.where(row + step < 8, moved, 1.0)
        after = jnp.where(row + 1 < 8, pltpu.roll(product, 7, 0), 1.0)
        return after, product[0:1]

    def segment(block, bank, slot, width, bias, reach):
        keep = jnp.ones((8, 2 * width), F32)
        for i in range(RUN // 2):
            score = raw[bank, slot, 8 * i : 8 * i + 8, 0 : 2 * width] + bias
            if reach is not None:
                score = jnp.where(reach > -i, score, DEAD)
            odds = jnp.exp2(jnp.minimum(score, EXP_MAX))
            lose = 1.0 / (1.0 + odds)
            xs[bank, slot, 8 * i : 8 * i + 8, 0 : 2 * width] = odds * lose * keep
            keep = keep * lose
        near, far = keep[:, :width], keep[:, width:]
        after, whole = suffix(near * far)
        values = kv_all[block, 1]
        out = None
        for half, factor in enumerate((after, after * near)):
            part = xs[bank, slot, :, half * width : (half + 1) * width].reshape(RUN // 2, 8, width)
            weight = (part * factor[None]).reshape(HALF, width).astype(BF16)
            first = half * DIM
            value = jnp.concatenate(
                [values[first : first + DIM], values[LANES + first : LANES + first + DIM]], axis=1
            )
            term = jnp.dot(value, weight, preferred_element_type=F32)
            out = term if out is None else out + term
        return out, whole

    def cover(group, part, tile, count, diagonal, bank):
        width = count * LANES
        q = jnp.concatenate(
            [q_top[tile + n] for n in range(count)] + [q_low[tile + n] for n in range(count)],
            axis=1,
        )
        bias = bias_all[head_core, head_local]
        bias = jnp.concatenate([bias] * (2 * count), axis=1)
        if diagonal:
            lane = lax.broadcasted_iota(jnp.int32, (8, 2 * width), 1)
            row = lax.broadcasted_iota(jnp.int32, (8, 2 * width), 0)
            half = lane // width
            inside = lax.rem(lane, width)
            owner = lax.rem(inside // SHARE, NY)
            share = rows_of(z, core, tile * NY + owner)
            query = SEG * owner + SHARE * share + lax.rem(inside, SHARE)
            query = jnp.where(inside < LANES, query, FAR)
            reach = query - row * RUN - (RUN - 1) + half * (RUN // 2) - SEG * part
        first = group * NY + part
        raw[bank, :, :, 0 : 2 * width] = jnp.dot(
            kv_all[pl.ds(first, BATCH), 0].reshape(BATCH * HALF, LANES), q,
            preferred_element_type=F32,
        ).reshape(BATCH, HALF, 2 * width)
        acc = [seg_acc[group, tile + n] for n in range(count)]
        keep = [seg_keep[group, tile + n][0:1] for n in range(count)]
        for index in range(BATCH):
            limit = reach - SEG * index if diagonal else None
            out, whole = segment(first + index, bank, index, width, bias, limit)
            for n in range(count):
                lanes = slice(n * LANES, (n + 1) * LANES)
                acc[n] = acc[n] * whole[:, lanes] + out[:, lanes]
                keep[n] = keep[n] * whole[:, lanes]
        for n in range(count):
            seg_acc[group, tile + n] = acc[n]
            seg_keep[group, tile + n] = jnp.broadcast_to(keep[n], (8, LANES))

    def attend(group, part, between):
        count = TILES - group
        odd = lax.rem(count, 2)
        pairs = (count - 1) // 2
        first = group + 2 - odd

        for single in range(2):
            for more in range(2):

                @pl.when(jnp.logical_and(odd == single, (pairs > 0) == (more == 1)))
                def _():
                    cover(group, part, group, 2 - single, True, 0)
                    if more:
                        cover(group, part, first, 2, False, 1)

        between()

        @pl.when(pairs == 2)
        def _():
            cover(group, part, first + 2, 2, False, 0)

        @pl.when(pairs == 3)
        def _():
            cover(group, part, first + 2, 2, False, 0)
            cover(group, part, first + 4, 2, False, 1)

    def stop_at(step):
        turn_of = lax.rem(step + 2, 4)
        far = step >= STEPS - 2
        distance = (step + 2) // 4
        own = step < 2
        behind = jnp.logical_or(jnp.logical_and(far, turn_of == 0), lax.rem(step, 2) == 0)
        part = jnp.where(jnp.logical_or(own, far), lax.rem(step, 2), turn_of // 2) * BATCH
        group = lax.rem(z + NZ + jnp.where(behind, -distance, distance), NZ)
        return group, part

    def forward(index):
        distance, turn_of = index // NZ + 1, lax.rem(index, NZ)
        last = distance == NZ // 2
        behind = lax.rem(index, 2) == 0
        part = jnp.where(last, lax.rem(index, 2) * BATCH, 0) + turn_of // 2
        group = lax.rem(z + NZ + jnp.where(behind, -distance, distance), NZ)
        block = group * NY + part
        arrived(kv_all.at[block, core], kv_recv.at[block])
        for way in range(2):
            onward = jnp.logical_or(
                distance < 3, jnp.logical_and(distance == 3, (part < BATCH) == (way == 0))
            )

            @pl.when(jnp.logical_and(behind == (way == 0), onward))
            def _():
                ring_copy(block, way).start()

        share_copy(block).start()

    def visit(step, carry):
        def forward_if(low, high, index):
            @pl.when(jnp.logical_and(step >= low, step < high))
            def _():
                forward(index)

        forward_if(1, 2, 0)
        forward_if(1, 2, 1)
        forward_if(2, STEPS - 2, 2 * step)

        @pl.when(step == STEPS // 2)
        def _():
            for part in range(2):
                relay(wo_copy, wfull, wo_recv, part, 3)
                relay(wo_copy, wfull, wo_recv, 1 - part, 1)

        @pl.when(step == STEPS - 2)
        def _():
            for part in range(2):
                relay(wo_copy, wfull, wo_recv, part, 2)

        group, part = stop_at(step)
        block = group * NY + part
        here = jnp.logical_and(block // BATCH == me // BATCH, mine)
        for short in range(2):

            @pl.when(here == (short == 1))
            def _():
                arrived(
                    kv_all.at[pl.ds(block, BATCH - short), 1 - core], kv_recv.at[pair_at(block)]
                )

        def between():
            forward_if(1, 2, 2)
            forward_if(1, 2, 3)
            forward_if(2, STEPS - 2, 2 * step + 1)

        attend(group, part, between)
        return carry

    lax.fori_loop(0, STEPS, visit, 0)

    def combine(tile):
        acc = seg_acc[0, tile]
        for group in range(1, NZ):
            acc = acc * seg_keep[group, tile][0:1] + seg_acc[group, tile]
        return acc

    for pair in range(TILES // 2):
        flipped = jnp.concatenate([combine(2 * pair), combine(2 * pair + 1)], axis=0).T
        for part in range(NY):
            upper = flipped[SHARE * part : SHARE * part + 16]
            lower = flipped[SHARE * part + 16 : SHARE * (part + 1)]
            for n, folded in enumerate(weave(upper, lower)):
                block = (2 * pair + n) * NY + part
                packed[block] = folded
                here = back_here(block)

                @pl.when(here)
                def _():
                    att[my_slot] = folded

                @pl.when(jnp.logical_not(here))
                def _():
                    back_copy(block).start()

    bias_copy.wait_send()
    arrived(wfull.at[pl.ds(0, n_tp - 1)], wo_send)
    arrived(tok.at[pl.ds(0, n_tp - 1)], tok_send)
    arrived(kv_own, kv_send)
    whole(n_sp, mine, q_all, q_send)
    for way in range(2):
        arrived(kv_all.at[pl.ds(0, 14), 0], ring_send.at[way])
    arrived(kv_all.at[pl.ds(0, n_sp - 1), 0], share_send)
    whole(n_sp, back_here(me), att, back_send)
    whole(n_sp, back_here(me), att, back_recv)

    for pair in range(n_tp):
        for sub in range(2):
            values = []
            for head in (2 * pair, 2 * pair + 1):
                slot = head * 2 + sub
                values.append(att[slot].astype(F32))
            top = jnp.where(lane16 < DIM, values[0], turn(values[1]))
            low = jnp.where(lane16 < DIM, turn(values[0]), values[1])
            cols = slice(pair * LANES, (pair + 1) * LANES)
            att_rows[SHARE * sub : SHARE * sub + 16, cols] = top.astype(BF16)
            att_rows[SHARE * sub + 16 : SHARE * (sub + 1), cols] = low.astype(BF16)

    for part in range(2):
        arrived(wfull.at[pl.ds(0, 2)], wo_pair.at[part])

    def put(first):
        return pltpu.make_async_copy(
            mixed.at[:, pl.ds(first, COLS)], out_ref.at[:, pl.ds(first, COLS)],
            out_sem,
        )

    for first in range(0, out_ref.shape[1], COLS):
        w = wfull[:, :, :, first : first + COLS].reshape(att_rows.shape[1], COLS)
        mixed[:, first : first + COLS] = jnp.dot(
            att_rows[...], w, preferred_element_type=F32
        ).astype(BF16)
        put(first).start()
    pltpu.make_async_copy(mixed, out_ref, out_sem).wait()


def shards(tokens, w_query, w_key, w_value, head_bias, w_out):
    model, local_width = w_query.shape
    n_tp = lax.axis_size("tp")
    n_sp = lax.axis_size("sp")
    device_rows = tokens.shape[0]
    out_width = w_out.shape[1]

    smem = pl.BlockSpec(memory_space=pltpu.SMEM)
    anywhere = pl.BlockSpec(memory_space=pl.ANY)
    dma = pltpu.SemaphoreType.DMA

    def vmem(*shape):
        return pltpu.VMEM(shape, BF16)

    return pl.pallas_call(
        layer_kernel,
        out_shape=jax.ShapeDtypeStruct((device_rows, out_width), BF16),
        in_specs=[smem] + [anywhere] * 5,
        out_specs=anywhere,
        scratch_shapes=[
            vmem(n_tp, PARTS, device_rows // PARTS, model),
            vmem(model, 3 * local_width),
            vmem(n_tp, 2, local_width // 2, out_width),
            pltpu.VMEM((n_tp, device_rows, 3 * local_width), F32),
            pltpu.VMEM((2, 2, 8, LANES), F32),
            vmem(2, 2, HALF, LANES),
            vmem(2, SHARES, SHARE // 2, LANES),
            vmem(n_sp, SHARE // 2, LANES),
            vmem(n_sp, 2, HALF, LANES),
            vmem(TILES, LANES, LANES),
            vmem(TILES, LANES, LANES),
            pltpu.VMEM((2, BATCH, HALF, 4 * LANES), F32),
            pltpu.VMEM((2, BATCH, HALF, 4 * LANES), F32),
            pltpu.VMEM((NZ, TILES, DIM, LANES), F32),
            pltpu.VMEM((NZ, TILES, 8, LANES), F32),
            vmem(n_sp, SHARE // 2, LANES),
            vmem(32, SHARE // 2, LANES),
            vmem(device_rows, n_tp * local_width),
            vmem(device_rows, out_width),
            pltpu.SemaphoreType.REGULAR,
            dma,
            dma((5,)),
            dma,
            dma((n_tp // 2, PARTS)),
            dma((2,)),
            dma,
            dma((n_tp // 2, 2)),
            dma((2,)),
            dma,
            dma,
            dma,
            dma((n_sp + n_sp // BATCH,)),
            dma((2,)),
            dma,
            dma,
            dma,
            dma,
            dma,
        ],
        compiler_params=pltpu.CompilerParams(
            collective_id=0, has_side_effects=True, vmem_limit_bytes=60 * 2**20
        ),
        name="layer",
    )(
        head_bias,
        tokens.reshape(PARTS, device_rows // PARTS, model),
        w_query, w_key, w_value,
        w_out.reshape(2, local_width // 2, out_width),
    )


def solution(mesh):
    placed = (
        P(("sp", "tp"), None),
        P(None, "tp"),
        P(None, "tp"),
        P(None, "tp"),
        P("tp"),
        P("tp", None),
    )
    return jax.shard_map(
        shards, mesh=mesh, in_specs=placed, out_specs=P(("sp", "tp"), None), check_vma=False
    )
```

```python
import functools
import math

import jax
import jax.numpy as jnp
from jax import lax
from jax.experimental import pallas as pl
from jax.experimental.pallas import tpu as pltpu
from jax.sharding import PartitionSpec as P

MESH = pl.DeviceIdType.MESH
F32, BF16 = jnp.float32, jnp.bfloat16
LOG2E = math.log2(math.e)
PARTS = 4
COLS = 512
EXP_MAX = 126.0
DEAD = -1e30
NZ, NY = 8, 4
SEG = 512
HALF = 256
LANES = 128
DIM = 64
RUN = 64
UNITS = 8
SIDE = 4
BATCH = 2
STEPS = NZ * NY // BATCH


def layer_kernel(
    bias_ref, tokens_ref, wq_ref, wk_ref, wv_ref, wo_ref, out_ref,
    tok, wqkv, wfull, proj, bias_all, kv_own, q_own, q_all, kv_all, q_top, q_low, raw, xs,
    seg_acc, seg_keep, packed, att, att_rows, mixed,
    plane_sem, out_sem, load_sem, tok_send, tok_recv, tok_pair, wo_send, wo_recv, wo_pair,
    bias_send, bias_recv, kv_send, kv_recv, ring_send, share_send, q_send, q_recv, back_send, back_recv,
):
    me = lax.axis_index("sp")
    col = lax.axis_index("tp")
    n_sp, n_tp = NZ * NY, 8
    z, y = me // NY, lax.rem(me, NY)
    place, core = col // 2, lax.rem(col, 2)
    places = n_tp // 2
    sibling = place * 2 + 1 - core
    head_core, head_local = y // 2, lax.rem(y, 2)
    mine = core == head_core

    loads = [
        pltpu.make_async_copy(src, dst, load_sem.at[index])
        for index, (src, dst) in enumerate(
            [
                (tokens_ref, tok.at[col]),
                (wq_ref, wqkv.at[:, 0:LANES]),
                (wk_ref, wqkv.at[:, LANES : 2 * LANES]),
                (wv_ref, wqkv.at[:, 2 * LANES : 3 * LANES]),
                (wo_ref, wfull.at[col]),
            ]
        )
    ]
    for copy in loads:
        copy.start()

    barrier = pltpu.get_barrier_semaphore()
    for step in range(1, n_tp):
        pl.semaphore_signal(
            barrier, inc=1, device_id=(me, lax.rem(col + step, n_tp)), device_id_type=MESH
        )
    for step in range(1, NY):
        peer = z * NY + lax.rem(y + step, NY)
        for other in range(2):
            pl.semaphore_signal(
                barrier, inc=1, device_id=(peer, place * 2 + other), device_id_type=MESH
            )
    for step in range(1, NZ):
        peer = lax.rem(z + step, NZ) * NY + y
        pl.semaphore_signal(barrier, inc=1, device_id=(peer, col), device_id_type=MESH)
    for head in range(2):
        bias_all[core, head] = jnp.full((8, LANES), bias_ref[head] * LOG2E, F32)
    seg_acc[...] = jnp.zeros_like(seg_acc)
    seg_keep[...] = jnp.ones_like(seg_keep)
    pl.semaphore_wait(barrier, n_tp - 1 + 2 * (NY - 1) + NZ - 1)
    for step in range(1, NZ):
        peer = lax.rem(z + step, NZ) * NY + y
        pl.semaphore_signal(plane_sem, inc=1, device_id=(peer, col), device_id_type=MESH)

    def same_core(k):
        return lax.rem(place + k, places) * 2 + core

    def arrived(ref, sem):
        pltpu.make_async_copy(ref, ref, sem).wait()

    def link(kind, own, kept, sent, received, paired, part):
        if kind == 2:
            ahead = part < kept.shape[1] // 2
            block = same_core(3 if ahead else 1)
            src, target = kept.at[block, part], same_core(1 if ahead else 3)
        elif kind < places:
            src, block = own.at[part], col
            target = sibling if kind == 0 else same_core(kind)
        else:
            block = same_core(kind - places + 1)
            src, target = kept.at[block, part], sibling
        inside = kind == 0 or kind >= places
        return pltpu.make_async_remote_copy(
            src_ref=src, dst_ref=kept.at[block, part], send_sem=sent,
            recv_sem=paired.at[part % 2] if inside else received.at[block // 2, part],
            device_id=(me, target), device_id_type=MESH,
        )

    def token_copy(kind, part):
        return link(kind, tokens_ref, tok, tok_send, tok_recv, tok_pair, part)

    def wo_copy(kind, part):
        return link(kind, wo_ref, wfull, wo_send, wo_recv, wo_pair, part)

    def relay(copy, kept, received, part, k):
        block = same_core(k)
        arrived(kept.at[block, part], received.at[block // 2, part])
        copy(places + k - 1, part).start()
        if k != 2 and (part < kept.shape[1] // 2) == (k == 3):
            copy(2, part).start()

    bias_copy = pltpu.make_async_remote_copy(
        src_ref=bias_all.at[core], dst_ref=bias_all.at[core],
        send_sem=bias_send, recv_sem=bias_recv, device_id=(me, sibling), device_id_type=MESH,
    )

    turned = (2, 3, 0, 1)
    for part in range(PARTS // 2):
        token_copy(1, part).start()
        token_copy(3, turned[part]).start()
    for part in (0, 2, 1, 3):
        token_copy(0, part).start()
    bias_copy.start()

    def pair_at(block):
        return n_sp + block // BATCH

    def kv_copy(head, half, stage):
        aim = core * 2 + head
        own = aim == y
        sp = jnp.where(own, me, z * NY + aim)
        tp = jnp.where(own, sibling, place * 2 + half)
        return pltpu.make_async_remote_copy(
            src_ref=kv_own.at[head, half, pl.ds(LANES * (1 - stage), LANES)],
            dst_ref=kv_all.at[me, half, pl.ds(LANES * (1 - stage), LANES)],
            send_sem=kv_send,
            recv_sem=kv_recv.at[
                jnp.where(jnp.logical_and(own, core == half), pair_at(me), me)
            ],
            device_id=(sp, tp), device_id_type=MESH,
        )

    def ring_copy(block, way):
        peer = lax.rem(z + (1 if way == 0 else NZ - 1), NZ) * NY + y
        return pltpu.make_async_remote_copy(
            src_ref=kv_all.at[block, core], dst_ref=kv_all.at[block, core],
            send_sem=ring_send.at[way], recv_sem=kv_recv.at[block],
            device_id=(peer, col), device_id_type=MESH,
        )

    def share_copy(block):
        return pltpu.make_async_remote_copy(
            src_ref=kv_all.at[block, core], dst_ref=kv_all.at[block, core],
            send_sem=share_send, recv_sem=kv_recv.at[pair_at(block)],
            device_id=(me, sibling), device_id_type=MESH,
        )

    def keeper(tile, chosen):
        low = jnp.minimum(tile, NZ - 1 - tile)
        return jnp.where(
            low == 2, 3 * chosen, jnp.where(low == 3, 1, 4 + 2 * low) + chosen
        )

    low_tile = jnp.where(z >= 4, z // 2 - 2, jnp.where(lax.rem(z, 3) == 0, 2, 3))
    chosen = jnp.where(z >= 4, lax.rem(z, 2), z // 2)

    def rows_of(of_chosen, of_core, block):
        return lax.rem(2 * of_chosen + of_core + block, SIDE)

    def unit_block(unit):
        tile = jnp.where(unit >= SIDE, NZ - 1 - low_tile, low_tile)
        return tile * NY + lax.rem(unit, SIDE)

    def q_copy(head, step):
        to_chosen, to_core = step // 2, step % 2
        unit = jnp.where(z >= NZ // 2, SIDE, 0) + y
        return pltpu.make_async_remote_copy(
            src_ref=q_own.at[head, rows_of(to_chosen, to_core, me)], dst_ref=q_all.at[unit],
            send_sem=q_send, recv_sem=q_recv,
            device_id=(
                keeper(z, to_chosen) * NY + core * 2 + head, place * 2 + to_core
            ), device_id_type=MESH,
        )

    def q_here(head, step):
        to_chosen, to_core = step // 2, step % 2
        return jnp.logical_and(
            keeper(z, to_chosen) * NY + core * 2 + head == me, core == to_core
        )

    q_stays = jnp.logical_and(mine, jnp.logical_or(keeper(z, 0) == z, keeper(z, 1) == z))
    my_slot = place * NY + y

    def back_owner(unit, part):
        return rows_of(chosen, core, unit_block(unit)) * 2 + part

    def back_here(unit, part):
        return jnp.logical_and(unit_block(unit) == me, back_owner(unit, part) == col)

    back_stays = jnp.logical_and(
        jnp.logical_or(low_tile == z, NZ - 1 - low_tile == z), rows_of(chosen, core, me) == place
    )

    def back_copy(unit, part):
        return pltpu.make_async_remote_copy(
            src_ref=packed.at[unit, part], dst_ref=att.at[my_slot],
            send_sem=back_send, recv_sem=back_recv,
            device_id=(unit_block(unit), back_owner(unit, part)), device_id_type=MESH,
        )

    for copy in loads:
        copy.wait()
    def turn(value):
        return pltpu.roll(value, DIM, 1)

    def weave(upper, lower):
        left = lax.broadcasted_iota(jnp.int32, upper.shape, 1) < DIM
        first = jnp.where(left, upper, turn(lower)).astype(BF16)
        second = jnp.where(left, turn(upper), lower).astype(BF16)
        return first, second

    def strided(i, kind):
        return proj[:, RUN - 1 - i, kind * LANES : (kind + 1) * LANES]

    for part in range(PARTS // 2):
        relay(token_copy, tok, tok_recv, part, 3)
        token_copy(1, part + 2).start()
        relay(token_copy, tok, tok_recv, turned[part], 1)
        token_copy(3, turned[part + 2]).start()
    for stage in range(2):
        parts = (stage, stage + 2)
        relay(token_copy, tok, tok_recv, stage + 2, 3)
        relay(token_copy, tok, tok_recv, turned[stage + 2], 1)
        for part in parts:
            relay(token_copy, tok, tok_recv, part, 2)
        arrived(tok.at[pl.ds(0, 2)], tok_pair.at[stage])
        depth, model = tok.shape[2:]
        x = jnp.concatenate([tok[:, part].reshape(n_tp * depth, model) for part in parts], axis=0)
        both = jnp.dot(x, wqkv[...], preferred_element_type=F32)
        for index, part in enumerate(parts):
            proj[:, part * depth : (part + 1) * depth, :] = both[
                index * n_tp * depth : (index + 1) * n_tp * depth
            ].reshape(n_tp, depth, 3 * LANES)
        if stage == 1:
            for share in range(SIDE):
                upper = proj[2 * share, :, 0:LANES] * (LOG2E * DIM ** (-0.5))
                lower = proj[2 * share + 1, :, 0:LANES] * (LOG2E * DIM ** (-0.5))
                q_own[0, share], q_own[1, share] = weave(upper, lower)
            pl.semaphore_wait(plane_sem, NZ - 1)
            for head in range(2):
                for step in range(4):
                    here = q_here(head, step)

                    @pl.when(jnp.logical_not(here))
                    def _():
                        q_copy(head, step).start()

                    @pl.when(here)
                    def _():
                        q_all[jnp.where(z >= NZ // 2, SIDE, 0) + y] = q_own[
                            head, rows_of(step // 2, step % 2, me)
                        ]

        base = 16 * (1 - stage)
        for i in range(base, base + 16, 2):
            upper = jnp.concatenate([strided(i, 1), strided(i + 1, 1)], axis=0)
            lower = jnp.concatenate([strided(i + 32, 1), strided(i + 33, 1)], axis=0)
            kv_own[0, 0, 8 * i : 8 * i + 16], kv_own[1, 0, 8 * i : 8 * i + 16] = weave(
                upper, lower
            )
        for head in range(2):
            kv_copy(head, 0, stage).start()
        for index in range(2):
            first = base + 32 * index
            block = jnp.concatenate([strided(first + i, 2) for i in range(16)], axis=0)
            flipped = block.T.astype(BF16)
            at = LANES * (1 - stage) + DIM * index
            for head in range(2):
                kv_own[head, 1, at : at + DIM] = flipped[DIM * head : DIM * (head + 1)]
        for head in range(2):
            kv_copy(head, 1, stage).start()

    for part in range(2):
        for kind in (1, 3, 0):
            wo_copy(kind, 1 - part if kind == 3 else part).start()

    for head in range(2):

        @pl.when(core * 2 + head == y)
        def _():
            kv_all[me] = kv_own[head]

    def halves_here(block):
        return jnp.logical_and(block == me, mine)

    for step in range(NY):
        block = z * NY + lax.rem(y + step, NY)

        @pl.when(jnp.logical_not(halves_here(block)))
        def _():
            arrived(kv_all.at[block, core], kv_recv.at[block])

        for way in range(2):
            ring_copy(block, way).start()

        @pl.when(block != me)
        def _():
            share_copy(block).start()

    def whole(count, less, buffer, sem):
        for short in range(2):

            @pl.when(less == (short == 1))
            def _():
                arrived(buffer.at[pl.ds(0, count - short)], sem)

    whole(UNITS, q_stays, q_all, q_recv)

    for unit in range(UNITS):
        pair = q_all[unit].astype(F32)
        left = lax.broadcasted_iota(jnp.int32, pair.shape, 1) < DIM
        rows = [jnp.where(left, pair, 0.0), jnp.where(left, turn(pair), 0.0)]
        flipped = jnp.concatenate(rows, axis=0).T
        q_top[unit] = flipped.astype(BF16)
        q_low[unit] = jnp.concatenate([flipped[DIM:], flipped[:DIM]], axis=0).astype(BF16)

    arrived(bias_all.at[1 - core], bias_recv)

    def suffix(keep):
        row = lax.broadcasted_iota(jnp.int32, keep.shape, 0)
        product = keep
        for step in (1, 2, 4):
            moved = pltpu.roll(product, 8 - step, 0)
            product = product * jnp.where(row + step < 8, moved, 1.0)
        after = jnp.where(row + 1 < 8, pltpu.roll(product, 7, 0), 1.0)
        return after, product[0:1]

    def segment(block, bank, slot, width, bias, reach):
        keep = jnp.ones((8, 2 * width), F32)
        for i in range(RUN // 2):
            score = raw[bank, slot, 8 * i : 8 * i + 8, 0 : 2 * width] + bias
            if reach is not None:
                score = jnp.where(reach > -i, score, DEAD)
            odds = jnp.exp2(jnp.minimum(score, EXP_MAX))
            lose = 1.0 / (1.0 + odds)
            xs[bank, slot, 8 * i : 8 * i + 8, 0 : 2 * width] = odds * lose * keep
            keep = keep * lose
        near, far = keep[:, :width], keep[:, width:]
        after, whole = suffix(near * far)
        values = kv_all[block, 1]
        out = None
        for half, factor in enumerate((after, after * near)):
            part = xs[bank, slot, :, half * width : (half + 1) * width].reshape(RUN // 2, 8, width)
            weight = (part * factor[None]).reshape(HALF, width).astype(BF16)
            first = half * DIM
            value = jnp.concatenate(
                [values[first : first + DIM], values[LANES + first : LANES + first + DIM]], axis=1
            )
            term = jnp.dot(value, weight, preferred_element_type=F32)
            out = term if out is None else out + term
        return out, whole

    def cover(group, part, unit, diagonal, bank):
        count = 2
        width = count * LANES
        q = jnp.concatenate(
            [q_top[unit + n] for n in range(count)] + [q_low[unit + n] for n in range(count)],
            axis=1,
        )
        bias = bias_all[head_core, head_local]
        bias = jnp.concatenate([bias] * (2 * count), axis=1)
        if diagonal:
            lane = lax.broadcasted_iota(jnp.int32, (8, 2 * width), 1)
            row = lax.broadcasted_iota(jnp.int32, (8, 2 * width), 0)
            half, inside = lane // width, lax.rem(lane, width)
            owner = inside // LANES
            share = rows_of(chosen, core, group * NY + part + owner)
            query = SEG * owner + LANES * share + lax.rem(inside, LANES)
            reach = query - row * RUN - (RUN - 1) + half * (RUN // 2)
        first = group * NY + part
        raw[bank, :, :, 0 : 2 * width] = jnp.dot(
            kv_all[pl.ds(first, BATCH), 0].reshape(BATCH * HALF, LANES), q,
            preferred_element_type=F32,
        ).reshape(BATCH, HALF, 2 * width)
        acc = [seg_acc[group, unit + n] for n in range(count)]
        keep = [seg_keep[group, unit + n][0:1] for n in range(count)]
        for index in range(BATCH):
            limit = reach - SEG * index if diagonal else None
            out, whole = segment(first + index, bank, index, width, bias, limit)
            for n in range(count):
                lanes = slice(n * LANES, (n + 1) * LANES)
                acc[n] = acc[n] * whole[:, lanes] + out[:, lanes]
                keep[n] = keep[n] * whole[:, lanes]
        for n in range(count):
            seg_acc[group, unit + n] = acc[n]
            seg_keep[group, unit + n] = jnp.broadcast_to(keep[n], (8, LANES))

    def attend(group, part, between):
        def side(index, carry):
            tile = jnp.where(index == 0, low_tile, NZ - 1 - low_tile)
            base = index * SIDE

            @pl.when(group < tile)
            def _():
                cover(group, part, base, False, 0)
                cover(group, part, base + 2, False, 1)

            @pl.when(jnp.logical_and(group == tile, part == 0))
            def _():
                cover(group, part, base, True, 0)
                cover(group, part, base + 2, False, 1)

            @pl.when(jnp.logical_and(group == tile, part > 0))
            def _():
                cover(group, part, base + 2, True, 0)

            @pl.when(index == 0)
            def _():
                between()

            return carry

        lax.fori_loop(0, 2, side, 0)

    def stop_at(step):
        turn_of = lax.rem(step + 2, 4)
        far = step >= STEPS - 2
        distance = (step + 2) // 4
        own = step < 2
        behind = jnp.logical_or(jnp.logical_and(far, turn_of == 0), lax.rem(step, 2) == 0)
        part = jnp.where(jnp.logical_or(own, far), lax.rem(step, 2), turn_of // 2) * BATCH
        group = lax.rem(z + NZ + jnp.where(behind, -distance, distance), NZ)
        return group, part

    def forward(index):
        distance, turn_of = index // NZ + 1, lax.rem(index, NZ)
        last = distance == NZ // 2
        behind = lax.rem(index, 2) == 0
        part = jnp.where(last, lax.rem(index, 2) * BATCH, 0) + turn_of // 2
        group = lax.rem(z + NZ + jnp.where(behind, -distance, distance), NZ)
        block = group * NY + part
        arrived(kv_all.at[block, core], kv_recv.at[block])
        for way in range(2):
            onward = jnp.logical_or(
                distance < 3, jnp.logical_and(distance == 3, (part < BATCH) == (way == 0))
            )

            @pl.when(jnp.logical_and(behind == (way == 0), onward))
            def _():
                ring_copy(block, way).start()

        share_copy(block).start()

    def visit(step, carry):
        def forward_if(low, high, index):
            @pl.when(jnp.logical_and(step >= low, step < high))
            def _():
                forward(index)

        forward_if(1, 2, 0)
        forward_if(1, 2, 1)
        forward_if(2, STEPS - 2, 2 * step)

        @pl.when(step == STEPS // 2)
        def _():
            for part in range(2):
                relay(wo_copy, wfull, wo_recv, part, 3)
                relay(wo_copy, wfull, wo_recv, 1 - part, 1)

        @pl.when(step == STEPS - 2)
        def _():
            for part in range(2):
                relay(wo_copy, wfull, wo_recv, part, 2)

        group, part = stop_at(step)
        block = group * NY + part
        here = jnp.logical_and(block // BATCH == me // BATCH, mine)
        for short in range(2):

            @pl.when(here == (short == 1))
            def _():
                arrived(
                    kv_all.at[pl.ds(block, BATCH - short), 1 - core], kv_recv.at[pair_at(block)]
                )

        def between():
            forward_if(1, 2, 2)
            forward_if(1, 2, 3)
            forward_if(2, STEPS - 2, 2 * step + 1)

        attend(group, part, between)
        return carry

    lax.fori_loop(0, STEPS, visit, 0)

    def combine(unit):
        acc = seg_acc[0, unit]
        for group in range(1, NZ):
            acc = acc * seg_keep[group, unit][0:1] + seg_acc[group, unit]
        return acc

    for pair in range(UNITS // 2):
        flipped = jnp.concatenate([combine(2 * pair), combine(2 * pair + 1)], axis=0).T
        for part in range(2):
            upper = flipped[DIM * part : DIM * part + DIM // 2]
            lower = flipped[DIM * part + DIM // 2 : DIM * (part + 1)]
            for n, folded in enumerate(weave(upper, lower)):
                unit = 2 * pair + n
                packed[unit, part] = folded
                here = back_here(unit, part)

                @pl.when(here)
                def _():
                    att[my_slot] = folded

                @pl.when(jnp.logical_not(here))
                def _():
                    back_copy(unit, part).start()

    bias_copy.wait_send()
    arrived(wfull.at[pl.ds(0, n_tp - 1)], wo_send)
    arrived(tok.at[pl.ds(0, n_tp - 1)], tok_send)
    arrived(kv_own, kv_send)
    whole(UNITS, q_stays, q_all, q_send)
    for way in range(2):
        arrived(kv_all.at[pl.ds(0, 14), 0], ring_send.at[way])
    arrived(kv_all.at[pl.ds(0, n_sp - 1), 0], share_send)
    whole(2 * UNITS, back_stays, att, back_send)
    whole(2 * UNITS, back_stays, att, back_recv)

    for pair in range(n_tp):
        first, second = att[2 * pair].astype(F32), att[2 * pair + 1].astype(F32)
        cols = slice(pair * LANES, (pair + 1) * LANES)
        att_rows[0 : DIM // 2, cols], att_rows[DIM // 2 : DIM, cols] = weave(first, second)

    for part in range(2):
        arrived(wfull.at[pl.ds(0, 2)], wo_pair.at[part])

    def put(first):
        return pltpu.make_async_copy(
            mixed.at[:, pl.ds(first, COLS)], out_ref.at[:, pl.ds(first, COLS)],
            out_sem,
        )

    for first in range(0, out_ref.shape[1], COLS):
        w = wfull[:, :, :, first : first + COLS].reshape(att_rows.shape[1], COLS)
        mixed[:, first : first + COLS] = jnp.dot(
            att_rows[...], w, preferred_element_type=F32
        ).astype(BF16)
        put(first).start()
    pltpu.make_async_copy(mixed, out_ref, out_sem).wait()


def shards(tokens, w_query, w_key, w_value, head_bias, w_out):
    model, local_width = w_query.shape
    n_tp = lax.axis_size("tp")
    n_sp = lax.axis_size("sp")
    device_rows = tokens.shape[0]
    out_width = w_out.shape[1]

    smem = pl.BlockSpec(memory_space=pltpu.SMEM)
    anywhere = pl.BlockSpec(memory_space=pl.ANY)
    dma = pltpu.SemaphoreType.DMA

    def vmem(*shape):
        return pltpu.VMEM(shape, BF16)

    return pl.pallas_call(
        layer_kernel,
        out_shape=jax.ShapeDtypeStruct((device_rows, out_width), BF16),
        in_specs=[smem] + [anywhere] * 5,
        out_specs=anywhere,
        scratch_shapes=[
            vmem(n_tp, PARTS, device_rows // PARTS, model),
            vmem(model, 3 * local_width),
            vmem(n_tp, 2, local_width // 2, out_width),
            pltpu.VMEM((n_tp, device_rows, 3 * local_width), F32),
            pltpu.VMEM((2, 2, 8, LANES), F32),
            vmem(2, 2, HALF, LANES),
            vmem(2, SIDE, DIM, LANES),
            vmem(UNITS, DIM, LANES),
            vmem(n_sp, 2, HALF, LANES),
            vmem(UNITS, LANES, LANES),
            vmem(UNITS, LANES, LANES),
            pltpu.VMEM((2, BATCH, HALF, 4 * LANES), F32),
            pltpu.VMEM((2, BATCH, HALF, 4 * LANES), F32),
            pltpu.VMEM((NZ, UNITS, DIM, LANES), F32),
            pltpu.VMEM((NZ, UNITS, 8, LANES), F32),
            vmem(UNITS, 2, DIM // 2, LANES),
            vmem(2 * UNITS, DIM // 2, LANES),
            vmem(device_rows, n_tp * local_width),
            vmem(device_rows, out_width),
            pltpu.SemaphoreType.REGULAR,
            dma,
            dma((5,)),
            dma,
            dma((n_tp // 2, PARTS)),
            dma((2,)),
            dma,
            dma((n_tp // 2, 2)),
            dma((2,)),
            dma,
            dma,
            dma,
            dma((n_sp + n_sp // BATCH,)),
            dma((2,)),
            dma,
            dma,
            dma,
            dma,
            dma,
        ],
        compiler_params=pltpu.CompilerParams(
            collective_id=0, has_side_effects=True, vmem_limit_bytes=60 * 2**20
        ),
        name="layer",
    )(
        head_bias,
        tokens.reshape(PARTS, device_rows // PARTS, model),
        w_query, w_key, w_value,
        w_out.reshape(2, local_width // 2, out_width),
    )


def solution(mesh):
    placed = (
        P(("sp", "tp"), None),
        P(None, "tp"),
        P(None, "tp"),
        P(None, "tp"),
        P("tp"),
        P("tp", None),
    )
    return jax.shard_map(
        shards, mesh=mesh, in_specs=placed, out_specs=P(("sp", "tp"), None), check_vma=False
    )
```

```python
import functools
import math

import jax
import jax.numpy as jnp
from jax import lax
from jax.experimental import pallas as pl
from jax.experimental.pallas import tpu as pltpu
from jax.sharding import PartitionSpec as P

MESH = pl.DeviceIdType.MESH
F32, BF16 = jnp.float32, jnp.bfloat16
LOG2E = math.log2(math.e)
PARTS = 4
COLS = 512
EXP_MAX = 126.0
DEAD = -1e30
NZ, NY = 8, 4
SEG = 512
HALF = 256
LANES = 128
DIM = 64
RUN = 64
UNITS = 8
SIDE = 4
BATCH = 2
STEPS = NZ * NY // BATCH
INCOMING = (NZ - 1) * NY
EASE = 3


def layer_kernel(
    bias_ref, tokens_ref, wq_ref, wk_ref, wv_ref, wo_ref, out_ref,
    tok, wqkv, wfull, proj, bias_all, kv_own, q_own, q_all, kv_all, q_top, q_low, raw, xs,
    seg_acc, seg_keep, packed, att, att_rows, mixed,
    plane_sem, out_sem, load_sem, tok_send, tok_recv, tok_pair, wo_send, wo_recv, wo_pair,
    bias_send, bias_recv, kv_send, kv_recv, ring_send, share_send, q_send, q_recv, back_send, back_recv,
):
    me = lax.axis_index("sp")
    col = lax.axis_index("tp")
    n_sp, n_tp = NZ * NY, 8
    z, y = me // NY, lax.rem(me, NY)
    place, core = col // 2, lax.rem(col, 2)
    places = n_tp // 2
    sibling = place * 2 + 1 - core
    head_core, head_local = y // 2, lax.rem(y, 2)
    mine = core == head_core

    loads = [
        pltpu.make_async_copy(src, dst, load_sem.at[index])
        for index, (src, dst) in enumerate(
            [
                (tokens_ref, tok.at[col]),
                (wq_ref, wqkv.at[:, 0:LANES]),
                (wk_ref, wqkv.at[:, LANES : 2 * LANES]),
                (wv_ref, wqkv.at[:, 2 * LANES : 3 * LANES]),
                (wo_ref, wfull.at[col]),
            ]
        )
    ]
    for copy in loads:
        copy.start()

    barrier = pltpu.get_barrier_semaphore()
    for step in range(1, n_tp):
        pl.semaphore_signal(
            barrier, inc=1, device_id=(me, lax.rem(col + step, n_tp)), device_id_type=MESH
        )
    for step in range(1, NY):
        peer = z * NY + lax.rem(y + step, NY)
        for other in range(2):
            pl.semaphore_signal(
                barrier, inc=1, device_id=(peer, place * 2 + other), device_id_type=MESH
            )
    for step in range(1, NZ):
        peer = lax.rem(z + step, NZ) * NY + y
        pl.semaphore_signal(barrier, inc=1, device_id=(peer, col), device_id_type=MESH)
    for head in range(2):
        bias_all[core, head] = jnp.full((8, LANES), bias_ref[head] * LOG2E, F32)
    seg_acc[...] = jnp.zeros_like(seg_acc)
    seg_keep[...] = jnp.ones_like(seg_keep)
    pl.semaphore_wait(barrier, n_tp - 1 + 2 * (NY - 1) + NZ - 1)
    for step in range(1, NZ):
        peer = lax.rem(z + step, NZ) * NY + y
        pl.semaphore_signal(plane_sem, inc=1, device_id=(peer, col), device_id_type=MESH)

    def same_core(k):
        return lax.rem(place + k, places) * 2 + core

    def arrived(ref, sem):
        pltpu.make_async_copy(ref, ref, sem).wait()

    def link(kind, own, kept, sent, received, paired, part):
        if kind == 2:
            ahead = part < kept.shape[1] // 2
            block = same_core(3 if ahead else 1)
            src, target = kept.at[block, part], same_core(1 if ahead else 3)
        elif kind < places:
            src, block = own.at[part], col
            target = sibling if kind == 0 else same_core(kind)
        else:
            block = same_core(kind - places + 1)
            src, target = kept.at[block, part], sibling
        inside = kind == 0 or kind >= places
        return pltpu.make_async_remote_copy(
            src_ref=src, dst_ref=kept.at[block, part], send_sem=sent,
            recv_sem=paired.at[part % 2] if inside else received.at[block // 2, part],
            device_id=(me, target), device_id_type=MESH,
        )

    def token_copy(kind, part):
        return link(kind, tokens_ref, tok, tok_send, tok_recv, tok_pair, part)

    def wo_copy(kind, part):
        return link(kind, wo_ref, wfull, wo_send, wo_recv, wo_pair, part)

    def relay(copy, kept, received, part, k):
        block = same_core(k)
        arrived(kept.at[block, part], received.at[block // 2, part])
        copy(places + k - 1, part).start()
        if k != 2 and (part < kept.shape[1] // 2) == (k == 3):
            copy(2, part).start()

    bias_copy = pltpu.make_async_remote_copy(
        src_ref=bias_all.at[core], dst_ref=bias_all.at[core],
        send_sem=bias_send, recv_sem=bias_recv, device_id=(me, sibling), device_id_type=MESH,
    )

    turned = (2, 3, 0, 1)
    for part in range(PARTS // 2):
        token_copy(1, part).start()
        token_copy(3, turned[part]).start()
    for part in (0, 2, 1, 3):
        token_copy(0, part).start()
    bias_copy.start()

    def pair_at(block):
        return n_sp + block // BATCH

    def kv_copy(head, half, stage):
        aim = core * 2 + head
        own = aim == y
        sp = jnp.where(own, me, z * NY + aim)
        tp = jnp.where(own, sibling, place * 2 + half)
        return pltpu.make_async_remote_copy(
            src_ref=kv_own.at[head, half, pl.ds(LANES * (1 - stage), LANES)],
            dst_ref=kv_all.at[me, half, pl.ds(LANES * (1 - stage), LANES)],
            send_sem=kv_send,
            recv_sem=kv_recv.at[
                jnp.where(jnp.logical_and(own, core == half), pair_at(me), me)
            ],
            device_id=(sp, tp), device_id_type=MESH,
        )

    def ring_copy(block, way):
        peer = lax.rem(z + (1 if way == 0 else NZ - 1), NZ) * NY + y
        return pltpu.make_async_remote_copy(
            src_ref=kv_all.at[block, core], dst_ref=kv_all.at[block, core],
            send_sem=ring_send.at[way], recv_sem=kv_recv.at[block],
            device_id=(peer, col), device_id_type=MESH,
        )

    def share_copy(block):
        return pltpu.make_async_remote_copy(
            src_ref=kv_all.at[block, core], dst_ref=kv_all.at[block, core],
            send_sem=share_send, recv_sem=kv_recv.at[pair_at(block)],
            device_id=(me, sibling), device_id_type=MESH,
        )

    def keeper(tile, chosen):
        low = jnp.minimum(tile, NZ - 1 - tile)
        return lax.rem(2 * low + chosen + 5, NZ)

    low_tile = lax.rem(z + 3, NZ) // 2
    chosen = lax.rem(z + 3, 2)

    def rows_of(of_chosen, of_core, block):
        return lax.rem(2 * of_chosen + of_core + block, SIDE)

    def unit_block(unit):
        tile = jnp.where(unit >= SIDE, NZ - 1 - low_tile, low_tile)
        return tile * NY + lax.rem(unit, SIDE)

    def q_copy(head, step):
        to_chosen, to_core = step // 2, step % 2
        unit = jnp.where(z >= NZ // 2, SIDE, 0) + y
        return pltpu.make_async_remote_copy(
            src_ref=q_own.at[head, rows_of(to_chosen, to_core, me)], dst_ref=q_all.at[unit],
            send_sem=q_send, recv_sem=q_recv,
            device_id=(
                keeper(z, to_chosen) * NY + core * 2 + head, place * 2 + to_core
            ), device_id_type=MESH,
        )

    def q_here(head, step):
        to_chosen, to_core = step // 2, step % 2
        return jnp.logical_and(
            keeper(z, to_chosen) * NY + core * 2 + head == me, core == to_core
        )

    q_stays = jnp.logical_and(mine, jnp.logical_or(keeper(z, 0) == z, keeper(z, 1) == z))
    my_slot = place * NY + y

    def back_owner(unit, part):
        return rows_of(chosen, core, unit_block(unit)) * 2 + part

    def back_here(unit, part):
        return jnp.logical_and(unit_block(unit) == me, back_owner(unit, part) == col)

    back_stays = jnp.logical_and(
        jnp.logical_or(low_tile == z, NZ - 1 - low_tile == z), rows_of(chosen, core, me) == place
    )

    def back_copy(unit, part):
        return pltpu.make_async_remote_copy(
            src_ref=packed.at[unit, part], dst_ref=att.at[my_slot],
            send_sem=back_send, recv_sem=back_recv,
            device_id=(unit_block(unit), back_owner(unit, part)), device_id_type=MESH,
        )

    for copy in loads:
        copy.wait()
    def turn(value):
        return pltpu.roll(value, DIM, 1)

    def weave(upper, lower):
        left = lax.broadcasted_iota(jnp.int32, upper.shape, 1) < DIM
        first = jnp.where(left, upper, turn(lower)).astype(BF16)
        second = jnp.where(left, turn(upper), lower).astype(BF16)
        return first, second

    def strided(i, kind):
        return proj[:, RUN - 1 - i, kind * LANES : (kind + 1) * LANES]

    for part in range(PARTS // 2):
        relay(token_copy, tok, tok_recv, part, 3)
        token_copy(1, part + 2).start()
        relay(token_copy, tok, tok_recv, turned[part], 1)
        token_copy(3, turned[part + 2]).start()
    for stage in range(2):
        parts = (stage, stage + 2)
        relay(token_copy, tok, tok_recv, stage + 2, 3)
        relay(token_copy, tok, tok_recv, turned[stage + 2], 1)
        for part in parts:
            relay(token_copy, tok, tok_recv, part, 2)
        arrived(tok.at[pl.ds(0, 2)], tok_pair.at[stage])
        depth, model = tok.shape[2:]
        x = jnp.concatenate([tok[:, part].reshape(n_tp * depth, model) for part in parts], axis=0)
        both = jnp.dot(x, wqkv[...], preferred_element_type=F32)
        for index, part in enumerate(parts):
            proj[:, part * depth : (part + 1) * depth, :] = both[
                index * n_tp * depth : (index + 1) * n_tp * depth
            ].reshape(n_tp, depth, 3 * LANES)
        if stage == 1:
            for share in range(SIDE):
                upper = proj[2 * share, :, 0:LANES] * (LOG2E * DIM ** (-0.5))
                lower = proj[2 * share + 1, :, 0:LANES] * (LOG2E * DIM ** (-0.5))
                q_own[0, share], q_own[1, share] = weave(upper, lower)
            pl.semaphore_wait(plane_sem, NZ - 1)
            for head in range(2):
                for step in range(4):
                    here = q_here(head, step)

                    @pl.when(jnp.logical_not(here))
                    def _():
                        q_copy(head, step).start()

                    @pl.when(here)
                    def _():
                        q_all[jnp.where(z >= NZ // 2, SIDE, 0) + y] = q_own[
                            head, rows_of(step // 2, step % 2, me)
                        ]

        base = 16 * (1 - stage)
        for i in range(base, base + 16, 2):
            upper = jnp.concatenate([strided(i, 1), strided(i + 1, 1)], axis=0)
            lower = jnp.concatenate([strided(i + 32, 1), strided(i + 33, 1)], axis=0)
            kv_own[0, 0, 8 * i : 8 * i + 16], kv_own[1, 0, 8 * i : 8 * i + 16] = weave(
                upper, lower
            )
        for head in range(2):
            kv_copy(head, 0, stage).start()
        for index in range(2):
            first = base + 32 * index
            block = jnp.concatenate([strided(first + i, 2) for i in range(16)], axis=0)
            flipped = block.T.astype(BF16)
            at = LANES * (1 - stage) + DIM * index
            for head in range(2):
                kv_own[head, 1, at : at + DIM] = flipped[DIM * head : DIM * (head + 1)]
        for head in range(2):
            kv_copy(head, 1, stage).start()

    for part in range(2):
        for kind in (1, 3, 0):
            wo_copy(kind, 1 - part if kind == 3 else part).start()

    for head in range(2):

        @pl.when(core * 2 + head == y)
        def _():
            kv_all[me] = kv_own[head]

    def halves_here(block):
        return jnp.logical_and(block == me, mine)

    for step in range(NY):
        block = z * NY + lax.rem(y + step, NY)

        @pl.when(jnp.logical_not(halves_here(block)))
        def _():
            arrived(kv_all.at[block, core], kv_recv.at[block])

        for way in range(2):
            ring_copy(block, way).start()

        @pl.when(block != me)
        def _():
            share_copy(block).start()

    def whole(count, less, buffer, sem):
        for short in range(2):

            @pl.when(less == (short == 1))
            def _():
                arrived(buffer.at[pl.ds(0, count - short)], sem)

    whole(UNITS, q_stays, q_all, q_recv)

    for unit in range(UNITS):
        pair = q_all[unit].astype(F32)
        left = lax.broadcasted_iota(jnp.int32, pair.shape, 1) < DIM
        rows = [jnp.where(left, pair, 0.0), jnp.where(left, turn(pair), 0.0)]
        flipped = jnp.concatenate(rows, axis=0).T
        q_top[unit] = flipped.astype(BF16)
        q_low[unit] = jnp.concatenate([flipped[DIM:], flipped[:DIM]], axis=0).astype(BF16)

    arrived(bias_all.at[1 - core], bias_recv)

    def suffix(keep):
        row = lax.broadcasted_iota(jnp.int32, keep.shape, 0)
        product = keep
        for step in (1, 2, 4):
            moved = pltpu.roll(product, 8 - step, 0)
            product = product * jnp.where(row + step < 8, moved, 1.0)
        after = jnp.where(row + 1 < 8, pltpu.roll(product, 7, 0), 1.0)
        return after, product[0:1]

    def segment(block, bank, slot, width, bias, reach):
        keep = jnp.ones((8, 2 * width), F32)
        for i in range(RUN // 2):
            score = raw[bank, slot, 8 * i : 8 * i + 8, 0 : 2 * width] + bias
            if reach is not None:
                score = jnp.where(reach > -i, score, DEAD)
            odds = jnp.exp2(jnp.minimum(score, EXP_MAX))
            lose = 1.0 / (1.0 + odds)
            xs[bank, slot, 8 * i : 8 * i + 8, 0 : 2 * width] = odds * lose * keep
            keep = keep * lose
        near, far = keep[:, :width], keep[:, width:]
        after, whole = suffix(near * far)
        values = kv_all[block, 1]
        out = None
        for half, factor in enumerate((after, after * near)):
            part = xs[bank, slot, :, half * width : (half + 1) * width].reshape(RUN // 2, 8, width)
            weight = (part * factor[None]).reshape(HALF, width).astype(BF16)
            first = half * DIM
            value = jnp.concatenate(
                [values[first : first + DIM], values[LANES + first : LANES + first + DIM]], axis=1
            )
            term = jnp.dot(value, weight, preferred_element_type=F32)
            out = term if out is None else out + term
        return out, whole

    def cover(group, part, unit, diagonal, bank):
        count = 2
        width = count * LANES
        q = jnp.concatenate(
            [q_top[unit + n] for n in range(count)] + [q_low[unit + n] for n in range(count)],
            axis=1,
        )
        bias = bias_all[head_core, head_local]
        bias = jnp.concatenate([bias] * (2 * count), axis=1)
        if diagonal:
            lane = lax.broadcasted_iota(jnp.int32, (8, 2 * width), 1)
            row = lax.broadcasted_iota(jnp.int32, (8, 2 * width), 0)
            half, inside = lane // width, lax.rem(lane, width)
            owner = inside // LANES
            share = rows_of(chosen, core, group * NY + part + owner)
            query = SEG * owner + LANES * share + lax.rem(inside, LANES)
            reach = query - row * RUN - (RUN - 1) + half * (RUN // 2)
        first = group * NY + part
        raw[bank, :, :, 0 : 2 * width] = jnp.dot(
            kv_all[pl.ds(first, BATCH), 0].reshape(BATCH * HALF, LANES), q,
            preferred_element_type=F32,
        ).reshape(BATCH, HALF, 2 * width)
        acc = [seg_acc[group, unit + n] for n in range(count)]
        keep = [seg_keep[group, unit + n][0:1] for n in range(count)]
        for index in range(BATCH):
            limit = reach - SEG * index if diagonal else None
            out, whole = segment(first + index, bank, index, width, bias, limit)
            for n in range(count):
                lanes = slice(n * LANES, (n + 1) * LANES)
                acc[n] = acc[n] * whole[:, lanes] + out[:, lanes]
                keep[n] = keep[n] * whole[:, lanes]
        for n in range(count):
            seg_acc[group, unit + n] = acc[n]
            seg_keep[group, unit + n] = jnp.broadcast_to(keep[n], (8, LANES))

    def attend(group, part, state):
        def side(index, state):
            passed, done = state
            tile = jnp.where(index == 0, low_tile, NZ - 1 - low_tile)
            base = index * SIDE

            @pl.when(group < tile)
            def _():
                cover(group, part, base, False, 0)
                cover(group, part, base + 2, False, 1)

            @pl.when(jnp.logical_and(group == tile, part == 0))
            def _():
                cover(group, part, base, True, 0)
                cover(group, part, base + 2, False, 1)

            @pl.when(jnp.logical_and(group == tile, part > 0))
            def _():
                cover(group, part, base + 2, True, 0)

            busy = jnp.where(group <= tile, 1, 0)
            done = done + busy
            more = jnp.where(done >= EASE, 2 * busy, 0)
            return forward_to(passed, jnp.minimum(passed + more, INCOMING)), done

        return lax.fori_loop(0, 2, side, state)

    def stop_at(step):
        turn_of = lax.rem(step + 2, 4)
        far = step >= STEPS - 2
        distance = (step + 2) // 4
        own = step < 2
        behind = jnp.logical_or(jnp.logical_and(far, turn_of == 0), lax.rem(step, 2) == 0)
        part = jnp.where(jnp.logical_or(own, far), lax.rem(step, 2), turn_of // 2) * BATCH
        group = lax.rem(z + NZ + jnp.where(behind, -distance, distance), NZ)
        return group, part

    def forward(index):
        distance, turn_of = index // NZ + 1, lax.rem(index, NZ)
        last = distance == NZ // 2
        behind = lax.rem(index, 2) == 0
        part = jnp.where(last, lax.rem(index, 2) * BATCH, 0) + turn_of // 2
        group = lax.rem(z + NZ + jnp.where(behind, -distance, distance), NZ)
        block = group * NY + part
        arrived(kv_all.at[block, core], kv_recv.at[block])
        for way in range(2):
            onward = jnp.logical_or(
                distance < 3, jnp.logical_and(distance == 3, (part < BATCH) == (way == 0))
            )

            @pl.when(jnp.logical_and(behind == (way == 0), onward))
            def _():
                ring_copy(block, way).start()

        share_copy(block).start()

    def forward_to(passed, target):
        def one(index, carry):
            forward(index)
            return carry

        target = jnp.maximum(passed, target)
        lax.fori_loop(passed, target, one, 0)
        return target

    def visit(step, state):
        passed, done = state
        needed = jnp.where(step < 2, 0, 2 * step - 1 - lax.rem(step, 2))
        passed = forward_to(passed, needed)

        @pl.when(step == STEPS // 2)
        def _():
            for part in range(2):
                relay(wo_copy, wfull, wo_recv, part, 3)
                relay(wo_copy, wfull, wo_recv, 1 - part, 1)

        @pl.when(step == STEPS - 2)
        def _():
            for part in range(2):
                relay(wo_copy, wfull, wo_recv, part, 2)

        group, part = stop_at(step)
        block = group * NY + part
        here = jnp.logical_and(block // BATCH == me // BATCH, mine)
        for short in range(2):

            @pl.when(here == (short == 1))
            def _():
                arrived(
                    kv_all.at[pl.ds(block, BATCH - short), 1 - core], kv_recv.at[pair_at(block)]
                )

        return attend(group, part, (passed, done))

    lax.fori_loop(0, STEPS, visit, (jnp.int32(0), jnp.int32(0)))

    def combine(unit):
        acc = seg_acc[0, unit]
        for group in range(1, NZ):
            acc = acc * seg_keep[group, unit][0:1] + seg_acc[group, unit]
        return acc

    for pair in range(UNITS // 2):
        flipped = jnp.concatenate([combine(2 * pair), combine(2 * pair + 1)], axis=0).T
        for part in range(2):
            upper = flipped[DIM * part : DIM * part + DIM // 2]
            lower = flipped[DIM * part + DIM // 2 : DIM * (part + 1)]
            for n, folded in enumerate(weave(upper, lower)):
                unit = 2 * pair + n
                packed[unit, part] = folded
                here = back_here(unit, part)

                @pl.when(here)
                def _():
                    att[my_slot] = folded

                @pl.when(jnp.logical_not(here))
                def _():
                    back_copy(unit, part).start()

    bias_copy.wait_send()
    arrived(wfull.at[pl.ds(0, n_tp - 1)], wo_send)
    arrived(tok.at[pl.ds(0, n_tp - 1)], tok_send)
    arrived(kv_own, kv_send)
    whole(UNITS, q_stays, q_all, q_send)
    for way in range(2):
        arrived(kv_all.at[pl.ds(0, 14), 0], ring_send.at[way])
    arrived(kv_all.at[pl.ds(0, n_sp - 1), 0], share_send)
    whole(2 * UNITS, back_stays, att, back_send)
    whole(2 * UNITS, back_stays, att, back_recv)

    for pair in range(n_tp):
        first, second = att[2 * pair].astype(F32), att[2 * pair + 1].astype(F32)
        cols = slice(pair * LANES, (pair + 1) * LANES)
        att_rows[0 : DIM // 2, cols], att_rows[DIM // 2 : DIM, cols] = weave(first, second)

    for part in range(2):
        arrived(wfull.at[pl.ds(0, 2)], wo_pair.at[part])

    def put(first):
        return pltpu.make_async_copy(
            mixed.at[:, pl.ds(first, COLS)], out_ref.at[:, pl.ds(first, COLS)],
            out_sem,
        )

    for first in range(0, out_ref.shape[1], COLS):
        w = wfull[:, :, :, first : first + COLS].reshape(att_rows.shape[1], COLS)
        mixed[:, first : first + COLS] = jnp.dot(
            att_rows[...], w, preferred_element_type=F32
        ).astype(BF16)
        put(first).start()
    pltpu.make_async_copy(mixed, out_ref, out_sem).wait()


def shards(tokens, w_query, w_key, w_value, head_bias, w_out):
    model, local_width = w_query.shape
    n_tp = lax.axis_size("tp")
    n_sp = lax.axis_size("sp")
    device_rows = tokens.shape[0]
    out_width = w_out.shape[1]

    smem = pl.BlockSpec(memory_space=pltpu.SMEM)
    anywhere = pl.BlockSpec(memory_space=pl.ANY)
    dma = pltpu.SemaphoreType.DMA

    def vmem(*shape):
        return pltpu.VMEM(shape, BF16)

    return pl.pallas_call(
        layer_kernel,
        out_shape=jax.ShapeDtypeStruct((device_rows, out_width), BF16),
        in_specs=[smem] + [anywhere] * 5,
        out_specs=anywhere,
        scratch_shapes=[
            vmem(n_tp, PARTS, device_rows // PARTS, model),
            vmem(model, 3 * local_width),
            vmem(n_tp, 2, local_width // 2, out_width),
            pltpu.VMEM((n_tp, device_rows, 3 * local_width), F32),
            pltpu.VMEM((2, 2, 8, LANES), F32),
            vmem(2, 2, HALF, LANES),
            vmem(2, SIDE, DIM, LANES),
            vmem(UNITS, DIM, LANES),
            vmem(n_sp, 2, HALF, LANES),
            vmem(UNITS, LANES, LANES),
            vmem(UNITS, LANES, LANES),
            pltpu.VMEM((2, BATCH, HALF, 4 * LANES), F32),
            pltpu.VMEM((2, BATCH, HALF, 4 * LANES), F32),
            pltpu.VMEM((NZ, UNITS, DIM, LANES), F32),
            pltpu.VMEM((NZ, UNITS, 8, LANES), F32),
            vmem(UNITS, 2, DIM // 2, LANES),
            vmem(2 * UNITS, DIM // 2, LANES),
            vmem(device_rows, n_tp * local_width),
            vmem(device_rows, out_width),
            pltpu.SemaphoreType.REGULAR,
            dma,
            dma((5,)),
            dma,
            dma((n_tp // 2, PARTS)),
            dma((2,)),
            dma,
            dma((n_tp // 2, 2)),
            dma((2,)),
            dma,
            dma,
            dma,
            dma((n_sp + n_sp // BATCH,)),
            dma((2,)),
            dma,
            dma,
            dma,
            dma,
            dma,
        ],
        compiler_params=pltpu.CompilerParams(
            collective_id=0, has_side_effects=True, vmem_limit_bytes=60 * 2**20
        ),
        name="layer",
    )(
        head_bias,
        tokens.reshape(PARTS, device_rows // PARTS, model),
        w_query, w_key, w_value,
        w_out.reshape(2, local_width // 2, out_width),
    )


def solution(mesh):
    placed = (
        P(("sp", "tp"), None),
        P(None, "tp"),
        P(None, "tp"),
        P(None, "tp"),
        P("tp"),
        P("tp", None),
    )
    return jax.shard_map(
        shards, mesh=mesh, in_specs=placed, out_specs=P(("sp", "tp"), None), check_vma=False
    )
```

```python
import functools
import math

import jax
import jax.numpy as jnp
from jax import lax
from jax.experimental import pallas as pl
from jax.experimental.pallas import tpu as pltpu
from jax.sharding import PartitionSpec as P

MESH = pl.DeviceIdType.MESH
F32, BF16 = jnp.float32, jnp.bfloat16
LOG2E = math.log2(math.e)
PARTS = 4
COLS = 512
EXP_MAX = 126.0
DEAD = -1e30
NZ, NY = 8, 4
SEG = 512
HALF = 256
LANES = 128
DIM = 64
RUN = 64
SHARE = 32
SHARES = SEG // SHARE
TILES = 8
FAR = 1 << 20
BATCH = 2
STEPS = NZ * NY // BATCH


def layer_kernel(
    bias_ref, tokens_ref, wq_ref, wk_ref, wv_ref, wo_ref, out_ref,
    tok, wqkv, wfull, proj, bias_all, kv_own, q_own, q_all, kv_all, q_top, q_low, raw, xs,
    seg_acc, seg_keep, packed, att, att_rows, mixed,
    plane_sem, out_sem, load_sem, tok_send, tok_recv, tok_pair, wo_send, wo_recv, wo_pair,
    bias_send, bias_recv, kv_send, kv_recv, ring_send, share_send, q_send, q_recv, back_send, back_recv,
):
    me = lax.axis_index("sp")
    col = lax.axis_index("tp")
    n_sp, n_tp = NZ * NY, 8
    z, y = me // NY, lax.rem(me, NY)
    place, core = col // 2, lax.rem(col, 2)
    places = n_tp // 2
    sibling = place * 2 + 1 - core
    head_core, head_local = y // 2, lax.rem(y, 2)
    mine = core == head_core

    loads = [
        pltpu.make_async_copy(src, dst, load_sem.at[index])
        for index, (src, dst) in enumerate(
            [
                (tokens_ref, tok.at[col]),
                (wq_ref, wqkv.at[:, 0:LANES]),
                (wk_ref, wqkv.at[:, LANES : 2 * LANES]),
                (wv_ref, wqkv.at[:, 2 * LANES : 3 * LANES]),
                (wo_ref, wfull.at[col]),
            ]
        )
    ]
    for copy in loads:
        copy.start()

    barrier = pltpu.get_barrier_semaphore()
    for step in range(1, n_tp):
        pl.semaphore_signal(
            barrier, inc=1, device_id=(me, lax.rem(col + step, n_tp)), device_id_type=MESH
        )
    for step in range(1, NY):
        peer = z * NY + lax.rem(y + step, NY)
        for other in range(2):
            pl.semaphore_signal(
                barrier, inc=1, device_id=(peer, place * 2 + other), device_id_type=MESH
            )
    for step in range(1, NZ):
        peer = lax.rem(z + step, NZ) * NY + y
        pl.semaphore_signal(barrier, inc=1, device_id=(peer, col), device_id_type=MESH)
    for head in range(2):
        bias_all[core, head] = jnp.full((8, LANES), bias_ref[head] * LOG2E, F32)
    seg_acc[...] = jnp.zeros_like(seg_acc)
    seg_keep[...] = jnp.ones_like(seg_keep)
    pl.semaphore_wait(barrier, n_tp - 1 + 2 * (NY - 1) + NZ - 1)
    for step in range(1, NZ):
        peer = lax.rem(z + step, NZ) * NY + y
        pl.semaphore_signal(plane_sem, inc=1, device_id=(peer, col), device_id_type=MESH)

    def same_core(k):
        return lax.rem(place + k, places) * 2 + core

    def arrived(ref, sem):
        pltpu.make_async_copy(ref, ref, sem).wait()

    def link(kind, own, kept, sent, received, paired, part):
        if kind == 2:
            ahead = part < kept.shape[1] // 2
            block = same_core(3 if ahead else 1)
            src, target = kept.at[block, part], same_core(1 if ahead else 3)
        elif kind < places:
            src, block = own.at[part], col
            target = sibling if kind == 0 else same_core(kind)
        else:
            block = same_core(kind - places + 1)
            src, target = kept.at[block, part], sibling
        inside = kind == 0 or kind >= places
        return pltpu.make_async_remote_copy(
            src_ref=src, dst_ref=kept.at[block, part], send_sem=sent,
            recv_sem=paired.at[part % 2] if inside else received.at[block // 2, part],
            device_id=(me, target), device_id_type=MESH,
        )

    def token_copy(kind, part):
        return link(kind, tokens_ref, tok, tok_send, tok_recv, tok_pair, part)

    def wo_copy(kind, part):
        return link(kind, wo_ref, wfull, wo_send, wo_recv, wo_pair, part)

    def relay(copy, kept, received, part, k):
        block = same_core(k)
        arrived(kept.at[block, part], received.at[block // 2, part])
        copy(places + k - 1, part).start()
        if k != 2 and (part < kept.shape[1] // 2) == (k == 3):
            copy(2, part).start()

    bias_copy = pltpu.make_async_remote_copy(
        src_ref=bias_all.at[core], dst_ref=bias_all.at[core],
        send_sem=bias_send, recv_sem=bias_recv, device_id=(me, sibling), device_id_type=MESH,
    )

    turned = (2, 3, 0, 1)
    for part in range(PARTS // 2):
        token_copy(1, part).start()
        token_copy(3, turned[part]).start()
    for part in (0, 2, 1, 3):
        token_copy(0, part).start()
    bias_copy.start()

    def pair_at(block):
        return n_sp + block // BATCH

    def early_at(part):
        return n_sp + n_sp // BATCH + part

    def own_copy(block, way, stage):
        peer = lax.rem(z + (1 if way == 0 else NZ - 1), NZ) * NY + y
        rows = pl.ds(LANES * (1 - stage), LANES)
        return pltpu.make_async_remote_copy(
            src_ref=kv_all.at[block, core, rows], dst_ref=kv_all.at[block, core, rows],
            send_sem=ring_send.at[way], recv_sem=kv_recv.at[block],
            device_id=(peer, col), device_id_type=MESH,
        )

    def kv_copy(head, half, stage):
        aim = core * 2 + head
        own = aim == y
        sp = jnp.where(own, me, z * NY + aim)
        tp = jnp.where(own, sibling, place * 2 + half)
        return pltpu.make_async_remote_copy(
            src_ref=kv_own.at[head, half, pl.ds(LANES * (1 - stage), LANES)],
            dst_ref=kv_all.at[me, half, pl.ds(LANES * (1 - stage), LANES)],
            send_sem=kv_send,
            recv_sem=kv_recv.at[
                jnp.where(
                    jnp.logical_and(own, core == half),
                    pair_at(me),
                    early_at(y) if stage == 0 else me,
                )
            ],
            device_id=(sp, tp), device_id_type=MESH,
        )

    def ring_copy(block, way):
        peer = lax.rem(z + (1 if way == 0 else NZ - 1), NZ) * NY + y
        return pltpu.make_async_remote_copy(
            src_ref=kv_all.at[block, core], dst_ref=kv_all.at[block, core],
            send_sem=ring_send.at[way], recv_sem=kv_recv.at[block],
            device_id=(peer, col), device_id_type=MESH,
        )

    def share_copy(block):
        return pltpu.make_async_remote_copy(
            src_ref=kv_all.at[block, core], dst_ref=kv_all.at[block, core],
            send_sem=share_send, recv_sem=kv_recv.at[pair_at(block)],
            device_id=(me, sibling), device_id_type=MESH,
        )

    def rows_of(to_z, to_core, block):
        return lax.rem(2 * to_z + to_core + 2 * block, SHARES)

    def q_copy(head, step):
        to_z, to_core = step // 2, lax.rem(step, 2)
        return pltpu.make_async_remote_copy(
            src_ref=q_own.at[head, rows_of(to_z, to_core, me)], dst_ref=q_all.at[me],
            send_sem=q_send, recv_sem=q_recv,
            device_id=(to_z * NY + core * 2 + head, place * 2 + to_core), device_id_type=MESH,
        )

    def q_here(head, step):
        to_z, to_core = step // 2, lax.rem(step, 2)
        return jnp.logical_and(to_z * NY + core * 2 + head == me, to_core == core)

    def back_owner(block):
        return lax.rem(z + block, n_tp)

    my_slot = (place * NY + y) * 2 + core

    def back_here(block):
        return jnp.logical_and(block == me, back_owner(block) == col)

    def back_copy(block):
        return pltpu.make_async_remote_copy(
            src_ref=packed.at[block], dst_ref=att.at[my_slot],
            send_sem=back_send, recv_sem=back_recv,
            device_id=(block, back_owner(block)), device_id_type=MESH,
        )

    for copy in loads:
        copy.wait()
    def turn(value):
        return pltpu.roll(value, DIM, 1)

    lane16 = lax.broadcasted_iota(jnp.int32, (16, LANES), 1)

    def weave(upper, lower):
        first = jnp.where(lane16 < DIM, upper, turn(lower)).astype(BF16)
        second = jnp.where(lane16 < DIM, turn(upper), lower).astype(BF16)
        return first, second

    def strided(i, kind):
        return proj[:, RUN - 1 - i, kind * LANES : (kind + 1) * LANES]

    def send_q(step, carry):
        for head in range(2):

            @pl.when(jnp.logical_not(q_here(head, step)))
            def _():
                q_copy(head, step).start()

        return carry

    for part in range(PARTS // 2):
        relay(token_copy, tok, tok_recv, part, 3)
        token_copy(1, part + 2).start()
        relay(token_copy, tok, tok_recv, turned[part], 1)
        token_copy(3, turned[part + 2]).start()
    for stage in range(2):
        parts = (stage, stage + 2)
        relay(token_copy, tok, tok_recv, stage + 2, 3)
        relay(token_copy, tok, tok_recv, turned[stage + 2], 1)
        for part in parts:
            relay(token_copy, tok, tok_recv, part, 2)
        arrived(tok.at[pl.ds(0, 2)], tok_pair.at[stage])
        depth, model = tok.shape[2:]
        x = jnp.concatenate([tok[:, part].reshape(n_tp * depth, model) for part in parts], axis=0)
        both = jnp.dot(x, wqkv[...], preferred_element_type=F32)
        for index, part in enumerate(parts):
            proj[:, part * depth : (part + 1) * depth, :] = both[
                index * n_tp * depth : (index + 1) * n_tp * depth
            ].reshape(n_tp, depth, 3 * LANES)
        if stage == 1:
            for share in range(SHARES):
                block, first = share // 2, 32 * (share % 2)
                q = proj[block, first : first + 32, 0:LANES] * (LOG2E * DIM ** (-0.5))
                q_own[0, share], q_own[1, share] = weave(q[:16], q[16:])
            pl.semaphore_wait(plane_sem, NZ - 1)
            lax.fori_loop(0, 2 * NZ, send_q, 0)
        base = 16 * (1 - stage)
        for i in range(base, base + 16, 2):
            upper = jnp.concatenate([strided(i, 1), strided(i + 1, 1)], axis=0)
            lower = jnp.concatenate([strided(i + 32, 1), strided(i + 33, 1)], axis=0)
            kv_own[0, 0, 8 * i : 8 * i + 16], kv_own[1, 0, 8 * i : 8 * i + 16] = weave(
                upper, lower
            )
        for head in range(2):
            kv_copy(head, 0, stage).start()
        for index in range(2):
            first = base + 32 * index
            block = jnp.concatenate([strided(first + i, 2) for i in range(16)], axis=0)
            flipped = block.T.astype(BF16)
            at = LANES * (1 - stage) + DIM * index
            for head in range(2):
                kv_own[head, 1, at : at + DIM] = flipped[DIM * head : DIM * (head + 1)]
        for head in range(2):
            kv_copy(head, 1, stage).start()

    for part in range(2):
        for kind in (1, 3, 0):
            wo_copy(kind, 1 - part if kind == 3 else part).start()

    for head in range(2):

        @pl.when(core * 2 + head == y)
        def _():
            kv_all[me] = kv_own[head]
            q_all[me] = q_own[head, rows_of(z, core, me)]

    def halves_here(block):
        return jnp.logical_and(block == me, mine)

    for stage in range(2):
        for step in range(NY):
            part = lax.rem(y + step, NY)
            block = z * NY + part
            rows = pl.ds(LANES * (1 - stage), LANES)

            @pl.when(jnp.logical_not(halves_here(block)))
            def _():
                arrived(
                    kv_all.at[block, core, rows],
                    kv_recv.at[early_at(part) if stage == 0 else block],
                )

            for way in range(2):
                own_copy(block, way, stage).start()

            if stage == 1:

                @pl.when(block != me)
                def _():
                    share_copy(block).start()

    def whole(count, less, buffer, sem):
        for short in range(2):

            @pl.when(less == (short == 1))
            def _():
                arrived(buffer.at[pl.ds(0, count - short)], sem)

    whole(n_sp, mine, q_all, q_recv)

    for tile in range(TILES):
        pieces = []
        for part in range(NY):
            pair = q_all[tile * NY + part].astype(F32)
            pieces.append(jnp.where(lane16 < DIM, pair, 0.0))
            pieces.append(jnp.where(lane16 < DIM, turn(pair), 0.0))
        flipped = jnp.concatenate(pieces, axis=0).T
        q_top[tile] = flipped.astype(BF16)
        q_low[tile] = jnp.concatenate([flipped[DIM:], flipped[:DIM]], axis=0).astype(BF16)

    arrived(bias_all.at[1 - core], bias_recv)

    def suffix(keep):
        row = lax.broadcasted_iota(jnp.int32, keep.shape, 0)
        product = keep
        for step in (1, 2, 4):
            moved = pltpu.roll(product, 8 - step, 0)
            product = product * jnp.where(row + step < 8, moved, 1.0)
        after = jnp.where(row + 1 < 8, pltpu.roll(product, 7, 0), 1.0)
        return after, product[0:1]

    def segment(block, bank, slot, width, bias, reach):
        keep = jnp.ones((8, 2 * width), F32)
        for i in range(RUN // 2):
            score = raw[bank, slot, 8 * i : 8 * i + 8, 0 : 2 * width] + bias
            if reach is not None:
                score = jnp.where(reach > -i, score, DEAD)
            odds = jnp.exp2(jnp.minimum(score, EXP_MAX))
            lose = 1.0 / (1.0 + odds)
            xs[bank, slot, 8 * i : 8 * i + 8, 0 : 2 * width] = odds * lose * keep
            keep = keep * lose
        near, far = keep[:, :width], keep[:, width:]
        after, whole = suffix(near * far)
        values = kv_all[block, 1]
        out = None
        for half, factor in enumerate((after, after * near)):
            part = xs[bank, slot, :, half * width : (half + 1) * width].reshape(RUN // 2, 8, width)
            weight = (part * factor[None]).reshape(HALF, width).astype(BF16)
            first = half * DIM
            value = jnp.concatenate(
                [values[first : first + DIM], values[LANES + first : LANES + first + DIM]], axis=1
            )
            term = jnp.dot(value, weight, preferred_element_type=F32)
            out = term if out is None else out + term
        return out, whole

    def cover(group, part, tile, count, diagonal, bank):
        width = count * LANES
        q = jnp.concatenate(
            [q_top[tile + n] for n in range(count)] + [q_low[tile + n] for n in range(count)],
            axis=1,
        )
        bias = bias_all[head_core, head_local]
        bias = jnp.concatenate([bias] * (2 * count), axis=1)
        if diagonal:
            lane = lax.broadcasted_iota(jnp.int32, (8, 2 * width), 1)
            row = lax.broadcasted_iota(jnp.int32, (8, 2 * width), 0)
            half = lane // width
            inside = lax.rem(lane, width)
            owner = lax.rem(inside // SHARE, NY)
            share = rows_of(z, core, tile * NY + owner)
            query = SEG * owner + SHARE * share + lax.rem(inside, SHARE)
            query = jnp.where(inside < LANES, query, FAR)
            reach = query - row * RUN - (RUN - 1) + half * (RUN // 2) - SEG * part
        first = group * NY + part
        raw[bank, :, :, 0 : 2 * width] = jnp.dot(
            kv_all[pl.ds(first, BATCH), 0].reshape(BATCH * HALF, LANES), q,
            preferred_element_type=F32,
        ).reshape(BATCH, HALF, 2 * width)
        acc = [seg_acc[group, tile + n] for n in range(count)]
        keep = [seg_keep[group, tile + n][0:1] for n in range(count)]
        for index in range(BATCH):
            limit = reach - SEG * index if diagonal else None
            out, whole = segment(first + index, bank, index, width, bias, limit)
            for n in range(count):
                lanes = slice(n * LANES, (n + 1) * LANES)
                acc[n] = acc[n] * whole[:, lanes] + out[:, lanes]
                keep[n] = keep[n] * whole[:, lanes]
        for n in range(count):
            seg_acc[group, tile + n] = acc[n]
            seg_keep[group, tile + n] = jnp.broadcast_to(keep[n], (8, LANES))

    def attend(group, part, between):
        count = TILES - group
        odd = lax.rem(count, 2)
        pairs = (count - 1) // 2
        first = group + 2 - odd

        for single in range(2):
            for more in range(2):

                @pl.when(jnp.logical_and(odd == single, (pairs > 0) == (more == 1)))
                def _():
                    cover(group, part, group, 2 - single, True, 0)
                    if more:
                        cover(group, part, first, 2, False, 1)

        between()

        @pl.when(pairs == 2)
        def _():
            cover(group, part, first + 2, 2, False, 0)

        @pl.when(pairs == 3)
        def _():
            cover(group, part, first + 2, 2, False, 0)
            cover(group, part, first + 4, 2, False, 1)

    def stop_at(step):
        turn_of = lax.rem(step + 2, 4)
        far = step >= STEPS - 2
        distance = (step + 2) // 4
        own = step < 2
        behind = jnp.logical_or(jnp.logical_and(far, turn_of == 0), lax.rem(step, 2) == 0)
        part = jnp.where(jnp.logical_or(own, far), lax.rem(step, 2), turn_of // 2) * BATCH
        group = lax.rem(z + NZ + jnp.where(behind, -distance, distance), NZ)
        return group, part

    def forward(index):
        distance, turn_of = index // NZ + 1, lax.rem(index, NZ)
        last = distance == NZ // 2
        behind = lax.rem(index, 2) == 0
        part = jnp.where(last, lax.rem(index, 2) * BATCH, 0) + turn_of // 2
        group = lax.rem(z + NZ + jnp.where(behind, -distance, distance), NZ)
        block = group * NY + part
        arrived(kv_all.at[block, core], kv_recv.at[block])
        for way in range(2):
            onward = jnp.logical_or(
                distance < 3, jnp.logical_and(distance == 3, (part < BATCH) == (way == 0))
            )

            @pl.when(jnp.logical_and(behind == (way == 0), onward))
            def _():
                ring_copy(block, way).start()

        share_copy(block).start()

    def visit(step, carry):
        def forward_if(low, high, index):
            @pl.when(jnp.logical_and(step >= low, step < high))
            def _():
                forward(index)

        forward_if(1, 2, 0)
        forward_if(1, 2, 1)
        forward_if(2, STEPS - 2, 2 * step)

        @pl.when(step == STEPS // 2)
        def _():
            for part in range(2):
                relay(wo_copy, wfull, wo_recv, part, 3)
                relay(wo_copy, wfull, wo_recv, 1 - part, 1)

        @pl.when(step == STEPS - 2)
        def _():
            for part in range(2):
                relay(wo_copy, wfull, wo_recv, part, 2)

        group, part = stop_at(step)
        block = group * NY + part
        here = jnp.logical_and(block // BATCH == me // BATCH, mine)
        for short in range(2):

            @pl.when(here == (short == 1))
            def _():
                arrived(
                    kv_all.at[pl.ds(block, BATCH - short), 1 - core], kv_recv.at[pair_at(block)]
                )

        def between():
            forward_if(1, 2, 2)
            forward_if(1, 2, 3)
            forward_if(2, STEPS - 2, 2 * step + 1)

        attend(group, part, between)
        return carry

    lax.fori_loop(0, STEPS, visit, 0)

    def combine(tile):
        acc = seg_acc[0, tile]
        for group in range(1, NZ):
            acc = acc * seg_keep[group, tile][0:1] + seg_acc[group, tile]
        return acc

    for pair in range(TILES // 2):
        flipped = jnp.concatenate([combine(2 * pair), combine(2 * pair + 1)], axis=0).T
        for part in range(NY):
            upper = flipped[SHARE * part : SHARE * part + 16]
            lower = flipped[SHARE * part + 16 : SHARE * (part + 1)]
            for n, folded in enumerate(weave(upper, lower)):
                block = (2 * pair + n) * NY + part
                packed[block] = folded
                here = back_here(block)

                @pl.when(here)
                def _():
                    att[my_slot] = folded

                @pl.when(jnp.logical_not(here))
                def _():
                    back_copy(block).start()

    bias_copy.wait_send()
    arrived(wfull.at[pl.ds(0, n_tp - 1)], wo_send)
    arrived(tok.at[pl.ds(0, n_tp - 1)], tok_send)
    arrived(kv_own, kv_send)
    whole(n_sp, mine, q_all, q_send)
    for way in range(2):
        arrived(kv_all.at[pl.ds(0, 14), 0], ring_send.at[way])
    arrived(kv_all.at[pl.ds(0, n_sp - 1), 0], share_send)
    whole(n_sp, back_here(me), att, back_send)
    whole(n_sp, back_here(me), att, back_recv)

    for pair in range(n_tp):
        for sub in range(2):
            values = []
            for head in (2 * pair, 2 * pair + 1):
                slot = head * 2 + sub
                values.append(att[slot].astype(F32))
            top = jnp.where(lane16 < DIM, values[0], turn(values[1]))
            low = jnp.where(lane16 < DIM, turn(values[0]), values[1])
            cols = slice(pair * LANES, (pair + 1) * LANES)
            att_rows[SHARE * sub : SHARE * sub + 16, cols] = top.astype(BF16)
            att_rows[SHARE * sub + 16 : SHARE * (sub + 1), cols] = low.astype(BF16)

    for part in range(2):
        arrived(wfull.at[pl.ds(0, 2)], wo_pair.at[part])

    def put(first):
        return pltpu.make_async_copy(
            mixed.at[:, pl.ds(first, COLS)], out_ref.at[:, pl.ds(first, COLS)],
            out_sem,
        )

    for first in range(0, out_ref.shape[1], COLS):
        w = wfull[:, :, :, first : first + COLS].reshape(att_rows.shape[1], COLS)
        mixed[:, first : first + COLS] = jnp.dot(
            att_rows[...], w, preferred_element_type=F32
        ).astype(BF16)
        put(first).start()
    pltpu.make_async_copy(mixed, out_ref, out_sem).wait()


def shards(tokens, w_query, w_key, w_value, head_bias, w_out):
    model, local_width = w_query.shape
    n_tp = lax.axis_size("tp")
    n_sp = lax.axis_size("sp")
    device_rows = tokens.shape[0]
    out_width = w_out.shape[1]

    smem = pl.BlockSpec(memory_space=pltpu.SMEM)
    anywhere = pl.BlockSpec(memory_space=pl.ANY)
    dma = pltpu.SemaphoreType.DMA

    def vmem(*shape):
        return pltpu.VMEM(shape, BF16)

    return pl.pallas_call(
        layer_kernel,
        out_shape=jax.ShapeDtypeStruct((device_rows, out_width), BF16),
        in_specs=[smem] + [anywhere] * 5,
        out_specs=anywhere,
        scratch_shapes=[
            vmem(n_tp, PARTS, device_rows // PARTS, model),
            vmem(model, 3 * local_width),
            vmem(n_tp, 2, local_width // 2, out_width),
            pltpu.VMEM((n_tp, device_rows, 3 * local_width), F32),
            pltpu.VMEM((2, 2, 8, LANES), F32),
            vmem(2, 2, HALF, LANES),
            vmem(2, SHARES, SHARE // 2, LANES),
            vmem(n_sp, SHARE // 2, LANES),
            vmem(n_sp, 2, HALF, LANES),
            vmem(TILES, LANES, LANES),
            vmem(TILES, LANES, LANES),
            pltpu.VMEM((2, BATCH, HALF, 4 * LANES), F32),
            pltpu.VMEM((2, BATCH, HALF, 4 * LANES), F32),
            pltpu.VMEM((NZ, TILES, DIM, LANES), F32),
            pltpu.VMEM((NZ, TILES, 8, LANES), F32),
            vmem(n_sp, SHARE // 2, LANES),
            vmem(32, SHARE // 2, LANES),
            vmem(device_rows, n_tp * local_width),
            vmem(device_rows, out_width),
            pltpu.SemaphoreType.REGULAR,
            dma,
            dma((5,)),
            dma,
            dma((n_tp // 2, PARTS)),
            dma((2,)),
            dma,
            dma((n_tp // 2, 2)),
            dma((2,)),
            dma,
            dma,
            dma,
            dma((n_sp + n_sp // BATCH + NY,)),
            dma((2,)),
            dma,
            dma,
            dma,
            dma,
            dma,
        ],
        compiler_params=pltpu.CompilerParams(
            collective_id=0, has_side_effects=True, vmem_limit_bytes=60 * 2**20
        ),
        name="layer",
    )(
        head_bias,
        tokens.reshape(PARTS, device_rows // PARTS, model),
        w_query, w_key, w_value,
        w_out.reshape(2, local_width // 2, out_width),
    )


def solution(mesh):
    placed = (
        P(("sp", "tp"), None),
        P(None, "tp"),
        P(None, "tp"),
        P(None, "tp"),
        P("tp"),
        P("tp", None),
    )
    return jax.shard_map(
        shards, mesh=mesh, in_specs=placed, out_specs=P(("sp", "tp"), None), check_vma=False
    )
```

```python
import functools
import math

import jax
import jax.numpy as jnp
from jax import lax
from jax.experimental import pallas as pl
from jax.experimental.pallas import tpu as pltpu
from jax.sharding import PartitionSpec as P

MESH = pl.DeviceIdType.MESH
F32, BF16 = jnp.float32, jnp.bfloat16
LOG2E = math.log2(math.e)
PARTS = 4
COLS = 512
EXP_MAX = 126.0
DEAD = -1e30
NZ, NY = 8, 4
SEG = 512
HALF = 256
LANES = 128
DIM = 64
RUN = 64
SHARE = 32
SHARES = SEG // SHARE
TILES = 8
FAR = 1 << 20
BATCH = 2
STEPS = NZ * NY // BATCH


def layer_kernel(
    bias_ref, tokens_ref, wq_ref, wk_ref, wv_ref, wo_ref, out_ref,
    tok, wqkv, wfull, proj, bias_all, kv_own, q_own, q_all, kv_all, q_top, q_low, raw, xs,
    seg_acc, seg_keep, packed, att, att_rows, mixed,
    plane_sem, out_sem, load_sem, tok_send, tok_recv, tok_pair, wo_send, wo_recv, wo_pair,
    bias_send, bias_recv, kv_send, kv_recv, ring_send, share_send, q_send, q_recv, back_send, back_recv,
):
    me = lax.axis_index("sp")
    col = lax.axis_index("tp")
    n_sp, n_tp = NZ * NY, 8
    z, y = me // NY, lax.rem(me, NY)
    place, core = col // 2, lax.rem(col, 2)
    places = n_tp // 2
    sibling = place * 2 + 1 - core
    head_core, head_local = y // 2, lax.rem(y, 2)
    mine = core == head_core

    loads = [
        pltpu.make_async_copy(src, dst, load_sem.at[index])
        for index, (src, dst) in enumerate(
            [
                (tokens_ref, tok.at[col]),
                (wq_ref, wqkv.at[:, 0:LANES]),
                (wk_ref, wqkv.at[:, LANES : 2 * LANES]),
                (wv_ref, wqkv.at[:, 2 * LANES : 3 * LANES]),
                (wo_ref, wfull.at[col]),
            ]
        )
    ]
    for copy in loads:
        copy.start()

    barrier = pltpu.get_barrier_semaphore()
    for step in range(1, n_tp):
        pl.semaphore_signal(
            barrier, inc=1, device_id=(me, lax.rem(col + step, n_tp)), device_id_type=MESH
        )
    for step in range(1, NY):
        peer = z * NY + lax.rem(y + step, NY)
        for other in range(2):
            pl.semaphore_signal(
                barrier, inc=1, device_id=(peer, place * 2 + other), device_id_type=MESH
            )
    for step in range(1, NZ):
        peer = lax.rem(z + step, NZ) * NY + y
        pl.semaphore_signal(barrier, inc=1, device_id=(peer, col), device_id_type=MESH)
    for head in range(2):
        bias_all[core, head] = jnp.full((8, LANES), bias_ref[head] * LOG2E, F32)
    seg_acc[...] = jnp.zeros_like(seg_acc)
    seg_keep[...] = jnp.ones_like(seg_keep)
    pl.semaphore_wait(barrier, n_tp - 1 + 2 * (NY - 1) + NZ - 1)
    for step in range(1, NZ):
        peer = lax.rem(z + step, NZ) * NY + y
        pl.semaphore_signal(plane_sem, inc=1, device_id=(peer, col), device_id_type=MESH)

    def same_core(k):
        return lax.rem(place + k, places) * 2 + core

    def arrived(ref, sem):
        pltpu.make_async_copy(ref, ref, sem).wait()

    def link(kind, own, kept, sent, received, paired, part):
        if kind == 2:
            ahead = part < kept.shape[1] // 2
            block = same_core(3 if ahead else 1)
            src, target = kept.at[block, part], same_core(1 if ahead else 3)
        elif kind < places:
            src, block = own.at[part], col
            target = sibling if kind == 0 else same_core(kind)
        else:
            block = same_core(kind - places + 1)
            src, target = kept.at[block, part], sibling
        inside = kind == 0 or kind >= places
        return pltpu.make_async_remote_copy(
            src_ref=src, dst_ref=kept.at[block, part], send_sem=sent,
            recv_sem=paired.at[part % 2] if inside else received.at[block // 2, part],
            device_id=(me, target), device_id_type=MESH,
        )

    def token_copy(kind, part):
        return link(kind, tokens_ref, tok, tok_send, tok_recv, tok_pair, part)

    def wo_copy(kind, part):
        return link(kind, wo_ref, wfull, wo_send, wo_recv, wo_pair, part)

    def relay(copy, kept, received, part, k):
        block = same_core(k)
        arrived(kept.at[block, part], received.at[block // 2, part])
        copy(places + k - 1, part).start()
        if k != 2 and (part < kept.shape[1] // 2) == (k == 3):
            copy(2, part).start()

    bias_copy = pltpu.make_async_remote_copy(
        src_ref=bias_all.at[core], dst_ref=bias_all.at[core],
        send_sem=bias_send, recv_sem=bias_recv, device_id=(me, sibling), device_id_type=MESH,
    )

    turned = (2, 3, 0, 1)
    for part in range(PARTS // 2):
        token_copy(1, part).start()
        token_copy(3, turned[part]).start()
    for part in (0, 2, 1, 3):
        token_copy(0, part).start()
    bias_copy.start()

    def pair_at(block):
        return n_sp + block // BATCH

    def early_at(part):
        return n_sp + n_sp // BATCH + part

    def own_copy(block, way, stage):
        peer = lax.rem(z + (1 if way == 0 else NZ - 1), NZ) * NY + y
        rows = pl.ds(LANES * (1 - stage), LANES)
        return pltpu.make_async_remote_copy(
            src_ref=kv_all.at[block, core, rows], dst_ref=kv_all.at[block, core, rows],
            send_sem=ring_send.at[way], recv_sem=kv_recv.at[block],
            device_id=(peer, col), device_id_type=MESH,
        )

    def kv_copy(head, half, stage):
        aim = core * 2 + head
        own = aim == y
        sp = jnp.where(own, me, z * NY + aim)
        tp = jnp.where(own, sibling, place * 2 + half)
        return pltpu.make_async_remote_copy(
            src_ref=kv_own.at[head, half, pl.ds(LANES * (1 - stage), LANES)],
            dst_ref=kv_all.at[me, half, pl.ds(LANES * (1 - stage), LANES)],
            send_sem=kv_send,
            recv_sem=kv_recv.at[
                jnp.where(
                    jnp.logical_and(own, core == half),
                    pair_at(me),
                    early_at(y) if stage == 0 else me,
                )
            ],
            device_id=(sp, tp), device_id_type=MESH,
        )

    def ring_copy(block, way):
        peer = lax.rem(z + (1 if way == 0 else NZ - 1), NZ) * NY + y
        return pltpu.make_async_remote_copy(
            src_ref=kv_all.at[block, core], dst_ref=kv_all.at[block, core],
            send_sem=ring_send.at[way], recv_sem=kv_recv.at[block],
            device_id=(peer, col), device_id_type=MESH,
        )

    def share_copy(block):
        return pltpu.make_async_remote_copy(
            src_ref=kv_all.at[block, core], dst_ref=kv_all.at[block, core],
            send_sem=share_send, recv_sem=kv_recv.at[pair_at(block)],
            device_id=(me, sibling), device_id_type=MESH,
        )

    def rows_of(to_z, to_core, block):
        return lax.rem(2 * to_z + to_core + 2 * block, SHARES)

    def q_copy(head, step):
        to_z, to_core = step // 2, lax.rem(step, 2)
        return pltpu.make_async_remote_copy(
            src_ref=q_own.at[head, rows_of(to_z, to_core, me)], dst_ref=q_all.at[me],
            send_sem=q_send, recv_sem=q_recv,
            device_id=(to_z * NY + core * 2 + head, place * 2 + to_core), device_id_type=MESH,
        )

    def q_here(head, step):
        to_z, to_core = step // 2, lax.rem(step, 2)
        return jnp.logical_and(to_z * NY + core * 2 + head == me, to_core == core)

    def back_owner(block):
        return lax.rem(z + block, n_tp)

    my_slot = (place * NY + y) * 2 + core

    def back_here(block):
        return jnp.logical_and(block == me, back_owner(block) == col)

    def back_copy(block):
        return pltpu.make_async_remote_copy(
            src_ref=packed.at[block], dst_ref=att.at[my_slot],
            send_sem=back_send, recv_sem=back_recv,
            device_id=(block, back_owner(block)), device_id_type=MESH,
        )

    for copy in loads:
        copy.wait()
    def turn(value):
        return pltpu.roll(value, DIM, 1)

    lane16 = lax.broadcasted_iota(jnp.int32, (16, LANES), 1)

    def weave(upper, lower):
        first = jnp.where(lane16 < DIM, upper, turn(lower)).astype(BF16)
        second = jnp.where(lane16 < DIM, turn(upper), lower).astype(BF16)
        return first, second

    def strided(i, kind):
        return proj[:, RUN - 1 - i, kind * LANES : (kind + 1) * LANES]

    def send_q(stage, to_z, carry):
        step = 2 * to_z + stage
        for head in range(2):

            @pl.when(jnp.logical_not(q_here(head, step)))
            def _():
                q_copy(head, step).start()

        return carry

    for part in range(PARTS // 2):
        relay(token_copy, tok, tok_recv, part, 3)
        token_copy(1, part + 2).start()
        relay(token_copy, tok, tok_recv, turned[part], 1)
        token_copy(3, turned[part + 2]).start()
    for stage in range(2):
        parts = (stage, stage + 2)
        relay(token_copy, tok, tok_recv, stage + 2, 3)
        relay(token_copy, tok, tok_recv, turned[stage + 2], 1)
        for part in parts:
            relay(token_copy, tok, tok_recv, part, 2)
        arrived(tok.at[pl.ds(0, 2)], tok_pair.at[stage])
        depth, model = tok.shape[2:]
        x = jnp.concatenate([tok[:, part].reshape(n_tp * depth, model) for part in parts], axis=0)
        both = jnp.dot(x, wqkv[...], preferred_element_type=F32)
        for index, part in enumerate(parts):
            proj[:, part * depth : (part + 1) * depth, :] = both[
                index * n_tp * depth : (index + 1) * n_tp * depth
            ].reshape(n_tp, depth, 3 * LANES)
        for block in range(n_tp):
            scale = LOG2E * DIM ** (-0.5)
            upper = proj[block, 16 * stage : 16 * stage + 16, 0:LANES] * scale
            lower = proj[block, 16 * stage + 32 : 16 * stage + 48, 0:LANES] * scale
            share = 2 * block + stage
            q_own[0, share], q_own[1, share] = weave(upper, lower)
        if stage == 0:
            pl.semaphore_wait(plane_sem, NZ - 1)
        lax.fori_loop(0, NZ, functools.partial(send_q, stage), 0)
        base = 16 * (1 - stage)
        for i in range(base, base + 16, 2):
            upper = jnp.concatenate([strided(i, 1), strided(i + 1, 1)], axis=0)
            lower = jnp.concatenate([strided(i + 32, 1), strided(i + 33, 1)], axis=0)
            kv_own[0, 0, 8 * i : 8 * i + 16], kv_own[1, 0, 8 * i : 8 * i + 16] = weave(
                upper, lower
            )
        for head in range(2):
            kv_copy(head, 0, stage).start()
        for index in range(2):
            first = base + 32 * index
            block = jnp.concatenate([strided(first + i, 2) for i in range(16)], axis=0)
            flipped = block.T.astype(BF16)
            at = LANES * (1 - stage) + DIM * index
            for head in range(2):
                kv_own[head, 1, at : at + DIM] = flipped[DIM * head : DIM * (head + 1)]
        for head in range(2):
            kv_copy(head, 1, stage).start()

    for part in range(2):
        for kind in (1, 3, 0):
            wo_copy(kind, 1 - part if kind == 3 else part).start()

    for head in range(2):

        @pl.when(core * 2 + head == y)
        def _():
            kv_all[me] = kv_own[head]
            q_all[me] = q_own[head, rows_of(z, core, me)]

    def halves_here(block):
        return jnp.logical_and(block == me, mine)

    for stage in range(2):
        for step in range(NY):
            part = lax.rem(y + step, NY)
            block = z * NY + part
            rows = pl.ds(LANES * (1 - stage), LANES)

            @pl.when(jnp.logical_not(halves_here(block)))
            def _():
                arrived(
                    kv_all.at[block, core, rows],
                    kv_recv.at[early_at(part) if stage == 0 else block],
                )

            for way in range(2):
                own_copy(block, way, stage).start()

            if stage == 1:

                @pl.when(block != me)
                def _():
                    share_copy(block).start()

    def whole(count, less, buffer, sem):
        for short in range(2):

            @pl.when(less == (short == 1))
            def _():
                arrived(buffer.at[pl.ds(0, count - short)], sem)

    whole(n_sp, mine, q_all, q_recv)

    for tile in range(TILES):
        pieces = []
        for part in range(NY):
            pair = q_all[tile * NY + part].astype(F32)
            pieces.append(jnp.where(lane16 < DIM, pair, 0.0))
            pieces.append(jnp.where(lane16 < DIM, turn(pair), 0.0))
        flipped = jnp.concatenate(pieces, axis=0).T
        q_top[tile] = flipped.astype(BF16)
        q_low[tile] = jnp.concatenate([flipped[DIM:], flipped[:DIM]], axis=0).astype(BF16)

    arrived(bias_all.at[1 - core], bias_recv)

    def suffix(keep):
        row = lax.broadcasted_iota(jnp.int32, keep.shape, 0)
        product = keep
        for step in (1, 2, 4):
            moved = pltpu.roll(product, 8 - step, 0)
            product = product * jnp.where(row + step < 8, moved, 1.0)
        after = jnp.where(row + 1 < 8, pltpu.roll(product, 7, 0), 1.0)
        return after, product[0:1]

    def segment(block, bank, slot, width, bias, reach):
        keep = jnp.ones((8, 2 * width), F32)
        for i in range(RUN // 2):
            score = raw[bank, slot, 8 * i : 8 * i + 8, 0 : 2 * width] + bias
            if reach is not None:
                score = jnp.where(reach > -i, score, DEAD)
            odds = jnp.exp2(jnp.minimum(score, EXP_MAX))
            lose = 1.0 / (1.0 + odds)
            xs[bank, slot, 8 * i : 8 * i + 8, 0 : 2 * width] = odds * lose * keep
            keep = keep * lose
        near, far = keep[:, :width], keep[:, width:]
        after, whole = suffix(near * far)
        values = kv_all[block, 1]
        out = None
        for half, factor in enumerate((after, after * near)):
            part = xs[bank, slot, :, half * width : (half + 1) * width].reshape(RUN // 2, 8, width)
            weight = (part * factor[None]).reshape(HALF, width).astype(BF16)
            first = half * DIM
            value = jnp.concatenate(
                [values[first : first + DIM], values[LANES + first : LANES + first + DIM]], axis=1
            )
            term = jnp.dot(value, weight, preferred_element_type=F32)
            out = term if out is None else out + term
        return out, whole

    def cover(group, part, tile, count, diagonal, bank):
        width = count * LANES
        q = jnp.concatenate(
            [q_top[tile + n] for n in range(count)] + [q_low[tile + n] for n in range(count)],
            axis=1,
        )
        bias = bias_all[head_core, head_local]
        bias = jnp.concatenate([bias] * (2 * count), axis=1)
        if diagonal:
            lane = lax.broadcasted_iota(jnp.int32, (8, 2 * width), 1)
            row = lax.broadcasted_iota(jnp.int32, (8, 2 * width), 0)
            half = lane // width
            inside = lax.rem(lane, width)
            owner = lax.rem(inside // SHARE, NY)
            share = rows_of(z, core, tile * NY + owner)
            place_in = 32 * (lax.rem(inside, SHARE) // 16) + lax.rem(inside, 16)
            query = SEG * owner + 64 * (share // 2) + 16 * lax.rem(share, 2) + place_in
            query = jnp.where(inside < LANES, query, FAR)
            reach = query - row * RUN - (RUN - 1) + half * (RUN // 2) - SEG * part
        first = group * NY + part
        raw[bank, :, :, 0 : 2 * width] = jnp.dot(
            kv_all[pl.ds(first, BATCH), 0].reshape(BATCH * HALF, LANES), q,
            preferred_element_type=F32,
        ).reshape(BATCH, HALF, 2 * width)
        acc = [seg_acc[group, tile + n] for n in range(count)]
        keep = [seg_keep[group, tile + n][0:1] for n in range(count)]
        for index in range(BATCH):
            limit = reach - SEG * index if diagonal else None
            out, whole = segment(first + index, bank, index, width, bias, limit)
            for n in range(count):
                lanes = slice(n * LANES, (n + 1) * LANES)
                acc[n] = acc[n] * whole[:, lanes] + out[:, lanes]
                keep[n] = keep[n] * whole[:, lanes]
        for n in range(count):
            seg_acc[group, tile + n] = acc[n]
            seg_keep[group, tile + n] = jnp.broadcast_to(keep[n], (8, LANES))

    def attend(group, part, between):
        count = TILES - group
        odd = lax.rem(count, 2)
        pairs = (count - 1) // 2
        first = group + 2 - odd

        for single in range(2):
            for more in range(2):

                @pl.when(jnp.logical_and(odd == single, (pairs > 0) == (more == 1)))
                def _():
                    cover(group, part, group, 2 - single, True, 0)
                    if more:
                        cover(group, part, first, 2, False, 1)

        between()

        @pl.when(pairs == 2)
        def _():
            cover(group, part, first + 2, 2, False, 0)

        @pl.when(pairs == 3)
        def _():
            cover(group, part, first + 2, 2, False, 0)
            cover(group, part, first + 4, 2, False, 1)

    def stop_at(step):
        turn_of = lax.rem(step + 2, 4)
        far = step >= STEPS - 2
        distance = (step + 2) // 4
        own = step < 2
        behind = jnp.logical_or(jnp.logical_and(far, turn_of == 0), lax.rem(step, 2) == 0)
        part = jnp.where(jnp.logical_or(own, far), lax.rem(step, 2), turn_of // 2) * BATCH
        group = lax.rem(z + NZ + jnp.where(behind, -distance, distance), NZ)
        return group, part

    def forward(index):
        distance, turn_of = index // NZ + 1, lax.rem(index, NZ)
        last = distance == NZ // 2
        behind = lax.rem(index, 2) == 0
        part = jnp.where(last, lax.rem(index, 2) * BATCH, 0) + turn_of // 2
        group = lax.rem(z + NZ + jnp.where(behind, -distance, distance), NZ)
        block = group * NY + part
        arrived(kv_all.at[block, core], kv_recv.at[block])
        for way in range(2):
            onward = jnp.logical_or(
                distance < 3, jnp.logical_and(distance == 3, (part < BATCH) == (way == 0))
            )

            @pl.when(jnp.logical_and(behind == (way == 0), onward))
            def _():
                ring_copy(block, way).start()

        share_copy(block).start()

    def visit(step, carry):
        def forward_if(low, high, index):
            @pl.when(jnp.logical_and(step >= low, step < high))
            def _():
                forward(index)

        forward_if(2, 3, 2)
        forward_if(2, 3, 3)
        forward_if(3, STEPS - 2, 2 * step)

        @pl.when(step == STEPS // 2)
        def _():
            for part in range(2):
                relay(wo_copy, wfull, wo_recv, part, 3)
                relay(wo_copy, wfull, wo_recv, 1 - part, 1)

        @pl.when(step == STEPS - 2)
        def _():
            for part in range(2):
                relay(wo_copy, wfull, wo_recv, part, 2)

        group, part = stop_at(step)
        block = group * NY + part
        here = jnp.logical_and(block // BATCH == me // BATCH, mine)
        for short in range(2):

            @pl.when(here == (short == 1))
            def _():
                arrived(
                    kv_all.at[pl.ds(block, BATCH - short), 1 - core], kv_recv.at[pair_at(block)]
                )

        def between():
            forward_if(1, 2, 0)
            forward_if(1, 2, 1)
            forward_if(2, 3, 4)
            forward_if(2, STEPS - 2, 2 * step + 1)

        attend(group, part, between)
        return carry

    lax.fori_loop(0, STEPS, visit, 0)

    def combine(tile):
        acc = seg_acc[0, tile]
        for group in range(1, NZ):
            acc = acc * seg_keep[group, tile][0:1] + seg_acc[group, tile]
        return acc

    for pair in range(TILES // 2):
        flipped = jnp.concatenate([combine(2 * pair), combine(2 * pair + 1)], axis=0).T
        for part in range(NY):
            upper = flipped[SHARE * part : SHARE * part + 16]
            lower = flipped[SHARE * part + 16 : SHARE * (part + 1)]
            for n, folded in enumerate(weave(upper, lower)):
                block = (2 * pair + n) * NY + part
                packed[block] = folded
                here = back_here(block)

                @pl.when(here)
                def _():
                    att[my_slot] = folded

                @pl.when(jnp.logical_not(here))
                def _():
                    back_copy(block).start()

    bias_copy.wait_send()
    arrived(wfull.at[pl.ds(0, n_tp - 1)], wo_send)
    arrived(tok.at[pl.ds(0, n_tp - 1)], tok_send)
    arrived(kv_own, kv_send)
    whole(n_sp, mine, q_all, q_send)
    for way in range(2):
        arrived(kv_all.at[pl.ds(0, 14), 0], ring_send.at[way])
    arrived(kv_all.at[pl.ds(0, n_sp - 1), 0], share_send)
    whole(n_sp, back_here(me), att, back_send)
    whole(n_sp, back_here(me), att, back_recv)

    for pair in range(n_tp):
        for sub in range(2):
            values = []
            for head in (2 * pair, 2 * pair + 1):
                slot = head * 2 + sub
                values.append(att[slot].astype(F32))
            top = jnp.where(lane16 < DIM, values[0], turn(values[1]))
            low = jnp.where(lane16 < DIM, turn(values[0]), values[1])
            cols = slice(pair * LANES, (pair + 1) * LANES)
            att_rows[16 * sub : 16 * sub + 16, cols] = top.astype(BF16)
            att_rows[16 * sub + 32 : 16 * sub + 48, cols] = low.astype(BF16)

    for part in range(2):
        arrived(wfull.at[pl.ds(0, 2)], wo_pair.at[part])

    def put(first):
        return pltpu.make_async_copy(
            mixed.at[:, pl.ds(first, COLS)], out_ref.at[:, pl.ds(first, COLS)],
            out_sem,
        )

    for first in range(0, out_ref.shape[1], COLS):
        w = wfull[:, :, :, first : first + COLS].reshape(att_rows.shape[1], COLS)
        mixed[:, first : first + COLS] = jnp.dot(
            att_rows[...], w, preferred_element_type=F32
        ).astype(BF16)
        put(first).start()
    pltpu.make_async_copy(mixed, out_ref, out_sem).wait()


def shards(tokens, w_query, w_key, w_value, head_bias, w_out):
    model, local_width = w_query.shape
    n_tp = lax.axis_size("tp")
    n_sp = lax.axis_size("sp")
    device_rows = tokens.shape[0]
    out_width = w_out.shape[1]

    smem = pl.BlockSpec(memory_space=pltpu.SMEM)
    anywhere = pl.BlockSpec(memory_space=pl.ANY)
    dma = pltpu.SemaphoreType.DMA

    def vmem(*shape):
        return pltpu.VMEM(shape, BF16)

    return pl.pallas_call(
        layer_kernel,
        out_shape=jax.ShapeDtypeStruct((device_rows, out_width), BF16),
        in_specs=[smem] + [anywhere] * 5,
        out_specs=anywhere,
        scratch_shapes=[
            vmem(n_tp, PARTS, device_rows // PARTS, model),
            vmem(model, 3 * local_width),
            vmem(n_tp, 2, local_width // 2, out_width),
            pltpu.VMEM((n_tp, device_rows, 3 * local_width), F32),
            pltpu.VMEM((2, 2, 8, LANES), F32),
            vmem(2, 2, HALF, LANES),
            vmem(2, SHARES, SHARE // 2, LANES),
            vmem(n_sp, SHARE // 2, LANES),
            vmem(n_sp, 2, HALF, LANES),
            vmem(TILES, LANES, LANES),
            vmem(TILES, LANES, LANES),
            pltpu.VMEM((2, BATCH, HALF, 4 * LANES), F32),
            pltpu.VMEM((2, BATCH, HALF, 4 * LANES), F32),
            pltpu.VMEM((NZ, TILES, DIM, LANES), F32),
            pltpu.VMEM((NZ, TILES, 8, LANES), F32),
            vmem(n_sp, SHARE // 2, LANES),
            vmem(32, SHARE // 2, LANES),
            vmem(device_rows, n_tp * local_width),
            vmem(device_rows, out_width),
            pltpu.SemaphoreType.REGULAR,
            dma,
            dma((5,)),
            dma,
            dma((n_tp // 2, PARTS)),
            dma((2,)),
            dma,
            dma((n_tp // 2, 2)),
            dma((2,)),
            dma,
            dma,
            dma,
            dma((n_sp + n_sp // BATCH + NY,)),
            dma((2,)),
            dma,
            dma,
            dma,
            dma,
            dma,
        ],
        compiler_params=pltpu.CompilerParams(
            collective_id=0, has_side_effects=True, vmem_limit_bytes=60 * 2**20
        ),
        name="layer",
    )(
        head_bias,
        tokens.reshape(PARTS, device_rows // PARTS, model),
        w_query, w_key, w_value,
        w_out.reshape(2, local_width // 2, out_width),
    )


def solution(mesh):
    placed = (
        P(("sp", "tp"), None),
        P(None, "tp"),
        P(None, "tp"),
        P(None, "tp"),
        P("tp"),
        P("tp", None),
    )
    return jax.shard_map(
        shards, mesh=mesh, in_specs=placed, out_specs=P(("sp", "tp"), None), check_vma=False
    )
```

```python
import functools
import math

import jax
import jax.numpy as jnp
from jax import lax
from jax.experimental import pallas as pl
from jax.experimental.pallas import tpu as pltpu
from jax.sharding import PartitionSpec as P

MESH = pl.DeviceIdType.MESH
F32, BF16 = jnp.float32, jnp.bfloat16
LOG2E = math.log2(math.e)
PARTS = 4
COLS = 512
EXP_MAX = 126.0
DEAD = -1e30
NZ, NY = 8, 4
SEG = 512
HALF = 256
LANES = 128
DIM = 64
RUN = 64
SHARE = 32
SHARES = SEG // SHARE
TILES = 8
FAR = 1 << 20
BATCH = 2
STEPS = NZ * NY // BATCH


def layer_kernel(
    bias_ref, tokens_ref, wq_ref, wk_ref, wv_ref, wo_ref, out_ref,
    tok, wqkv, wfull, proj, bias_all, kv_own, q_own, q_all, kv_all, q_top, q_low, raw, xs,
    seg_acc, seg_keep, packed, att, att_rows, mixed,
    plane_sem, out_sem, load_sem, tok_send, tok_recv, tok_pair, wo_send, wo_recv, wo_pair,
    bias_send, bias_recv, kv_send, kv_recv, ring_send, share_send, q_send, q_recv, back_send, back_recv,
):
    me = lax.axis_index("sp")
    col = lax.axis_index("tp")
    n_sp, n_tp = NZ * NY, 8
    z, y = me // NY, lax.rem(me, NY)
    place, core = col // 2, lax.rem(col, 2)
    places = n_tp // 2
    sibling = place * 2 + 1 - core
    head_core, head_local = y // 2, lax.rem(y, 2)
    mine = core == head_core

    loads = [
        pltpu.make_async_copy(src, dst, load_sem.at[index])
        for index, (src, dst) in enumerate(
            [
                (tokens_ref, tok.at[col]),
                (wq_ref, wqkv.at[:, 0:LANES]),
                (wk_ref, wqkv.at[:, LANES : 2 * LANES]),
                (wv_ref, wqkv.at[:, 2 * LANES : 3 * LANES]),
                (wo_ref, wfull.at[col]),
            ]
        )
    ]
    for copy in loads:
        copy.start()

    barrier = pltpu.get_barrier_semaphore()
    for step in range(1, n_tp):
        pl.semaphore_signal(
            barrier, inc=1, device_id=(me, lax.rem(col + step, n_tp)), device_id_type=MESH
        )
    for step in range(1, NY):
        peer = z * NY + lax.rem(y + step, NY)
        for other in range(2):
            pl.semaphore_signal(
                barrier, inc=1, device_id=(peer, place * 2 + other), device_id_type=MESH
            )
    for step in range(1, NZ):
        peer = lax.rem(z + step, NZ) * NY + y
        pl.semaphore_signal(barrier, inc=1, device_id=(peer, col), device_id_type=MESH)
    for head in range(2):
        bias_all[core, head] = jnp.full((8, LANES), bias_ref[head] * LOG2E, F32)
    seg_acc[...] = jnp.zeros_like(seg_acc)
    seg_keep[...] = jnp.ones_like(seg_keep)
    pl.semaphore_wait(barrier, n_tp - 1 + 2 * (NY - 1) + NZ - 1)
    for step in range(1, NZ):
        peer = lax.rem(z + step, NZ) * NY + y
        pl.semaphore_signal(plane_sem, inc=1, device_id=(peer, col), device_id_type=MESH)

    def same_core(k):
        return lax.rem(place + k, places) * 2 + core

    def arrived(ref, sem):
        pltpu.make_async_copy(ref, ref, sem).wait()

    def link(kind, own, kept, sent, received, paired, part):
        if kind == 2:
            ahead = part < kept.shape[1] // 2
            block = same_core(3 if ahead else 1)
            src, target = kept.at[block, part], same_core(1 if ahead else 3)
        elif kind < places:
            src, block = own.at[part], col
            target = sibling if kind == 0 else same_core(kind)
        else:
            block = same_core(kind - places + 1)
            src, target = kept.at[block, part], sibling
        inside = kind == 0 or kind >= places
        return pltpu.make_async_remote_copy(
            src_ref=src, dst_ref=kept.at[block, part], send_sem=sent,
            recv_sem=paired.at[part % 2] if inside else received.at[block // 2, part],
            device_id=(me, target), device_id_type=MESH,
        )

    def token_copy(kind, part):
        return link(kind, tokens_ref, tok, tok_send, tok_recv, tok_pair, part)

    def wo_copy(kind, part):
        return link(kind, wo_ref, wfull, wo_send, wo_recv, wo_pair, part)

    def relay(copy, kept, received, part, k):
        block = same_core(k)
        arrived(kept.at[block, part], received.at[block // 2, part])
        copy(places + k - 1, part).start()
        if k != 2 and (part < kept.shape[1] // 2) == (k == 3):
            copy(2, part).start()

    bias_copy = pltpu.make_async_remote_copy(
        src_ref=bias_all.at[core], dst_ref=bias_all.at[core],
        send_sem=bias_send, recv_sem=bias_recv, device_id=(me, sibling), device_id_type=MESH,
    )

    turned = (2, 3, 0, 1)
    for part in range(PARTS // 2):
        token_copy(1, part).start()
        token_copy(3, turned[part]).start()
    for part in (0, 2, 1, 3):
        token_copy(0, part).start()
    bias_copy.start()

    def pair_at(block):
        return n_sp + block // BATCH

    def early_at(part):
        return n_sp + n_sp // BATCH + part

    def own_copy(block, way, stage):
        peer = lax.rem(z + (1 if way == 0 else NZ - 1), NZ) * NY + y
        rows = pl.ds(LANES * (1 - stage), LANES)
        return pltpu.make_async_remote_copy(
            src_ref=kv_all.at[block, core, rows], dst_ref=kv_all.at[block, core, rows],
            send_sem=ring_send.at[way], recv_sem=kv_recv.at[block],
            device_id=(peer, col), device_id_type=MESH,
        )

    def kv_copy(head, half, stage):
        aim = core * 2 + head
        own = aim == y
        sp = jnp.where(own, me, z * NY + aim)
        tp = jnp.where(own, sibling, place * 2 + half)
        return pltpu.make_async_remote_copy(
            src_ref=kv_own.at[head, half, pl.ds(LANES * (1 - stage), LANES)],
            dst_ref=kv_all.at[me, half, pl.ds(LANES * (1 - stage), LANES)],
            send_sem=kv_send,
            recv_sem=kv_recv.at[
                jnp.where(
                    jnp.logical_and(own, core == half),
                    pair_at(me),
                    early_at(y) if stage == 0 else me,
                )
            ],
            device_id=(sp, tp), device_id_type=MESH,
        )

    def ring_copy(block, way):
        peer = lax.rem(z + (1 if way == 0 else NZ - 1), NZ) * NY + y
        return pltpu.make_async_remote_copy(
            src_ref=kv_all.at[block, core], dst_ref=kv_all.at[block, core],
            send_sem=ring_send.at[way], recv_sem=kv_recv.at[block],
            device_id=(peer, col), device_id_type=MESH,
        )

    def share_copy(block):
        return pltpu.make_async_remote_copy(
            src_ref=kv_all.at[block, core], dst_ref=kv_all.at[block, core],
            send_sem=share_send, recv_sem=kv_recv.at[pair_at(block)],
            device_id=(me, sibling), device_id_type=MESH,
        )

    def rows_of(to_z, to_core, block):
        return lax.rem(2 * to_z + to_core + 2 * block, SHARES)

    def q_copy(head, step):
        to_z, to_core = step // 2, lax.rem(step, 2)
        return pltpu.make_async_remote_copy(
            src_ref=q_own.at[head, rows_of(to_z, to_core, me)], dst_ref=q_all.at[me],
            send_sem=q_send, recv_sem=q_recv,
            device_id=(to_z * NY + core * 2 + head, place * 2 + to_core), device_id_type=MESH,
        )

    def q_here(head, step):
        to_z, to_core = step // 2, lax.rem(step, 2)
        return jnp.logical_and(to_z * NY + core * 2 + head == me, to_core == core)

    def back_owner(block):
        return lax.rem(z + block, n_tp)

    my_slot = (place * NY + y) * 2 + core

    def back_here(block):
        return jnp.logical_and(block == me, back_owner(block) == col)

    def back_copy(block):
        return pltpu.make_async_remote_copy(
            src_ref=packed.at[block], dst_ref=att.at[my_slot],
            send_sem=back_send, recv_sem=back_recv,
            device_id=(block, back_owner(block)), device_id_type=MESH,
        )

    for copy in loads:
        copy.wait()
    def turn(value):
        return pltpu.roll(value, DIM, 1)

    lane16 = lax.broadcasted_iota(jnp.int32, (16, LANES), 1)

    def weave(upper, lower):
        first = jnp.where(lane16 < DIM, upper, turn(lower)).astype(BF16)
        second = jnp.where(lane16 < DIM, turn(upper), lower).astype(BF16)
        return first, second

    def strided(i, kind):
        return proj[:, RUN - 1 - i, kind * LANES : (kind + 1) * LANES]

    def send_q(stage, to_z, carry):
        step = 2 * to_z + stage
        for head in range(2):

            @pl.when(jnp.logical_not(q_here(head, step)))
            def _():
                q_copy(head, step).start()

        return carry

    for part in range(PARTS // 2):
        relay(token_copy, tok, tok_recv, part, 3)
        token_copy(1, part + 2).start()
        relay(token_copy, tok, tok_recv, turned[part], 1)
        token_copy(3, turned[part + 2]).start()
    for stage in range(2):
        parts = (stage, stage + 2)
        relay(token_copy, tok, tok_recv, stage + 2, 3)
        relay(token_copy, tok, tok_recv, turned[stage + 2], 1)
        for part in parts:
            relay(token_copy, tok, tok_recv, part, 2)
        arrived(tok.at[pl.ds(0, 2)], tok_pair.at[stage])
        depth, model = tok.shape[2:]
        x = jnp.concatenate([tok[:, part].reshape(n_tp * depth, model) for part in parts], axis=0)
        both = jnp.dot(x, wqkv[...], preferred_element_type=F32)
        for index, part in enumerate(parts):
            proj[:, part * depth : (part + 1) * depth, :] = both[
                index * n_tp * depth : (index + 1) * n_tp * depth
            ].reshape(n_tp, depth, 3 * LANES)
        base = 16 * (1 - stage)
        for i in range(base, base + 16, 2):
            upper = jnp.concatenate([strided(i, 1), strided(i + 1, 1)], axis=0)
            lower = jnp.concatenate([strided(i + 32, 1), strided(i + 33, 1)], axis=0)
            kv_own[0, 0, 8 * i : 8 * i + 16], kv_own[1, 0, 8 * i : 8 * i + 16] = weave(
                upper, lower
            )
        for head in range(2):
            kv_copy(head, 0, stage).start()
        for index in range(2):
            first = base + 32 * index
            block = jnp.concatenate([strided(first + i, 2) for i in range(16)], axis=0)
            flipped = block.T.astype(BF16)
            at = LANES * (1 - stage) + DIM * index
            for head in range(2):
                kv_own[head, 1, at : at + DIM] = flipped[DIM * head : DIM * (head + 1)]
        for head in range(2):
            kv_copy(head, 1, stage).start()
        for block in range(n_tp):
            scale = LOG2E * DIM ** (-0.5)
            upper = proj[block, 16 * stage : 16 * stage + 16, 0:LANES] * scale
            lower = proj[block, 16 * stage + 32 : 16 * stage + 48, 0:LANES] * scale
            share = 2 * block + stage
            q_own[0, share], q_own[1, share] = weave(upper, lower)
        if stage == 0:
            pl.semaphore_wait(plane_sem, NZ - 1)
        lax.fori_loop(0, NZ, functools.partial(send_q, stage), 0)

    for part in range(2):
        for kind in (1, 3, 0):
            wo_copy(kind, 1 - part if kind == 3 else part).start()

    for head in range(2):

        @pl.when(core * 2 + head == y)
        def _():
            kv_all[me] = kv_own[head]
            q_all[me] = q_own[head, rows_of(z, core, me)]

    def halves_here(block):
        return jnp.logical_and(block == me, mine)

    for stage in range(2):
        for step in range(NY):
            part = lax.rem(y + step, NY)
            block = z * NY + part
            rows = pl.ds(LANES * (1 - stage), LANES)

            @pl.when(jnp.logical_not(halves_here(block)))
            def _():
                arrived(
                    kv_all.at[block, core, rows],
                    kv_recv.at[early_at(part) if stage == 0 else block],
                )

            for way in range(2):
                own_copy(block, way, stage).start()

            if stage == 1:

                @pl.when(block != me)
                def _():
                    share_copy(block).start()

    def whole(count, less, buffer, sem):
        for short in range(2):

            @pl.when(less == (short == 1))
            def _():
                arrived(buffer.at[pl.ds(0, count - short)], sem)

    whole(n_sp, mine, q_all, q_recv)

    for tile in range(TILES):
        pieces = []
        for part in range(NY):
            pair = q_all[tile * NY + part].astype(F32)
            pieces.append(jnp.where(lane16 < DIM, pair, 0.0))
            pieces.append(jnp.where(lane16 < DIM, turn(pair), 0.0))
        flipped = jnp.concatenate(pieces, axis=0).T
        q_top[tile] = flipped.astype(BF16)
        q_low[tile] = jnp.concatenate([flipped[DIM:], flipped[:DIM]], axis=0).astype(BF16)

    arrived(bias_all.at[1 - core], bias_recv)

    def suffix(keep):
        row = lax.broadcasted_iota(jnp.int32, keep.shape, 0)
        product = keep
        for step in (1, 2, 4):
            moved = pltpu.roll(product, 8 - step, 0)
            product = product * jnp.where(row + step < 8, moved, 1.0)
        after = jnp.where(row + 1 < 8, pltpu.roll(product, 7, 0), 1.0)
        return after, product[0:1]

    def segment(block, bank, slot, width, bias, reach):
        keep = jnp.ones((8, 2 * width), F32)
        for i in range(RUN // 2):
            score = raw[bank, slot, 8 * i : 8 * i + 8, 0 : 2 * width] + bias
            if reach is not None:
                score = jnp.where(reach > -i, score, DEAD)
            odds = jnp.exp2(jnp.minimum(score, EXP_MAX))
            lose = 1.0 / (1.0 + odds)
            xs[bank, slot, 8 * i : 8 * i + 8, 0 : 2 * width] = odds * lose * keep
            keep = keep * lose
        near, far = keep[:, :width], keep[:, width:]
        after, whole = suffix(near * far)
        values = kv_all[block, 1]
        out = None
        for half, factor in enumerate((after, after * near)):
            part = xs[bank, slot, :, half * width : (half + 1) * width].reshape(RUN // 2, 8, width)
            weight = (part * factor[None]).reshape(HALF, width).astype(BF16)
            first = half * DIM
            value = jnp.concatenate(
                [values[first : first + DIM], values[LANES + first : LANES + first + DIM]], axis=1
            )
            term = jnp.dot(value, weight, preferred_element_type=F32)
            out = term if out is None else out + term
        return out, whole

    def cover(group, part, tile, count, diagonal, bank):
        width = count * LANES
        q = jnp.concatenate(
            [q_top[tile + n] for n in range(count)] + [q_low[tile + n] for n in range(count)],
            axis=1,
        )
        bias = bias_all[head_core, head_local]
        bias = jnp.concatenate([bias] * (2 * count), axis=1)
        if diagonal:
            lane = lax.broadcasted_iota(jnp.int32, (8, 2 * width), 1)
            row = lax.broadcasted_iota(jnp.int32, (8, 2 * width), 0)
            half = lane // width
            inside = lax.rem(lane, width)
            owner = lax.rem(inside // SHARE, NY)
            share = rows_of(z, core, tile * NY + owner)
            place_in = 32 * (lax.rem(inside, SHARE) // 16) + lax.rem(inside, 16)
            query = SEG * owner + 64 * (share // 2) + 16 * lax.rem(share, 2) + place_in
            query = jnp.where(inside < LANES, query, FAR)
            reach = query - row * RUN - (RUN - 1) + half * (RUN // 2) - SEG * part
        first = group * NY + part
        raw[bank, :, :, 0 : 2 * width] = jnp.dot(
            kv_all[pl.ds(first, BATCH), 0].reshape(BATCH * HALF, LANES), q,
            preferred_element_type=F32,
        ).reshape(BATCH, HALF, 2 * width)
        acc = [seg_acc[group, tile + n] for n in range(count)]
        keep = [seg_keep[group, tile + n][0:1] for n in range(count)]
        for index in range(BATCH):
            limit = reach - SEG * index if diagonal else None
            out, whole = segment(first + index, bank, index, width, bias, limit)
            for n in range(count):
                lanes = slice(n * LANES, (n + 1) * LANES)
                acc[n] = acc[n] * whole[:, lanes] + out[:, lanes]
                keep[n] = keep[n] * whole[:, lanes]
        for n in range(count):
            seg_acc[group, tile + n] = acc[n]
            seg_keep[group, tile + n] = jnp.broadcast_to(keep[n], (8, LANES))

    def attend(group, part, between):
        count = TILES - group
        odd = lax.rem(count, 2)
        pairs = (count - 1) // 2
        first = group + 2 - odd

        for single in range(2):
            for more in range(2):

                @pl.when(jnp.logical_and(odd == single, (pairs > 0) == (more == 1)))
                def _():
                    cover(group, part, group, 2 - single, True, 0)
                    if more:
                        cover(group, part, first, 2, False, 1)

        between()

        @pl.when(pairs == 2)
        def _():
            cover(group, part, first + 2, 2, False, 0)

        @pl.when(pairs == 3)
        def _():
            cover(group, part, first + 2, 2, False, 0)
            cover(group, part, first + 4, 2, False, 1)

    def stop_at(step):
        turn_of = lax.rem(step + 2, 4)
        far = step >= STEPS - 2
        distance = (step + 2) // 4
        own = step < 2
        behind = jnp.logical_or(jnp.logical_and(far, turn_of == 0), lax.rem(step, 2) == 0)
        part = jnp.where(jnp.logical_or(own, far), lax.rem(step, 2), turn_of // 2) * BATCH
        group = lax.rem(z + NZ + jnp.where(behind, -distance, distance), NZ)
        return group, part

    def forward(index):
        distance, turn_of = index // NZ + 1, lax.rem(index, NZ)
        last = distance == NZ // 2
        behind = lax.rem(index, 2) == 0
        part = jnp.where(last, lax.rem(index, 2) * BATCH, 0) + turn_of // 2
        group = lax.rem(z + NZ + jnp.where(behind, -distance, distance), NZ)
        block = group * NY + part
        arrived(kv_all.at[block, core], kv_recv.at[block])
        for way in range(2):
            onward = jnp.logical_or(
                distance < 3, jnp.logical_and(distance == 3, (part < BATCH) == (way == 0))
            )

            @pl.when(jnp.logical_and(behind == (way == 0), onward))
            def _():
                ring_copy(block, way).start()

        share_copy(block).start()

    def visit(step, carry):
        def forward_if(low, high, index):
            @pl.when(jnp.logical_and(step >= low, step < high))
            def _():
                forward(index)

        forward_if(2, 3, 2)
        forward_if(2, 3, 3)
        forward_if(3, STEPS - 2, 2 * step)

        @pl.when(step == STEPS // 2)
        def _():
            for part in range(2):
                relay(wo_copy, wfull, wo_recv, part, 3)
                relay(wo_copy, wfull, wo_recv, 1 - part, 1)

        @pl.when(step == STEPS - 2)
        def _():
            for part in range(2):
                relay(wo_copy, wfull, wo_recv, part, 2)

        group, part = stop_at(step)
        block = group * NY + part
        here = jnp.logical_and(block // BATCH == me // BATCH, mine)
        for short in range(2):

            @pl.when(here == (short == 1))
            def _():
                arrived(
                    kv_all.at[pl.ds(block, BATCH - short), 1 - core], kv_recv.at[pair_at(block)]
                )

        def between():
            forward_if(1, 2, 0)
            forward_if(1, 2, 1)
            forward_if(2, 3, 4)
            forward_if(2, STEPS - 2, 2 * step + 1)

        attend(group, part, between)
        return carry

    lax.fori_loop(0, STEPS, visit, 0)

    def combine(tile):
        acc = seg_acc[0, tile]
        for group in range(1, NZ):
            acc = acc * seg_keep[group, tile][0:1] + seg_acc[group, tile]
        return acc

    for pair in range(TILES // 2):
        flipped = jnp.concatenate([combine(2 * pair), combine(2 * pair + 1)], axis=0).T
        for part in range(NY):
            upper = flipped[SHARE * part : SHARE * part + 16]
            lower = flipped[SHARE * part + 16 : SHARE * (part + 1)]
            for n, folded in enumerate(weave(upper, lower)):
                block = (2 * pair + n) * NY + part
                packed[block] = folded
                here = back_here(block)

                @pl.when(here)
                def _():
                    att[my_slot] = folded

                @pl.when(jnp.logical_not(here))
                def _():
                    back_copy(block).start()

    bias_copy.wait_send()
    arrived(wfull.at[pl.ds(0, n_tp - 1)], wo_send)
    arrived(tok.at[pl.ds(0, n_tp - 1)], tok_send)
    arrived(kv_own, kv_send)
    whole(n_sp, mine, q_all, q_send)
    for way in range(2):
        arrived(kv_all.at[pl.ds(0, 14), 0], ring_send.at[way])
    arrived(kv_all.at[pl.ds(0, n_sp - 1), 0], share_send)
    whole(n_sp, back_here(me), att, back_send)
    whole(n_sp, back_here(me), att, back_recv)

    for pair in range(n_tp):
        for sub in range(2):
            values = []
            for head in (2 * pair, 2 * pair + 1):
                slot = head * 2 + sub
                values.append(att[slot].astype(F32))
            top = jnp.where(lane16 < DIM, values[0], turn(values[1]))
            low = jnp.where(lane16 < DIM, turn(values[0]), values[1])
            cols = slice(pair * LANES, (pair + 1) * LANES)
            att_rows[16 * sub : 16 * sub + 16, cols] = top.astype(BF16)
            att_rows[16 * sub + 32 : 16 * sub + 48, cols] = low.astype(BF16)

    for part in range(2):
        arrived(wfull.at[pl.ds(0, 2)], wo_pair.at[part])

    def put(first):
        return pltpu.make_async_copy(
            mixed.at[:, pl.ds(first, COLS)], out_ref.at[:, pl.ds(first, COLS)],
            out_sem,
        )

    for first in range(0, out_ref.shape[1], COLS):
        w = wfull[:, :, :, first : first + COLS].reshape(att_rows.shape[1], COLS)
        mixed[:, first : first + COLS] = jnp.dot(
            att_rows[...], w, preferred_element_type=F32
        ).astype(BF16)
        put(first).start()
    pltpu.make_async_copy(mixed, out_ref, out_sem).wait()


def shards(tokens, w_query, w_key, w_value, head_bias, w_out):
    model, local_width = w_query.shape
    n_tp = lax.axis_size("tp")
    n_sp = lax.axis_size("sp")
    device_rows = tokens.shape[0]
    out_width = w_out.shape[1]

    smem = pl.BlockSpec(memory_space=pltpu.SMEM)
    anywhere = pl.BlockSpec(memory_space=pl.ANY)
    dma = pltpu.SemaphoreType.DMA

    def vmem(*shape):
        return pltpu.VMEM(shape, BF16)

    return pl.pallas_call(
        layer_kernel,
        out_shape=jax.ShapeDtypeStruct((device_rows, out_width), BF16),
        in_specs=[smem] + [anywhere] * 5,
        out_specs=anywhere,
        scratch_shapes=[
            vmem(n_tp, PARTS, device_rows // PARTS, model),
            vmem(model, 3 * local_width),
            vmem(n_tp, 2, local_width // 2, out_width),
            pltpu.VMEM((n_tp, device_rows, 3 * local_width), F32),
            pltpu.VMEM((2, 2, 8, LANES), F32),
            vmem(2, 2, HALF, LANES),
            vmem(2, SHARES, SHARE // 2, LANES),
            vmem(n_sp, SHARE // 2, LANES),
            vmem(n_sp, 2, HALF, LANES),
            vmem(TILES, LANES, LANES),
            vmem(TILES, LANES, LANES),
            pltpu.VMEM((2, BATCH, HALF, 4 * LANES), F32),
            pltpu.VMEM((2, BATCH, HALF, 4 * LANES), F32),
            pltpu.VMEM((NZ, TILES, DIM, LANES), F32),
            pltpu.VMEM((NZ, TILES, 8, LANES), F32),
            vmem(n_sp, SHARE // 2, LANES),
            vmem(32, SHARE // 2, LANES),
            vmem(device_rows, n_tp * local_width),
            vmem(device_rows, out_width),
            pltpu.SemaphoreType.REGULAR,
            dma,
            dma((5,)),
            dma,
            dma((n_tp // 2, PARTS)),
            dma((2,)),
            dma,
            dma((n_tp // 2, 2)),
            dma((2,)),
            dma,
            dma,
            dma,
            dma((n_sp + n_sp // BATCH + NY,)),
            dma((2,)),
            dma,
            dma,
            dma,
            dma,
            dma,
        ],
        compiler_params=pltpu.CompilerParams(
            collective_id=0, has_side_effects=True, vmem_limit_bytes=60 * 2**20
        ),
        name="layer",
    )(
        head_bias,
        tokens.reshape(PARTS, device_rows // PARTS, model),
        w_query, w_key, w_value,
        w_out.reshape(2, local_width // 2, out_width),
    )


def solution(mesh):
    placed = (
        P(("sp", "tp"), None),
        P(None, "tp"),
        P(None, "tp"),
        P(None, "tp"),
        P("tp"),
        P("tp", None),
    )
    return jax.shard_map(
        shards, mesh=mesh, in_specs=placed, out_specs=P(("sp", "tp"), None), check_vma=False
    )
```
